32 devices in a mesh: kv: 8 (over z, y), tp: 4 (over x, core).
Axes of the slice: x: 2, y: 2, z: 4, core: 2. Of those that a mesh axis runs over, the one named last changes fastest.
Arguments:
- tokens: bfloat16 [5120, 4096], P('kv'), may hold values from -48 to 48
- query_weight: bfloat16 [4096, 2048], P(None, 'tp'), may hold values from -0.09375 to 0.09375
- key_weight: bfloat16 [4096, 512], P(None, 'tp'), may hold values from -0.09375 to 0.09375
- value_weight: bfloat16 [4096, 512], P(None, 'tp'), may hold values from -0.09375 to 0.09375
- gate_weight: bfloat16 [4096, 64], replicated, may hold values from -0.09375 to 0.09375
- summary_pos: bfloat16 [32, 64], replicated, may hold values from -6 to 6
- key_mixing: bfloat16 [32, 8], replicated, may hold values from -1 to 1
- value_mixing: bfloat16 [32, 8], replicated, may hold values from -1 to 1
- out_weight: bfloat16 [2048, 4096], P('tp'), may hold values from -0.125 to 0.125
- chosen: int32 [80, 8, 16], P('kv', 'tp'), may hold values from 0 to 79, as said below
Outputs:
- mixed: bfloat16 [5120, 4096], P(('kv', 'tp'))
The draws below stay inside these ranges and needn't reach their ends.
Inputs may be any that keep to these rules, and one draw needn't show every extreme that they name: `chosen`: entry [b, g, 0] is b itself; every entry is at most b. For the query blocks of one index of kv, one key head and any OTHER index of kv, at most 2 distinct blocks of that index's 64-position blocks are named, and exactly 2 of the index just before. Entries may repeat.
All inputs are finite; a program needn't handle non-finite values.
Results may differ from the reference program's by a relative error of at most 0.013.
The reference program's roundings to bfloat16 on the way count: a program that leaves them out, or rounds other values in their place, can miss the bound.
Values may be sent and summed in bfloat16 or wider, within the bound.
A program may use at most 192 MiB of HBM per device.

```python
import jax
import jax.numpy as jnp
from jax import lax

D = 4096
HEADS = 32
KV_HEADS = 8
HD = 64
CMP = 32
SB = 64
N_SEL = 16
CAP = 2
TOK_DEV = 640
TOKENS = 5120
N_TP = 4


def draw_tokens(key, part):
    base = jax.random.normal(key, (TOKENS, D), jnp.float32)
    return jnp.clip(base, -6.0, 6.0).astype(jnp.bfloat16)


def draw_chosen(key, part):
    per_device = TOK_DEV // SB
    block_total = TOKENS // SB
    device_total = block_total // per_device
    grid_shape = (block_total, KV_HEADS, N_SEL)
    column_shape = (block_total, KV_HEADS, 1)
    streams = jax.random.split(key, 8)
    query_block = jnp.arange(block_total, dtype=jnp.int32)[:, None, None]
    device_of = query_block // per_device
    head_ids = jnp.arange(KV_HEADS, dtype=jnp.int32)[None, :, None]
    first_pick = jax.random.randint(streams[0], (device_total, KV_HEADS, device_total), 0, per_device)
    pick_step = jax.random.randint(streams[1], (device_total, KV_HEADS, device_total), 1, per_device)
    popular = jax.random.randint(streams[2], (4,), 0, device_total)
    use_popular = jax.random.randint(streams[3], grid_shape, 0, 2)
    popular_pick = popular[jax.random.randint(streams[4], grid_shape, 0, 4)]
    drawn_pick = jax.random.randint(streams[5], grid_shape, 0, device_of + 1)
    source = jnp.where((use_popular == 1) & (popular_pick <= device_of), popular_pick, drawn_pick)
    which = jax.random.randint(streams[6], grid_shape, 0, CAP)
    candidate = (first_pick[device_of, head_ids, source] + which * pick_step[device_of, head_ids, source]) % per_device
    at_home = jax.random.randint(streams[7], grid_shape, device_of * per_device, query_block + 1)
    picks = jnp.where(source == device_of, at_home, source * per_device + candidate)
    before = jnp.maximum(device_of - 1, 0)
    half_away = jnp.maximum(device_of - device_total // 2, 0)
    first_before = first_pick[device_of, head_ids, before]
    own_block = jnp.broadcast_to(query_block, column_shape)
    slot_one = jnp.where(device_of >= 1, before * per_device + first_before, own_block)
    slot_two = jnp.where(device_of >= device_total // 2, half_away * per_device + first_pick[device_of, head_ids, half_away], own_block)
    slot_three = jnp.where(device_of >= 1, before * per_device + (first_before + pick_step[device_of, head_ids, before]) % per_device, own_block)
    return jnp.concatenate([own_block, jnp.broadcast_to(slot_one, column_shape), jnp.broadcast_to(slot_two, column_shape), jnp.broadcast_to(slot_three, column_shape), picks[:, :, 4:]], axis=2).astype(jnp.int32)


def shard_levels(stream_key, shape, pieces, smallest, high):
    def one(position, shards_of):
        draws = jax.random.uniform(jax.random.fold_in(jax.random.fold_in(stream_key, 6), position), (shards_of,), jnp.float32, smallest / len(pieces), high / len(pieces))
        return jnp.repeat(jnp.exp(draws), shape[position] // shards_of).reshape((-1,) + (1,) * (len(shape) - position - 1))

    gain = one(*pieces[0])
    for cut in pieces[1:]:
        gain = gain * one(*cut)
    return gain


def bell_draw(rng, extent, spread, most, cuts=(), kind=jnp.bfloat16):
    result = jax.random.normal(rng, extent, jnp.float32) * spread
    if len(cuts) > 0:
        result = shard_levels(rng, extent, cuts, -0.22, 0.18) * result
    return jnp.clip(result, min=-most, max=most).astype(kind)


def setup_inputs(seed: int = 0) -> dict:
    arg_keys = jax.random.split(jax.random.key(seed), 11)
    return {
        "tokens": draw_tokens(jax.random.fold_in(arg_keys[10], 71), 0),
        "query_weight": bell_draw(arg_keys[1], (D, HEADS * HD), D ** -0.5, 0.09375, ((1, 4),)),
        "key_weight": bell_draw(arg_keys[2], (D, KV_HEADS * HD), D ** -0.5, 0.09375, ((1, 4),)),
        "value_weight": bell_draw(arg_keys[3], (D, KV_HEADS * HD), D ** -0.5, 0.09375, ((1, 4),)),
        "gate_weight": bell_draw(arg_keys[4], (D, 2 * HEADS), D ** -0.5, 0.09375),
        "summary_pos": bell_draw(arg_keys[5], (CMP, HD), 1.0, 6.0),
        "key_mixing": bell_draw(arg_keys[6], (CMP, KV_HEADS), CMP ** -0.5, 1.0),
        "value_mixing": bell_draw(arg_keys[7], (CMP, KV_HEADS), CMP ** -0.5, 1.0),
        "out_weight": bell_draw(arg_keys[8], (HEADS * HD, D), (HEADS * HD) ** -0.5, 0.125, ((0, 4),)),
        "chosen": draw_chosen(jax.random.fold_in(arg_keys[10], 71), 0),
    }


floor_score = -1e30


def masked_weights(scores, visible):
    probs = jax.nn.softmax(jnp.where(visible, scores, floor_score), axis=-1)
    return jnp.where(jnp.any(visible, axis=-1, keepdims=True), probs, 0.0)


def first_named(picked_ids):
    slot_count = picked_ids.shape[-1]
    repeated = picked_ids[..., :, None] == picked_ids[..., None, :]
    earlier = jnp.arange(slot_count)[None, :] < jnp.arange(slot_count)[:, None]
    return jnp.logical_not(jnp.any(repeated & earlier, axis=-1))


def summarize(source, offsets, mixing):
    span_count = source.shape[0] // CMP
    windows = source.astype(jnp.float32).reshape(span_count, CMP, source.shape[1], HD)
    windows = windows + offsets.astype(jnp.float32)[None, :, None, :]
    return jnp.einsum('njgd,jg->ngd', windows, mixing.astype(jnp.float32),
                      precision=lax.Precision.HIGHEST).astype(jnp.bfloat16)


def reference(tokens, query_weight, key_weight, value_weight, gate_weight, summary_pos, key_mixing,
              value_mixing, out_weight, chosen):
    length = tokens.shape[0]
    group_size = HEADS // KV_HEADS
    score_scale = HD ** -0.5
    queries = jnp.dot(tokens, query_weight, preferred_element_type=jnp.float32).astype(jnp.bfloat16)
    key_rows = jnp.dot(tokens, key_weight, preferred_element_type=jnp.float32).astype(jnp.bfloat16)
    key_rows = key_rows.reshape(length, KV_HEADS, HD)
    value_rows = jnp.dot(tokens, value_weight, preferred_element_type=jnp.float32).astype(jnp.bfloat16)
    value_rows = value_rows.reshape(length, KV_HEADS, HD)
    gate_vals = jax.nn.sigmoid(jnp.dot(tokens, gate_weight, preferred_element_type=jnp.float32))
    gate_vals = gate_vals.reshape(length // SB, SB, KV_HEADS, group_size, 2)
    key_summary = summarize(key_rows, summary_pos, key_mixing).astype(jnp.float32)
    value_summary = summarize(value_rows, summary_pos, value_mixing).astype(jnp.float32)
    span_ends = jnp.arange(length // CMP, dtype=jnp.int32) * CMP + (CMP - 1)
    block_table = jnp.concatenate([key_rows, value_rows], axis=-1).reshape(length // SB, SB, KV_HEADS, 2 * HD)
    head_ids = jnp.arange(KV_HEADS, dtype=jnp.int32)[:, None]
    unique_all = first_named(chosen)

    def one_block(inputs):
        query_blk, gate_blk, picked_ids, unique, offset = inputs
        query_pos = offset + jnp.arange(SB, dtype=jnp.int32)
        query_f = query_blk.astype(jnp.float32).reshape(SB, KV_HEADS, group_size, HD)
        summary_scores = jnp.einsum('qgrd,ngd->grqn', query_f, key_summary) * score_scale
        summary_probs = masked_weights(summary_scores, (span_ends[None, :] <= query_pos[:, None])[None, None])
        summary_probs = lax.optimization_barrier(summary_probs.astype(jnp.bfloat16)).astype(jnp.float32)
        summary_out = jnp.einsum('grqn,ngd->qgrd', summary_probs, value_summary)
        picked = block_table[picked_ids, :, head_ids, :]
        picked = picked.reshape(KV_HEADS, N_SEL * SB, 2 * HD).astype(jnp.float32)
        key_pos = (picked_ids[:, :, None] * SB + jnp.arange(SB, dtype=jnp.int32)).reshape(KV_HEADS, N_SEL * SB)
        counted = jnp.broadcast_to(unique[:, :, None], (KV_HEADS, N_SEL, SB)).reshape(KV_HEADS, N_SEL * SB)
        visible = counted[:, None, :] & (key_pos[:, None, :] <= query_pos[None, :, None])
        chosen_scores = jnp.einsum('qgrd,gmd->grqm', query_f, picked[..., :HD]) * score_scale
        chosen_probs = masked_weights(chosen_scores, visible[:, None])
        chosen_probs = lax.optimization_barrier(chosen_probs.astype(jnp.bfloat16)).astype(jnp.float32)
        chosen_out = jnp.einsum('grqm,gmd->qgrd', chosen_probs, picked[..., HD:])
        blended = gate_blk[..., 0:1] * summary_out + gate_blk[..., 1:2] * chosen_out
        return blended.reshape(SB, HEADS * HD).astype(jnp.bfloat16)

    offsets = jnp.arange(length // SB, dtype=jnp.int32) * SB
    attention = lax.map(one_block, (queries.reshape(length // SB, SB, HEADS * HD), gate_vals, chosen,
                                    unique_all, offsets)).reshape(length, HEADS * HD)
    width = HEADS * HD // N_TP
    summed = jnp.zeros((length, D), jnp.float32)
    for head_part in range(N_TP):
        partial_value = jnp.dot(attention[:, head_part * width:(head_part + 1) * width],
                          out_weight[head_part * width:(head_part + 1) * width],
                          preferred_element_type=jnp.float32).astype(jnp.bfloat16)
        summed = summed + lax.optimization_barrier(partial_value).astype(jnp.float32)
    return summed.astype(jnp.bfloat16)
```

```python
import functools
import types

import jax
import jax.numpy as jnp
from jax import lax
from jax.experimental import pallas as pl
from jax.experimental.pallas import tpu as pltpu
from jax.sharding import PartitionSpec as P

HD = 64
CMP = 32
SB = 64
N_SEL = 16
LANES = 128
PIECES = 4
LOW = -1e30
F32 = jnp.float32
BF16 = jnp.bfloat16
MESH = pl.DeviceIdType.MESH
VMEM_LIMIT = 64_000_000
NT = (((1,), (1,)), ((), ()))


def requests(n, G, nb, k):
    place = lax.broadcasted_iota(jnp.int32, k.named.shape, 1)
    for g in range(G):
        k.named[g] = jnp.full(k.named.shape[1:], -1, jnp.int32)
        k.named[g, :nb, :N_SEL] = k.chosen[:, g, :]
        c = k.named[g]
        source = jnp.zeros_like(c)
        for s in range(1, n):
            source = source + jnp.where(c >= s * nb, 1, 0)
        inside = c - source * nb
        for s in range(n):
            hit = (c >= 0) & (source == s)
            lo = jnp.where(hit, inside, nb)
            lo = jnp.min(jnp.min(lo, axis=0, keepdims=True), axis=1, keepdims=True)
            lo = jnp.where(lo == nb, 0, lo)
            hi = jnp.where(hit, inside, 0)
            hi = jnp.max(jnp.max(hi, axis=0, keepdims=True), axis=1, keepdims=True)
            k.req[s, 2 * g : 2 * g + 1] = jnp.broadcast_to(lo, (1, LANES))
            k.req[s, 2 * g + 1 : 2 * g + 2] = jnp.broadcast_to(hi, (1, LANES))


def biases(n, G, nb, k, me):
    for g in range(G):
        c = k.named[g]
        lane = lax.broadcasted_iota(jnp.int32, c.shape, 1)
        bias = jnp.full(c.shape, LOW, F32)

        def mark(bias, hit, at):
            hit = jnp.max(jnp.where(hit, 1.0, 0.0), axis=1, keepdims=True)
            return jnp.where((lane == at) & (hit > 0.0), 0.0, bias)

        for j in range(nb):
            bias = mark(bias, c == me * nb + j, j)
        for s in range(n - 1):
            lo = k.req[s, 2 * g : 2 * g + 1]
            hi = k.req[s, 2 * g + 1 : 2 * g + 2]
            at = jnp.where(me > s, nb + 2 * (me - s - 1), -5)
            real = c >= 0
            bias = mark(bias, real & (c == s * nb + lo), at)
            bias = mark(bias, real & (c == s * nb + hi) & (hi != lo), at + 1)
        k.bias[g] = bias


class Travel:
    def __init__(self, k, pieces):
        tp, me = lax.axis_index("tp"), lax.axis_index("kv")
        core, side = lax.rem(tp, 2), tp // 2
        self.k, self.pieces = k, pieces
        self.across = {"tp": (1 - side) * 2 + core}
        self.partner = {"tp": side * 2 + 1 - core}
        self.beside = {"kv": me + 1 - 2 * lax.rem(me, 2)}
        self.mine = lax.rem(me, 2)
        self.columns = k.wfar.shape[2]
        self.first = k.ow.shape[1] - self.columns
        self.size = self.columns // 2 // pieces

    def cols(self, half, j, base=0):
        at = base + half * (self.columns // 2) + j * self.size
        return pl.ds(pl.multiple_of(at, LANES), self.size)

    def copy(self, src, dst, send, recv, target):
        return pltpu.make_async_remote_copy(
            src_ref=src, dst_ref=dst, send_sem=send, recv_sem=recv,
            device_id=target, device_id_type=MESH,
        )

    def x(self, j):
        k = self.k
        return self.copy(
            k.ow_hbm.at[:, self.cols(self.mine, j, self.first)], k.wfar.at[1, :, self.cols(self.mine, j)],
            k.wx_s.at[j], k.wx_r.at[j], self.across,
        )

    def p(self):
        k = self.k
        return self.copy(
            k.ow_hbm.at[:, pl.ds(self.first, self.columns)], k.wfar.at[0], k.wp_s, k.wp_r, self.partner
        )

    def y(self, j):
        here = self.k.wfar.at[1, :, self.cols(self.mine, j)]
        return self.copy(here, here, self.k.wy_s.at[j], self.k.wy_r.at[j], self.beside)

    def y_arrival(self, j):
        here = self.k.wfar.at[1, :, self.cols(1 - self.mine, j)]
        return self.copy(here, here, self.k.wy_s.at[j], self.k.wy_r.at[j], self.beside)

    def d(self, h, j):
        k = self.k
        at = self.cols(self.mine if h == 0 else 1 - self.mine, j)
        return self.copy(
            k.wfar.at[1, :, at], k.wfar.at[2, :, at], k.wd_s.at[h, j], k.wd_r.at[h, j], self.partner
        )

    def start(self):
        for j in range(self.pieces):
            self.x(j).start()
        self.p().start()

    def relay_x(self, j):
        self.x(j).wait_recv()
        self.y(j).start()
        self.d(0, j).start()

    def relay_y(self, j):
        self.y_arrival(j).wait_recv()
        self.d(1, j).start()

    def arrived(self):
        self.p().wait_recv()
        for h in range(2):
            for j in range(self.pieces):
                self.d(h, j).wait_recv()

    def sent(self):
        self.p().wait_send()
        for j in range(self.pieces):
            self.x(j).wait_send()
            self.y(j).wait_send()
            for h in range(2):
                self.d(h, j).wait_send()


def project(n, G, R, nb, kc, k, ow_loads, travel):
    tp = lax.axis_index("tp")
    me = lax.axis_index("kv")
    rows = nb * SB
    depth = k.tok.shape[1]
    chunks = depth // kc
    spans = rows // CMP
    slot = k.sum_send.shape[0] // 2

    def part(i):
        return pl.ds(i * kc, kc)

    def loads(i):
        return [
            pltpu.make_async_copy(k.tok_hbm.at[:, part(i)], k.tok.at[:, part(i)], k.sem_tok.at[i]),
            pltpu.make_async_copy(k.kw_hbm.at[part(i)], k.kvw.at[part(i), pl.ds(0, LANES)], k.sem_kw.at[i]),
            pltpu.make_async_copy(k.vw_hbm.at[part(i)], k.kvw.at[part(i), pl.ds(LANES, LANES)], k.sem_vw.at[i]),
        ]

    half_gates = k.gw.shape[0] // 2

    def late(i):
        return [
            pltpu.make_async_copy(k.qw_hbm.at[part(i)], k.qw.at[part(i)], k.sem_qw.at[i]),
            pltpu.make_async_copy(k.gw_hbm.at[:, part(i)], k.gw.at[pl.ds(0, half_gates), part(i)], k.sem_gw.at[0, i]),
            pltpu.make_async_copy(k.gw_hbm.at[:, part(i)], k.gw.at[pl.ds(half_gates, half_gates), part(i)], k.sem_gw.at[1, i]),
        ]

    for i in range(chunks):
        for c in loads(i):
            c.start()

    barrier = pltpu.get_barrier_semaphore()
    for i in range(1, n):
        pl.semaphore_signal(
            barrier, inc=1, device_id={"kv": lax.rem(me + i, n)}, device_id_type=MESH
        )
    for i in range(1, 4):
        pl.semaphore_signal(barrier, inc=1, device_id={"tp": lax.rem(tp + i, 4)}, device_id_type=MESH)

    requests(n, G, nb, k)
    pl.semaphore_wait(barrier, n + 2)

    def req_copy(i):
        return pltpu.make_async_remote_copy(
            src_ref=k.req.at[lax.rem(me + n - i, n)], dst_ref=k.req_in.at[i],
            send_sem=k.req_s.at[i], recv_sem=k.req_r.at[i],
            device_id={"kv": lax.rem(me + n - i, n)}, device_id_type=MESH,
        )

    def req_local(i):
        return pltpu.make_async_copy(k.req_in.at[i], k.req_smem.at[i], k.sem_req.at[i])

    def blk_copy(i):
        return pltpu.make_async_remote_copy(
            src_ref=k.send.at[i], dst_ref=k.far.at[i - 1],
            send_sem=k.blk_s.at[i], recv_sem=k.blk_r.at[i],
            device_id={"kv": lax.rem(me + i, n)}, device_id_type=MESH,
        )

    def sum_copy(i):
        return pltpu.make_async_remote_copy(
            src_ref=k.sum_send, dst_ref=k.sum_in.at[i],
            send_sem=k.sum_s.at[i], recv_sem=k.sum_r.at[i],
            device_id={"kv": lax.rem(me + i, n)}, device_id_type=MESH,
        )

    for i in range(1, n):
        req_copy(i).start()
    travel.start()

    biases(n, G, nb, k, me)
    bias_copy = pltpu.make_async_copy(k.bias, k.bias_smem, k.sem_bias)
    bias_copy.start()
    for i in range(1, n):

        @pl.when(me < i)
        def _():
            k.far[i - 1] = jnp.zeros(k.far.shape[1:], BF16)

    k.sum_key[...] = jnp.zeros_like(k.sum_key)
    k.sum_val[...] = jnp.zeros_like(k.sum_val)
    k.acc[:, : 2 * LANES] = jnp.zeros((rows, 2 * LANES), F32)

    def kv_step(i, carry):
        for c in loads(i):
            c.wait()
        for c in late(i):
            c.start()
        k.acc[:, : 2 * LANES] += jnp.dot(k.tok[:, part(i)], k.kvw[part(i), :], preferred_element_type=F32)
        return carry

    lax.fori_loop(0, chunks, kv_step, 0)
    first = range(1, min(4, n))
    for i in first:
        req_copy(i).wait_recv()
        req_local(i).start()
    for c in ow_loads:
        c.start()
    low = lax.broadcasted_iota(jnp.int32, (SB, LANES), 1) < HD
    mix_row = lax.broadcasted_iota(jnp.int32, k.km.shape, 0)
    mix_low = lax.broadcasted_iota(jnp.int32, (CMP, LANES), 1) < HD
    diagonal = lax.broadcasted_iota(jnp.int32, (CMP, CMP), 0) == lax.broadcasted_iota(
        jnp.int32, (CMP, CMP), 1
    )

    def mix_column(ref, head):
        line = jnp.where(mix_row == head, ref[...].astype(F32), 0.0)
        line = jnp.sum(line, axis=0, keepdims=True)
        return jnp.sum(jnp.where(diagonal, line, 0.0), axis=1, keepdims=True)

    k.pos_wide[:, :HD] = k.pos[...].astype(F32)
    k.pos_wide[:, HD:] = k.pos[...].astype(F32)
    both = []
    for ref, at in ((k.km, 0), (k.vm, LANES)):
        mix = jnp.where(mix_low, mix_column(ref, tp * G), mix_column(ref, tp * G + 1))
        t = k.acc[:, at : at + LANES].astype(BF16).astype(F32).reshape(spans, CMP, LANES)
        s = jnp.sum((t + k.pos_wide[...][None]) * mix[None], axis=1)
        both.append(jnp.concatenate([s, jnp.zeros((slot - spans, LANES), F32)], axis=0))
    both = jnp.concatenate(both, axis=0).astype(BF16)
    k.sum_send[...] = both
    k.sum_key[:slot] = both.astype(F32)[:slot]
    k.sum_val[:slot] = both.astype(F32)[slot:]
    for i in range(1, n):

        @pl.when(me + i < n)
        def _():
            sum_copy(i).start()

    for t in range(nb // 2):
        r0 = slice(t * LANES, (t + 1) * LANES)
        keys = k.acc[r0, :LANES].astype(BF16).astype(F32)
        vals = jnp.transpose(k.acc[r0, LANES : 2 * LANES].astype(BF16).astype(F32))
        k.keys[r0, :] = keys.astype(BF16)
        k.vals[:, r0] = vals.astype(BF16)
        keys_r = pltpu.roll(keys, HD, 1)
        vals_r = pltpu.roll(vals, HD, 1)
        for h in range(2):
            kk, kr = keys[h * SB : (h + 1) * SB], keys_r[h * SB : (h + 1) * SB]
            v_left, v_right = (vals, vals_r) if h == 0 else (vals_r, vals)
            for g in range(G):
                left, right = (kk, kr) if g == 0 else (kr, kk)
                v = slice(g * HD, (g + 1) * HD)
                c = g * nb + 2 * t + h
                k.left[c, :SB] = jnp.where(low, left, 0.0).astype(BF16)
                k.left[c, SB:] = jnp.where(low, v_left[v], 0.0).astype(BF16)
                k.right[c, :SB] = jnp.where(low, 0.0, right).astype(BF16)
                k.right[c, SB:] = jnp.where(low, 0.0, v_right[v]).astype(BF16)
    def answer(i):
        req_local(i).wait()

        @pl.when(me + i < n)
        def _():
            for g in range(G):
                lo = k.req_smem[i, 2 * g, 0]
                hi = k.req_smem[i, 2 * g + 1, 0]
                k.send[i, g] = k.left[g * nb + lo] + k.right[g * nb + hi]
            blk_copy(i).start()

    for i in reversed(first):
        answer(i)
    for i in range(len(first) + 1, n):
        req_copy(i).wait_recv()
        req_local(i).start()
    for i in range(n - 1, len(first), -1):
        answer(i)

    k.acc[...] = jnp.zeros_like(k.acc)
    k.gacc[...] = jnp.zeros_like(k.gacc)

    def q_step(i, carry):
        for c in late(i):
            c.wait()
        k.acc[...] += jnp.dot(k.tok[:, part(i)], k.qw[part(i), :], preferred_element_type=F32)
        k.gacc[...] += lax.dot_general(
            k.tok[:, part(i)], k.gw[:, part(i)], NT, preferred_element_type=F32
        )
        return carry

    lax.fori_loop(0, chunks, q_step, 0)
    travel.relay_x(0)
    wide_low = lax.broadcasted_iota(jnp.int32, k.gacc.shape, 1) < half_gates
    gates = jax.nn.sigmoid(k.gacc[...])
    gates_hi = gates.astype(BF16).astype(F32)
    gates = jnp.where(wide_low, gates_hi, gates - gates_hi).astype(BF16)
    spread_row = lax.broadcasted_iota(jnp.int32, (LANES, G * R * HD), 0)
    spread_col = lax.broadcasted_iota(jnp.int32, (LANES, G * R * HD), 1)
    spread_at = (tp * G * R + spread_col // HD) * 2
    for branch in range(2):
        spread = jnp.where(spread_row % half_gates == spread_at + branch, 1.0, 0.0).astype(BF16)
        k.gate[branch] = jnp.dot(gates, spread, preferred_element_type=F32)

    def query_step(b, carry):
        r0 = pl.ds(b * SB, SB)
        for g in range(G):
            for pair in range(R // 2):
                at = (g * R // 2 + pair) * LANES
                t = k.acc[r0, at : at + LANES].astype(BF16).astype(F32) * (HD ** -0.5)
                turned = pltpu.roll(t, HD, 1)
                e = 2 * pair * SB
                o = e + SB
                k.q[g, b, e : e + SB] = jnp.where(low, t, 0.0).astype(BF16)
                k.q[g, b, o : o + SB] = jnp.where(low, turned, 0.0).astype(BF16)
                k.q[g, b, R * SB + e : R * SB + e + SB] = jnp.where(low, 0.0, turned).astype(BF16)
                k.q[g, b, R * SB + o : R * SB + o + SB] = jnp.where(low, 0.0, t).astype(BF16)
        return carry

    lax.fori_loop(0, nb, query_step, 0)
    bias_copy.wait()
    for i in range(1, n):
        req_copy(i).wait_send()

        @pl.when(me + i < n)
        def _():
            sum_copy(i).wait_send()

        @pl.when(me - i >= 0)
        def _():
            sum_copy(i).wait_recv()
            both = k.sum_in[i].astype(F32)
            k.sum_key[i * slot : (i + 1) * slot] = both[:slot]
            k.sum_val[i * slot : (i + 1) * slot] = both[slot:]

    k.sum_keys[...] = k.sum_key[...].astype(BF16)
    k.sum_vals[...] = jnp.transpose(k.sum_val[...]).astype(BF16)
    span = lax.broadcasted_iota(jnp.int32, k.until.shape, 0)
    row = lax.broadcasted_iota(jnp.int32, k.until.shape, 1) % SB
    source, t = span // slot, span % slot
    k.until[...] = jnp.where(
        (t < spans) & (source <= me) & (source < n),
        (t - spans * source) * CMP + (CMP - 1) - row, 1 << 30,
    )

    def blocks_done():
        for i in range(1, n):

            @pl.when(me + i < n)
            def _():
                blk_copy(i).wait_send()

            @pl.when(me - i >= 0)
            def _():
                blk_copy(i).wait_recv()

    return blocks_done


def row8(x):
    return jnp.max(x.reshape(x.shape[0] // 8, 8, x.shape[1]), axis=0)


def sum8(x):
    return jnp.sum(x.reshape(x.shape[0] // 8, 8, x.shape[1]), axis=0)


def turn(outs):
    t = jnp.transpose(jnp.concatenate(outs, axis=0))
    turned = pltpu.roll(t, HD, 1)
    low = lax.broadcasted_iota(jnp.int32, (SB, LANES), 1) < HD
    tiles = []
    for first, second in ((t, turned), (turned, t)):
        for e in range(0, t.shape[0], 2 * SB):
            tiles.append(jnp.where(low, first[e : e + SB], second[e + SB : e + 2 * SB]))
    return tiles


def near(n, G, R, nb, k, blocks, b, carry):
    width = R * SB
    q = jnp.concatenate([k.q[g, b, g * width : (g + 1) * width] for g in range(G)], axis=0)
    keys = blocks * SB
    k.score[:keys] = lax.dot_general(k.keys[:keys], q, NT, preferred_element_type=F32)
    own = pl.ds(b * SB, SB)
    shape = (SB, G * width)
    later = lax.broadcasted_iota(jnp.int32, shape, 0) > lax.broadcasted_iota(jnp.int32, shape, 1) % SB
    k.score[own, :] += jnp.where(later, LOW, 0.0)

    def bias(j):
        return jnp.concatenate([jnp.full((8, width), k.bias_smem[g, b, j], F32) for g in range(G)], axis=1)

    top = None
    for j in range(blocks):
        t = row8(k.score[j * SB : (j + 1) * SB]) + bias(j)
        top = t if top is None else jnp.maximum(top, t)
    top = jnp.max(top, axis=0, keepdims=True)
    total = jnp.zeros((8, G * width), F32)
    weights = []
    for j in range(blocks):
        p = jnp.exp(k.score[j * SB : (j + 1) * SB] - (top - bias(j)[:1]))
        total = total + sum8(p)
        weights.append(p.astype(BF16))
    weights = jnp.concatenate(weights, axis=0)
    k.top[b] = jnp.broadcast_to(top, k.top.shape[1:])
    k.total[b] = total
    for g in range(G):
        cols = slice(g * width, (g + 1) * width)
        k.part[b, :, cols] = jnp.dot(
            k.vals[g * HD : (g + 1) * HD, :keys], weights[:, cols], preferred_element_type=F32
        )

    s = lax.dot_general(k.sum_keys[...], q, NT, preferred_element_type=F32)
    until = jnp.concatenate([k.until[...]] * (G * width // LANES), axis=1)
    s = jnp.where(until <= b * SB, s, LOW)
    top = jnp.max(row8(s), axis=0, keepdims=True)
    p = jnp.exp(s - top)
    total = jnp.sum(sum8(p), axis=0, keepdims=True)
    scale = jnp.where(top > LOW * 0.5, 1.0 / total, 0.0)
    p = p.astype(BF16)
    outs = []
    for g in range(G):
        cols = slice(g * width, (g + 1) * width)
        o = jnp.dot(k.sum_vals[g * HD : (g + 1) * HD, :], p[:, cols], preferred_element_type=F32)
        outs.append(o * scale[:, cols])
    for t, tile in enumerate(turn(outs)):
        cols = slice(t * LANES, (t + 1) * LANES)
        k.mixed[own, cols] = tile * k.gate[0, own, cols]
    return carry


def distant(n, G, R, nb, k, b):
    width = R * SB
    own = pl.ds(b * SB, SB)
    outs = []
    for g in range(G):
        cols = slice(g * width, (g + 1) * width)
        keys = k.far[:, g, :SB, :].reshape((n - 1) * SB, LANES)
        k.far_score[g] = lax.dot_general(keys, k.q[g, b], NT, preferred_element_type=F32)

        def bias(i, h):
            return k.bias_smem[g, b, nb + 2 * i + h]

        before = k.top[b, :1, cols]
        top = jnp.broadcast_to(before, (8, width))
        for i in range(n - 1):
            t = row8(k.far_score[g, i * SB : (i + 1) * SB])
            for h in range(2):
                top = jnp.maximum(top, t[:, h * width : (h + 1) * width] + bias(i, h))
        top = jnp.max(top, axis=0, keepdims=True)
        keep = jnp.exp(before - top)
        total = k.total[b, :, cols] * keep
        weights = []
        for i in range(n - 1):
            for h in range(2):
                s = k.far_score[g, i * SB : (i + 1) * SB, h * width : (h + 1) * width]
                p = jnp.exp(s - (top - bias(i, h)))
                total = total + sum8(p)
                weights.append(p.astype(BF16))
        weights = jnp.concatenate(weights, axis=0)
        vals = jnp.concatenate([k.far[i, g, SB:, :] for i in range(n - 1)], axis=1)
        o = k.part[b, :, cols] * keep + jnp.dot(vals, weights, preferred_element_type=F32)
        outs.append(o * (1.0 / jnp.sum(total, axis=0, keepdims=True)))
    for t, tile in enumerate(turn(outs)):
        cols = slice(t * LANES, (t + 1) * LANES)
        k.att[own, cols] = (k.mixed[own, cols] + tile * k.gate[1, own, cols]).astype(BF16)


def attend_and_mix(n, G, R, nb, cw, k, ow_loads, blocks_done, travel):
    tp = lax.axis_index("tp")
    core = lax.rem(tp, 2)
    side = tp // 2
    partner = side * 2 + 1 - core
    rows = nb * SB
    quarter = rows // 4
    half_blocks = nb // 2
    width = k.base.shape[1]
    chunks = width // cw
    side_cols = width // 2
    step_rows = SB // 2
    att, ow = k.att, k.ow

    few = (nb // 2 + 1) // 2 * 2

    def near_blocks(which):
        @pl.when(which == 0)
        def _():
            lax.fori_loop(0, half_blocks, functools.partial(near, n, G, R, nb, k, few), 0)

        @pl.when(which == 1)
        def _():
            lax.fori_loop(half_blocks, nb, functools.partial(near, n, G, R, nb, k, nb), 0)

    near_blocks(1 - side)
    for c in ow_loads:
        c.wait()
    travel.relay_x(1)
    blocks_done()

    def d_copy(j):
        return pltpu.make_async_remote_copy(
            src_ref=k.dsend.at[j], dst_ref=k.drecv.at[j],
            send_sem=k.d_s.at[j], recv_sem=k.d_r.at[j],
            device_id={"tp": partner}, device_id_type=MESH,
        )

    def e_copy(i):
        return pltpu.make_async_remote_copy(
            src_ref=k.esend.at[i], dst_ref=k.erecv.at[i],
            send_sem=k.e_s.at[i], recv_sem=k.e_r.at[i],
            device_id={"tp": partner}, device_id_type=MESH,
        )

    def x_copy(i):
        step = lax.rem(i, half_blocks)
        return pltpu.make_async_remote_copy(
            src_ref=k.xsend.at[i], dst_ref=k.xrecv.at[core, step],
            send_sem=k.x_s.at[i], recv_sem=k.x_r.at[core, step],
            device_id={"tp": (1 - side) * 2 + i // half_blocks}, device_id_type=MESH,
        )

    def x_arrival(c, step):
        return pltpu.make_async_remote_copy(
            src_ref=k.xsend.at[step], dst_ref=k.xrecv.at[c, step],
            send_sem=k.x_s.at[step], recv_sem=k.x_r.at[c, step],
            device_id={"tp": (1 - side) * 2 + core}, device_id_type=MESH,
        )

    other_first = (1 - side) * half_blocks

    def a_copy(i):
        to, step = i // half_blocks, lax.rem(i, half_blocks)
        rows_of = pl.ds(pl.multiple_of(other_first * SB + i * step_rows, step_rows), step_rows)
        into = pl.ds(pl.multiple_of(step * step_rows, step_rows), step_rows)
        return pltpu.make_async_remote_copy(
            src_ref=att.at[rows_of], dst_ref=k.att_in.at[1 + lax.rem(to + core, 2), into],
            send_sem=k.a_s.at[i], recv_sem=k.a_r.at[core, step],
            device_id={"tp": (1 - side) * 2 + to}, device_id_type=MESH,
        )

    def a_arrival(c, step):
        into = pl.ds(pl.multiple_of(step * step_rows, step_rows), step_rows)
        return pltpu.make_async_remote_copy(
            src_ref=att.at[into], dst_ref=k.att_in.at[1 + lax.rem(c + core, 2), into],
            send_sem=k.a_s.at[step], recv_sem=k.a_r.at[c, step],
            device_id={"tp": (1 - side) * 2 + core}, device_id_type=MESH,
        )

    def early_block(i):
        distant(n, G, R, nb, k, other_first + i)
        for h in range(2):
            a_copy(2 * i + h).start()
        a = att[pl.ds((other_first + i) * SB, SB), :]
        for j in range(side_cols // cw):
            cols = pl.ds(pl.multiple_of((1 - core) * side_cols + j * cw, cw), cw)
            k.esend[i, :, j * cw : (j + 1) * cw] = jnp.dot(
                a, ow[:, cols], preferred_element_type=F32
            ).astype(BF16)
        e_copy(i).start()
        for j in range(side_cols // cw):
            cols = pl.ds(pl.multiple_of(core * side_cols + j * cw, cw), cw)
            k.early[i, :, j * cw : (j + 1) * cw] = jnp.dot(
                a, ow[:, cols], preferred_element_type=F32
            ).astype(BF16)

    def forward(i):
        e_copy(i).wait_recv()
        for h in range(2):
            r = slice(h * step_rows, (h + 1) * step_rows)
            k.xsend[2 * i + h] = (k.early[i, r].astype(F32) + k.erecv[i, r].astype(F32)).astype(BF16)
            x_copy(2 * i + h).start()

    def early_step(i, carry):
        early_block(i)
        forward(i)
        for at, relay, j in ((0, travel.relay_x, 2), (1, travel.relay_y, 0), (2, travel.relay_x, 3), (3, travel.relay_y, 1)):

            @pl.when(i == min(at, half_blocks - 1))
            def _():
                relay(j)

        return carry

    lax.fori_loop(0, half_blocks, early_step, 0)

    own_first = side * half_blocks
    near_blocks(side)

    def own_att(b, carry):
        distant(n, G, R, nb, k, b)
        return carry

    lax.fori_loop(own_first, own_first + half_blocks, own_att, 0)
    theirs_at = pl.ds(pl.multiple_of(own_first * SB + (1 - core) * quarter, step_rows), quarter)
    ours_at = pl.ds(pl.multiple_of(own_first * SB + core * quarter, step_rows), quarter)
    p_copy = pltpu.make_async_remote_copy(
        src_ref=att.at[theirs_at], dst_ref=k.att_in.at[0], send_sem=k.p_s, recv_sem=k.p_r,
        device_id={"tp": partner}, device_id_type=MESH,
    )
    p_copy.start()
    travel.relay_y(2)

    def own_step(j, carry):
        w = ow[:, pl.ds(pl.multiple_of(j * cw, cw), cw)]
        theirs = att[theirs_at, :]
        k.dsend[j] = jnp.dot(theirs, w, preferred_element_type=F32).astype(BF16)
        d_copy(j).start()
        ours = att[ours_at, :]
        k.mine[j] = jnp.dot(ours, w, preferred_element_type=F32).astype(BF16)
        return carry

    lax.fori_loop(0, chunks, own_step, 0)

    travel.relay_y(3)
    travel.arrived()
    p_copy.wait_recv()
    for c in range(2):
        for step in range(half_blocks):
            a_arrival(c, step).wait_recv()

    def wide_step(j, carry):
        cols = pl.ds(pl.multiple_of(j * cw, cw), cw)
        out_cols = pl.ds(pl.multiple_of(travel.first + j * cw, cw), cw)
        o = jnp.dot(att[ours_at, :], ow[:, out_cols], preferred_element_type=F32)
        for slot in range(3):
            o = o + jnp.dot(k.att_in[slot], k.wfar[slot, :, cols], preferred_element_type=F32)
        k.out[:, out_cols] = o.astype(BF16)
        return carry

    lax.fori_loop(0, travel.columns // cw, wide_step, 0)
    def base_step(j, carry):
        d_copy(j).wait_recv()
        cols = pl.ds(pl.multiple_of(j * cw, cw), cw)
        k.base[:, cols] = k.mine[j].astype(F32) + k.drecv[j].astype(F32)
        d_copy(j).wait_send()
        return carry

    lax.fori_loop(0, chunks, base_step, 0)

    def last_step(s, carry):
        r = pl.ds(pl.multiple_of(s * step_rows, step_rows), step_rows)
        for c in range(2):
            x_arrival(c, s).wait_recv()
            cols = slice(c * side_cols, (c + 1) * side_cols)
            k.out[r, cols] = (k.base[r, cols] + k.xrecv[c, s].astype(F32)).astype(BF16)
        e_copy(s).wait_send()
        x_copy(s).wait_send()
        x_copy(half_blocks + s).wait_send()
        a_copy(s).wait_send()
        a_copy(half_blocks + s).wait_send()
        return carry

    lax.fori_loop(0, half_blocks, last_step, 0)
    p_copy.wait_send()
    travel.sent()


def layer_kernel(n, G, R, nb, kc, cw, names, *refs):
    k = types.SimpleNamespace(**dict(zip(names, refs, strict=True)))
    ow_loads = [pltpu.make_async_copy(k.ow_hbm, k.ow, k.sem_ow)]
    travel = Travel(k, PIECES)
    blocks_done = project(n, G, R, nb, kc, k, ow_loads, travel)
    attend_and_mix(n, G, R, nb, cw, k, ow_loads, blocks_done, travel)


def local(
    n,
    tokens, query_weight, key_weight, value_weight, gate_weight,
    summary_pos, key_mixing, value_mixing, out_weight, chosen,
):
    rows, depth = tokens.shape
    heads = query_weight.shape[1] // HD
    G = key_weight.shape[1] // HD
    R = heads // G
    nb = rows // SB
    spans = rows // CMP
    slot = -(-spans // 8) * 8
    all_spans = -(-n * slot // LANES) * LANES
    kc = min(1024, depth)
    chunks = depth // kc
    width = out_weight.shape[1]
    cw = 512
    wide = width // 2
    summed = width - wide
    oc = summed // cw
    gates_all = gate_weight.shape[1]
    assert G == 2 and n % 2 == 0 and 2 * gates_all == LANES and nb % 2 == 0

    vmem = pl.BlockSpec(memory_space=pltpu.VMEM)
    hbm = pl.BlockSpec(memory_space=pl.ANY)
    dma = pltpu.SemaphoreType.DMA
    V = pltpu.VMEM
    nbp = -(-nb // 8) * 8
    quarter = rows // 4
    half = nb // 2
    inputs = ["tok_hbm", "qw_hbm", "kw_hbm", "vw_hbm", "gw_hbm", "chosen", "km", "vm", "pos", "ow_hbm"]
    scratch = {
        "q": V((G, nb, 2 * R * SB, LANES), BF16),
        "tok": V((rows, depth), BF16),
        "qw": V((depth, heads * HD), BF16),
        "kvw": V((depth, 2 * LANES), BF16),
        "gw": V((LANES, depth), BF16),
        "ow": V(out_weight.shape, BF16),
        "acc": V((rows, heads * HD), F32),
        "gacc": V((rows, LANES), F32),
        "gate": V((2, rows, heads * HD), F32),
        "keys": V((rows, LANES), BF16),
        "vals": V((LANES, rows), BF16),
        "left": V((G * nb, 2 * SB, LANES), BF16),
        "right": V((G * nb, 2 * SB, LANES), BF16),
        "named": V((G, nbp, LANES), jnp.int32),
        "bias": V((G, nbp, LANES), F32),
        "bias_smem": pltpu.SMEM((G, nbp, LANES), F32),
        "pos_wide": V((CMP, LANES), F32),
        "req": V((n, 8, LANES), jnp.int32),
        "req_in": V((n, 8, LANES), jnp.int32),
        "req_smem": pltpu.SMEM((n, 8, LANES), jnp.int32),
        "send": V((n, G, 2 * SB, LANES), BF16),
        "far": V((n - 1, G, 2 * SB, LANES), BF16),
        "sum_send": V((2 * slot, LANES), BF16),
        "sum_in": V((n, 2 * slot, LANES), BF16),
        "sum_key": V((all_spans, LANES), F32),
        "sum_val": V((all_spans, LANES), F32),
        "sum_keys": V((all_spans, LANES), BF16),
        "sum_vals": V((LANES, all_spans), BF16),
        "until": V((all_spans, LANES), jnp.int32),
        "score": V((rows, heads * HD), F32),
        "far_score": V((G, (n - 1) * SB, 2 * R * SB), F32),
        "top": V((nb, 8, heads * HD), F32),
        "total": V((nb, 8, heads * HD), F32),
        "part": V((nb, HD, heads * HD), F32),
        "mixed": V((rows, heads * HD), F32),
        "att": V((rows, heads * HD), BF16),
        "mine": V((oc, quarter, cw), BF16),
        "dsend": V((oc, quarter, cw), BF16),
        "drecv": V((oc, quarter, cw), BF16),
        "early": V((half, SB, summed // 2), BF16),
        "esend": V((half, SB, summed // 2), BF16),
        "erecv": V((half, SB, summed // 2), BF16),
        "xsend": V((2 * half, SB // 2, summed // 2), BF16),
        "xrecv": V((2, half, SB // 2, summed // 2), BF16),
        "base": V((quarter, summed), F32),
        "wfar": V((3, out_weight.shape[0], wide), BF16),
        "att_in": V((3, quarter, heads * HD), BF16),
        "sem_ow": dma,
        "sem_bias": dma,
        "sem_req": dma((n,)),
        "sem_tok": dma((chunks,)), "sem_kw": dma((chunks,)), "sem_vw": dma((chunks,)),
        "sem_qw": dma((chunks,)), "sem_gw": dma((2, chunks)),
        "req_s": dma((n,)), "req_r": dma((n,)), "blk_s": dma((n,)), "blk_r": dma((n,)),
        "sum_s": dma((n,)), "sum_r": dma((n,)),
        "d_s": dma((oc,)), "d_r": dma((oc,)), "e_s": dma((half,)), "e_r": dma((half,)),
        "x_s": dma((2 * half,)), "x_r": dma((2, half)),
        "a_s": dma((2 * half,)), "a_r": dma((2, half)), "p_s": dma, "p_r": dma,
        "wx_s": dma((PIECES,)), "wx_r": dma((PIECES,)), "wp_s": dma, "wp_r": dma,
        "wy_s": dma((PIECES,)), "wy_r": dma((PIECES,)),
        "wd_s": dma((2, PIECES)), "wd_r": dma((2, PIECES)),
    }
    return pl.pallas_call(
        functools.partial(layer_kernel, n, G, R, nb, kc, cw, inputs + ["out"] + list(scratch)),
        name="layer",
        out_shape=pltpu.VMEM((quarter, width), BF16),
        in_specs=[hbm] * 5 + [vmem] * 4 + [hbm],
        out_specs=vmem,
        scratch_shapes=list(scratch.values()),
        compiler_params=pltpu.CompilerParams(
            collective_id=1, has_side_effects=True, vmem_limit_bytes=VMEM_LIMIT
        ),
    )(
        tokens, query_weight, key_weight, value_weight, gate_weight.T,
        chosen, key_mixing.T, value_mixing.T, summary_pos, out_weight,
    )


def solution(mesh):
    placed = (
        P("kv", None),
        P(None, "tp"),
        P(None, "tp"),
        P(None, "tp"),
        P(),
        P(),
        P(),
        P(),
        P("tp", None),
        P("kv", "tp", None),
    )
    return jax.shard_map(
        functools.partial(local, mesh.shape["kv"]),
        mesh=mesh, in_specs=placed, out_specs=P(("kv", "tp"), None), check_vma=False,
    )
```

```python
import functools
import types

import jax
import jax.numpy as jnp
from jax import lax
from jax.experimental import pallas as pl
from jax.experimental.pallas import tpu as pltpu
from jax.sharding import PartitionSpec as P

HD = 64
CMP = 32
SB = 64
N_SEL = 16
LANES = 128
PIECES = 4
LOW = -1e30
F32 = jnp.float32
BF16 = jnp.bfloat16
MESH = pl.DeviceIdType.MESH
VMEM_LIMIT = 64_000_000
NT = (((1,), (1,)), ((), ()))


def requests(n, G, nb, k):
    place = lax.broadcasted_iota(jnp.int32, k.named.shape, 1)
    for g in range(G):
        k.named[g] = jnp.full(k.named.shape[1:], -1, jnp.int32)
        k.named[g, :nb, :N_SEL] = k.chosen[:, g, :]
        c = k.named[g]
        source = jnp.zeros_like(c)
        for s in range(1, n):
            source = source + jnp.where(c >= s * nb, 1, 0)
        inside = c - source * nb
        for s in range(n):
            hit = (c >= 0) & (source == s)
            lo = jnp.where(hit, inside, nb)
            lo = jnp.min(jnp.min(lo, axis=0, keepdims=True), axis=1, keepdims=True)
            lo = jnp.where(lo == nb, 0, lo)
            hi = jnp.where(hit, inside, 0)
            hi = jnp.max(jnp.max(hi, axis=0, keepdims=True), axis=1, keepdims=True)
            k.req[s, 2 * g : 2 * g + 1] = jnp.broadcast_to(lo, (1, LANES))
            k.req[s, 2 * g + 1 : 2 * g + 2] = jnp.broadcast_to(hi, (1, LANES))


def biases(n, G, nb, k, me):
    for g in range(G):
        c = k.named[g]
        lane = lax.broadcasted_iota(jnp.int32, c.shape, 1)
        bias = jnp.full(c.shape, LOW, F32)

        def mark(bias, hit, at):
            hit = jnp.max(jnp.where(hit, 1.0, 0.0), axis=1, keepdims=True)
            return jnp.where((lane == at) & (hit > 0.0), 0.0, bias)

        for j in range(nb):
            bias = mark(bias, c == me * nb + j, j)
        for s in range(n - 1):
            lo = k.req[s, 2 * g : 2 * g + 1]
            hi = k.req[s, 2 * g + 1 : 2 * g + 2]
            at = jnp.where(me > s, nb + 2 * (me - s - 1), -5)
            real = c >= 0
            bias = mark(bias, real & (c == s * nb + lo), at)
            bias = mark(bias, real & (c == s * nb + hi) & (hi != lo), at + 1)
        k.bias[g] = bias


class Travel:
    def __init__(self, k, pieces):
        tp, me = lax.axis_index("tp"), lax.axis_index("kv")
        core, side = lax.rem(tp, 2), tp // 2
        self.k, self.pieces = k, pieces
        self.across = {"tp": (1 - side) * 2 + core}
        self.partner = {"tp": side * 2 + 1 - core}
        self.beside = {"kv": me + 1 - 2 * lax.rem(me, 2)}
        self.mine = lax.rem(me, 2)
        self.columns = k.wfar.shape[2]
        self.first = k.ow.shape[1] - self.columns
        self.size = self.columns // 2 // pieces

    def cols(self, half, j, base=0):
        at = base + half * (self.columns // 2) + j * self.size
        return pl.ds(pl.multiple_of(at, LANES), self.size)

    def copy(self, src, dst, send, recv, target):
        return pltpu.make_async_remote_copy(
            src_ref=src, dst_ref=dst, send_sem=send, recv_sem=recv,
            device_id=target, device_id_type=MESH,
        )

    def x(self, j):
        k = self.k
        return self.copy(
            k.ow_hbm.at[:, self.cols(self.mine, j, self.first)], k.wfar.at[1, :, self.cols(self.mine, j)],
            k.wx_s.at[j], k.wx_r.at[j], self.across,
        )

    def p(self):
        k = self.k
        return self.copy(
            k.ow_hbm.at[:, pl.ds(self.first, self.columns)], k.wfar.at[0], k.wp_s, k.wp_r, self.partner
        )

    def y(self, j):
        here = self.k.wfar.at[1, :, self.cols(self.mine, j)]
        return self.copy(here, here, self.k.wy_s.at[j], self.k.wy_r.at[j], self.beside)

    def y_arrival(self, j):
        here = self.k.wfar.at[1, :, self.cols(1 - self.mine, j)]
        return self.copy(here, here, self.k.wy_s.at[j], self.k.wy_r.at[j], self.beside)

    def d(self, h, j):
        k = self.k
        at = self.cols(self.mine if h == 0 else 1 - self.mine, j)
        return self.copy(
            k.wfar.at[1, :, at], k.wfar.at[2, :, at], k.wd_s.at[h, j], k.wd_r.at[h, j], self.partner
        )

    def start(self):
        for j in range(self.pieces):
            self.x(j).start()
        self.p().start()

    def relay_x(self, j):
        self.x(j).wait_recv()
        self.y(j).start()
        self.d(0, j).start()

    def relay_y(self, j):
        self.y_arrival(j).wait_recv()
        self.d(1, j).start()

    def arrived(self):
        self.p().wait_recv()
        for h in range(2):
            for j in range(self.pieces):
                self.d(h, j).wait_recv()

    def sent(self):
        self.p().wait_send()
        for j in range(self.pieces):
            self.x(j).wait_send()
            self.y(j).wait_send()
            for h in range(2):
                self.d(h, j).wait_send()


def project(n, G, R, nb, kc, k, ow_loads, travel):
    tp = lax.axis_index("tp")
    me = lax.axis_index("kv")
    rows = nb * SB
    depth = k.tok.shape[1]
    chunks = depth // kc
    spans = rows // CMP
    slot = k.sum_send.shape[0] // 2

    def part(i):
        return pl.ds(i * kc, kc)

    def loads(i):
        return [
            pltpu.make_async_copy(k.tok_hbm.at[:, part(i)], k.tok.at[:, part(i)], k.sem_tok.at[i]),
            pltpu.make_async_copy(k.kw_hbm.at[part(i)], k.kvw.at[part(i), pl.ds(0, LANES)], k.sem_kw.at[i]),
            pltpu.make_async_copy(k.vw_hbm.at[part(i)], k.kvw.at[part(i), pl.ds(LANES, LANES)], k.sem_vw.at[i]),
        ]

    half_gates = k.gw.shape[0] // 2

    def late(i):
        return [
            pltpu.make_async_copy(k.qw_hbm.at[part(i)], k.qw.at[part(i)], k.sem_qw.at[i]),
            pltpu.make_async_copy(k.gw_hbm.at[:, part(i)], k.gw.at[pl.ds(0, half_gates), part(i)], k.sem_gw.at[0, i]),
            pltpu.make_async_copy(k.gw_hbm.at[:, part(i)], k.gw.at[pl.ds(half_gates, half_gates), part(i)], k.sem_gw.at[1, i]),
        ]

    for i in range(chunks):
        for c in loads(i):
            c.start()

    barrier = pltpu.get_barrier_semaphore()
    for i in range(1, n):
        pl.semaphore_signal(
            barrier, inc=1, device_id={"kv": lax.rem(me + i, n)}, device_id_type=MESH
        )
    for i in range(1, 4):
        pl.semaphore_signal(barrier, inc=1, device_id={"tp": lax.rem(tp + i, 4)}, device_id_type=MESH)

    requests(n, G, nb, k)
    pl.semaphore_wait(barrier, n + 2)

    def req_copy(i):
        return pltpu.make_async_remote_copy(
            src_ref=k.req.at[lax.rem(me + n - i, n)], dst_ref=k.req_in.at[i],
            send_sem=k.req_s.at[i], recv_sem=k.req_r.at[i],
            device_id={"kv": lax.rem(me + n - i, n)}, device_id_type=MESH,
        )

    def req_local(i):
        return pltpu.make_async_copy(k.req_in.at[i], k.req_smem.at[i], k.sem_req.at[i])

    def blk_copy(i):
        return pltpu.make_async_remote_copy(
            src_ref=k.send.at[i], dst_ref=k.far.at[i - 1],
            send_sem=k.blk_s.at[i], recv_sem=k.blk_r.at[i],
            device_id={"kv": lax.rem(me + i, n)}, device_id_type=MESH,
        )

    def sum_copy(i):
        return pltpu.make_async_remote_copy(
            src_ref=k.sum_send, dst_ref=k.sum_in.at[i],
            send_sem=k.sum_s.at[i], recv_sem=k.sum_r.at[i],
            device_id={"kv": lax.rem(me + i, n)}, device_id_type=MESH,
        )

    for i in range(1, n):
        req_copy(i).start()
    travel.start()

    biases(n, G, nb, k, me)
    bias_copy = pltpu.make_async_copy(k.bias, k.bias_smem, k.sem_bias)
    bias_copy.start()
    for i in range(1, n):

        @pl.when(me < i)
        def _():
            k.far[i - 1] = jnp.zeros(k.far.shape[1:], BF16)

    k.q_near[...] = jnp.zeros_like(k.q_near)
    k.q_far[...] = jnp.zeros_like(k.q_far)
    k.sum_key[...] = jnp.zeros_like(k.sum_key)
    k.sum_val[...] = jnp.zeros_like(k.sum_val)
    k.acc[:, : 2 * LANES] = jnp.zeros((rows, 2 * LANES), F32)

    def kv_step(i, carry):
        for c in loads(i):
            c.wait()
        for c in late(i):
            c.start()
        k.acc[:, : 2 * LANES] += jnp.dot(k.tok[:, part(i)], k.kvw[part(i), :], preferred_element_type=F32)
        return carry

    lax.fori_loop(0, chunks, kv_step, 0)
    for c in ow_loads:
        c.start()
    low = lax.broadcasted_iota(jnp.int32, (SB, LANES), 1) < HD
    mix_row = lax.broadcasted_iota(jnp.int32, k.km.shape, 0)
    mix_low = lax.broadcasted_iota(jnp.int32, (CMP, LANES), 1) < HD
    diagonal = lax.broadcasted_iota(jnp.int32, (CMP, CMP), 0) == lax.broadcasted_iota(
        jnp.int32, (CMP, CMP), 1
    )

    def mix_column(ref, head):
        line = jnp.where(mix_row == head, ref[...].astype(F32), 0.0)
        line = jnp.sum(line, axis=0, keepdims=True)
        return jnp.sum(jnp.where(diagonal, line, 0.0), axis=1, keepdims=True)

    k.pos_wide[:, :HD] = k.pos[...].astype(F32)
    k.pos_wide[:, HD:] = k.pos[...].astype(F32)
    both = []
    for ref, at, more in ((k.km, 0, 1.0), (k.vm, LANES, 0.0)):
        mix = jnp.where(mix_low, mix_column(ref, tp * G), mix_column(ref, tp * G + 1))
        t = k.acc[:, at : at + LANES].astype(BF16).astype(F32).reshape(spans, CMP, LANES)
        s = jnp.sum((t + k.pos_wide[...][None]) * mix[None], axis=1)
        if slot > spans:
            s = jnp.concatenate([s, s[: slot - spans] * more], axis=0)
        both.append(s)
    both = jnp.concatenate(both, axis=0).astype(BF16)
    k.sum_send[...] = both
    k.sum_key[:slot] = both.astype(F32)[:slot]
    k.sum_val[:slot] = both.astype(F32)[slot:]
    for i in range(1, n):

        @pl.when(me + i < n)
        def _():
            sum_copy(i).start()

    for t in range(nb // 2):
        r0 = slice(t * LANES, (t + 1) * LANES)
        keys = k.acc[r0, :LANES].astype(BF16).astype(F32)
        vals = jnp.transpose(k.acc[r0, LANES : 2 * LANES].astype(BF16).astype(F32))
        k.keys[r0, :] = keys.astype(BF16)
        k.vals[:, r0] = vals.astype(BF16)
        keys_r = pltpu.roll(keys, HD, 1)
        vals_r = pltpu.roll(vals, HD, 1)
        for h in range(2):
            kk, kr = keys[h * SB : (h + 1) * SB], keys_r[h * SB : (h + 1) * SB]
            v_left, v_right = (vals, vals_r) if h == 0 else (vals_r, vals)
            for g in range(G):
                left, right = (kk, kr) if g == 0 else (kr, kk)
                v = slice(g * HD, (g + 1) * HD)
                c = g * nb + 2 * t + h
                k.left[c, :SB] = jnp.where(low, left, 0.0).astype(BF16)
                k.left[c, SB:] = jnp.where(low, v_left[v], 0.0).astype(BF16)
                k.right[c, :SB] = jnp.where(low, 0.0, right).astype(BF16)
                k.right[c, SB:] = jnp.where(low, 0.0, v_right[v]).astype(BF16)
    first = range(1, min(4, n))
    for i in first:
        req_copy(i).wait_recv()
        req_local(i).start()
    def answer(i):
        req_local(i).wait()

        @pl.when(me + i < n)
        def _():
            for g in range(G):
                lo = k.req_smem[i, 2 * g, 0]
                hi = k.req_smem[i, 2 * g + 1, 0]
                k.send[i, g] = k.left[g * nb + lo] + k.right[g * nb + hi]
            blk_copy(i).start()

    for i in reversed(first):
        answer(i)
    k.acc[...] = jnp.zeros_like(k.acc)
    k.gacc[...] = jnp.zeros_like(k.gacc)

    def q_step(i, carry):
        for c in late(i):
            c.wait()
        k.acc[...] += jnp.dot(k.tok[:, part(i)], k.qw[part(i), :], preferred_element_type=F32)
        k.gacc[...] += lax.dot_general(
            k.tok[:, part(i)], k.gw[:, part(i)], NT, preferred_element_type=F32
        )
        return carry

    q_step(0, 0)
    for i in range(len(first) + 1, n):
        req_copy(i).wait_recv()
        req_local(i).start()
    for i in range(n - 1, len(first), -1):
        answer(i)
    lax.fori_loop(1, chunks, q_step, 0)
    travel.relay_x(0)
    wide_low = lax.broadcasted_iota(jnp.int32, k.gacc.shape, 1) < half_gates
    gates = jax.nn.sigmoid(k.gacc[...])
    gates_hi = gates.astype(BF16).astype(F32)
    gates = jnp.where(wide_low, gates_hi, gates - gates_hi).astype(BF16)
    spread_row = lax.broadcasted_iota(jnp.int32, (LANES, G * R * HD), 0)
    spread_col = lax.broadcasted_iota(jnp.int32, (LANES, G * R * HD), 1)
    spread_at = (tp * G * R + spread_col // HD) * 2
    for branch in range(2):
        spread = jnp.where(spread_row % half_gates == spread_at + branch, 1.0, 0.0).astype(BF16)
        k.gate[branch] = jnp.dot(gates, spread, preferred_element_type=F32)

    tall_low = lax.broadcasted_iota(jnp.int32, (HD, LANES), 1) < SB

    def query_step(t, carry):
        r0 = pl.ds(pl.multiple_of(t * LANES, LANES), LANES)
        for g in range(G):
            for pair in range(R // 2):
                at = (g * R // 2 + pair) * LANES
                x = jnp.transpose(k.acc[r0, at : at + LANES].astype(BF16).astype(F32) * (HD ** -0.5))
                turned = pltpu.roll(x, SB, 1)
                for h, (left, right) in enumerate(((x, turned), (turned, x))):
                    y = jnp.where(tall_low, left[:HD], right[HD:]).astype(BF16)
                    lo = slice(pair * LANES, (pair + 1) * LANES)
                    hi = slice(R * SB + pair * LANES, R * SB + (pair + 1) * LANES)
                    k.q_near[2 * t + h, g * HD : (g + 1) * HD, g * R * SB + pair * LANES : g * R * SB + (pair + 1) * LANES] = y
                    k.q_far[g, 2 * t + h, :HD, lo] = y
                    k.q_far[g, 2 * t + h, HD:, hi] = y
        return carry

    lax.fori_loop(0, nb // 2, query_step, 0)
    bias_copy.wait()
    for i in range(1, n):
        req_copy(i).wait_send()

        @pl.when(me + i < n)
        def _():
            sum_copy(i).wait_send()

        @pl.when(me - i >= 0)
        def _():
            sum_copy(i).wait_recv()
            both = k.sum_in[i].astype(F32)
            k.sum_key[i * slot : (i + 1) * slot] = both[:slot]
            k.sum_val[i * slot : (i + 1) * slot] = both[slot:]

    k.sum_keys[...] = k.sum_key[...].astype(BF16)
    k.sum_vals[...] = jnp.transpose(k.sum_val[...]).astype(BF16)
    def blocks_done():
        for i in range(1, n):

            @pl.when(me + i < n)
            def _():
                blk_copy(i).wait_send()

            @pl.when(me - i >= 0)
            def _():
                blk_copy(i).wait_recv()

    return blocks_done


def row8(x):
    return jnp.max(x.reshape(x.shape[0] // 8, 8, x.shape[1]), axis=0)


def sum8(x):
    return jnp.sum(x.reshape(x.shape[0] // 8, 8, x.shape[1]), axis=0)


def turn(outs):
    t = jnp.transpose(jnp.concatenate(outs, axis=0))
    turned = pltpu.roll(t, HD, 1)
    low = lax.broadcasted_iota(jnp.int32, (SB, LANES), 1) < HD
    tiles = []
    for first, second in ((t, turned), (turned, t)):
        for e in range(0, t.shape[0], 2 * SB):
            tiles.append(jnp.where(low, first[e : e + SB], second[e + SB : e + 2 * SB]))
    return tiles


def near_scores(n, k, b):
    own = (b + 1) * SB
    count = n * k.sum_send.shape[0] // 2
    keys = jnp.concatenate([k.keys[:own], k.sum_keys[:count]], axis=0)
    k.score[b % 2, : own + count] = jnp.dot(keys, k.q_near[b], preferred_element_type=F32)


def near(n, G, R, nb, k, b):
    me = lax.axis_index("kv")
    width = R * SB
    score = k.score.at[b % 2]
    rows = slice(b * SB, (b + 1) * SB)
    shape = (SB, G * width)
    later = lax.broadcasted_iota(jnp.int32, shape, 0) > lax.broadcasted_iota(jnp.int32, shape, 1) % SB

    def bias(j):
        return jnp.concatenate([jnp.full((8, width), k.bias_smem[g, b, j], F32) for g in range(G)], axis=1)

    def block(j):
        s = score[j * SB : (j + 1) * SB]
        return s + jnp.where(later, LOW, 0.0) if j == b else s

    top = None
    for j in range(b + 1):
        t = row8(block(j)) + bias(j)
        top = t if top is None else jnp.maximum(top, t)
    top = jnp.max(top, axis=0, keepdims=True)
    total = jnp.zeros((8, G * width), F32)
    weights = []
    for j in range(b + 1):
        p = jnp.exp(block(j) - (top - bias(j)[:1]))
        total = total + sum8(p)
        weights.append(p.astype(BF16))
    if b % 2 == 0:
        weights.append(jnp.zeros(shape, BF16))
    keys = len(weights) * SB
    weights = jnp.concatenate(weights, axis=0)
    k.top[b] = jnp.broadcast_to(top, k.top.shape[1:])
    k.total[b] = total
    for g in range(G):
        cols = slice(g * width, (g + 1) * width)
        k.part[b, :, cols] = jnp.dot(
            k.vals[g * HD : (g + 1) * HD, :keys], weights[:, cols], preferred_element_type=F32
        )

    slot = k.sum_send.shape[0] // 2
    spans = nb * SB // CMP
    base = (b + 1) * SB
    seen_shape = (slot, G * width)
    span = lax.broadcasted_iota(jnp.int32, seen_shape, 0)
    seen = (span < spans) & (
        span * CMP + (CMP - 1) <= b * SB + lax.broadcasted_iota(jnp.int32, seen_shape, 1) % SB
    )

    def summary(i):
        s = score[base + i * slot : base + (i + 1) * slot]
        return jnp.where(seen, s, LOW) if i == 0 else s

    def gone(i):
        return jnp.where(me >= i, 0.0, LOW).astype(F32)

    top = row8(summary(0))
    for i in range(1, n):
        top = jnp.maximum(top, row8(summary(i)) + gone(i))
    top = jnp.max(top, axis=0, keepdims=True)
    total = jnp.zeros((8, G * width), F32)
    real = spans - spans // 8 * 8
    partial = lax.broadcasted_iota(jnp.int32, (8, G * width), 0) < real
    weights = []
    for i in range(n):
        p = jnp.exp(summary(i) - (top - gone(i)))
        total = total + sum8(p[: spans // 8 * 8])
        if real:
            total = total + jnp.where(partial, p[spans // 8 * 8 :], 0.0)
        weights.append(p)
    more = k.sum_vals.shape[1] - n * slot
    if more:
        weights.append(jnp.zeros((more, G * width), F32))
    weights = jnp.concatenate(weights, axis=0).astype(BF16)
    total = jnp.sum(total, axis=0, keepdims=True)
    scale = jnp.where(top > LOW * 0.5, 1.0 / total, 0.0)
    outs = []
    for g in range(G):
        cols = slice(g * width, (g + 1) * width)
        o = jnp.dot(k.sum_vals[g * HD : (g + 1) * HD, :], weights[:, cols], preferred_element_type=F32)
        outs.append(o * scale[:, cols])
    for t, tile in enumerate(turn(outs)):
        cols = slice(t * LANES, (t + 1) * LANES)
        k.mixed[rows, cols] = tile * k.gate[0, rows, cols]


def distant(n, G, R, nb, k, b):
    width = R * SB
    own = pl.ds(b * SB, SB)
    outs = []
    for g in range(G):
        cols = slice(g * width, (g + 1) * width)
        keys = k.far[:, g, :SB, :].reshape((n - 1) * SB, LANES)
        k.far_score[g] = jnp.dot(keys, k.q_far[g, b], preferred_element_type=F32)

        def bias(i, h):
            return k.bias_smem[g, b, nb + 2 * i + h]

        before = k.top[b, :1, cols]
        top = jnp.broadcast_to(before, (8, width))
        for i in range(n - 1):
            t = row8(k.far_score[g, i * SB : (i + 1) * SB])
            for h in range(2):
                top = jnp.maximum(top, t[:, h * width : (h + 1) * width] + bias(i, h))
        top = jnp.max(top, axis=0, keepdims=True)
        keep = jnp.exp(before - top)
        total = k.total[b, :, cols] * keep
        weights = []
        for i in range(n - 1):
            for h in range(2):
                s = k.far_score[g, i * SB : (i + 1) * SB, h * width : (h + 1) * width]
                p = jnp.exp(s - (top - bias(i, h)))
                total = total + sum8(p)
                weights.append(p.astype(BF16))
        weights = jnp.concatenate(weights, axis=0)
        vals = jnp.concatenate([k.far[i, g, SB:, :] for i in range(n - 1)], axis=1)
        o = k.part[b, :, cols] * keep + jnp.dot(vals, weights, preferred_element_type=F32)
        outs.append(o * (1.0 / jnp.sum(total, axis=0, keepdims=True)))
    for t, tile in enumerate(turn(outs)):
        cols = slice(t * LANES, (t + 1) * LANES)
        k.att[own, cols] = (k.mixed[own, cols] + tile * k.gate[1, own, cols]).astype(BF16)


def attend_and_mix(n, G, R, nb, cw, k, ow_loads, blocks_done, travel):
    tp = lax.axis_index("tp")
    core = lax.rem(tp, 2)
    side = tp // 2
    partner = side * 2 + 1 - core
    rows = nb * SB
    quarter = rows // 4
    half_blocks = nb // 2
    width = k.base.shape[1]
    chunks = width // cw
    side_cols = width // 2
    step_rows = SB // 2
    att, ow = k.att, k.ow

    near_scores(n, k, 0)
    for b in range(nb):
        if b + 1 < nb:
            near_scores(n, k, b + 1)
        near(n, G, R, nb, k, b)
    for c in ow_loads:
        c.wait()
    travel.relay_x(1)
    blocks_done()

    def d_copy(j):
        return pltpu.make_async_remote_copy(
            src_ref=k.dsend.at[j], dst_ref=k.drecv.at[j],
            send_sem=k.d_s.at[j], recv_sem=k.d_r.at[j],
            device_id={"tp": partner}, device_id_type=MESH,
        )

    def e_copy(i):
        return pltpu.make_async_remote_copy(
            src_ref=k.esend.at[i], dst_ref=k.erecv.at[i],
            send_sem=k.e_s.at[i], recv_sem=k.e_r.at[i],
            device_id={"tp": partner}, device_id_type=MESH,
        )

    def x_copy(i):
        step = lax.rem(i, half_blocks)
        return pltpu.make_async_remote_copy(
            src_ref=k.xsend.at[i], dst_ref=k.xrecv.at[core, step],
            send_sem=k.x_s.at[i], recv_sem=k.x_r.at[core, step],
            device_id={"tp": (1 - side) * 2 + i // half_blocks}, device_id_type=MESH,
        )

    def x_arrival(c, step):
        return pltpu.make_async_remote_copy(
            src_ref=k.xsend.at[step], dst_ref=k.xrecv.at[c, step],
            send_sem=k.x_s.at[step], recv_sem=k.x_r.at[c, step],
            device_id={"tp": (1 - side) * 2 + core}, device_id_type=MESH,
        )

    other_first = (1 - side) * half_blocks

    def a_copy(i):
        to, step = i // half_blocks, lax.rem(i, half_blocks)
        rows_of = pl.ds(pl.multiple_of(other_first * SB + i * step_rows, step_rows), step_rows)
        into = pl.ds(pl.multiple_of(step * step_rows, step_rows), step_rows)
        return pltpu.make_async_remote_copy(
            src_ref=att.at[rows_of], dst_ref=k.att_in.at[1 + lax.rem(to + core, 2), into],
            send_sem=k.a_s.at[i], recv_sem=k.a_r.at[core, step],
            device_id={"tp": (1 - side) * 2 + to}, device_id_type=MESH,
        )

    def a_arrival(c, step):
        into = pl.ds(pl.multiple_of(step * step_rows, step_rows), step_rows)
        return pltpu.make_async_remote_copy(
            src_ref=att.at[into], dst_ref=k.att_in.at[1 + lax.rem(c + core, 2), into],
            send_sem=k.a_s.at[step], recv_sem=k.a_r.at[c, step],
            device_id={"tp": (1 - side) * 2 + core}, device_id_type=MESH,
        )

    def early_block(i):
        distant(n, G, R, nb, k, other_first + i)
        for h in range(2):
            a_copy(2 * i + h).start()
        a = att[pl.ds((other_first + i) * SB, SB), :]
        for j in range(side_cols // cw):
            cols = pl.ds(pl.multiple_of((1 - core) * side_cols + j * cw, cw), cw)
            k.esend[i, :, j * cw : (j + 1) * cw] = jnp.dot(
                a, ow[:, cols], preferred_element_type=F32
            ).astype(BF16)
        e_copy(i).start()
        for j in range(side_cols // cw):
            cols = pl.ds(pl.multiple_of(core * side_cols + j * cw, cw), cw)
            k.early[i, :, j * cw : (j + 1) * cw] = jnp.dot(
                a, ow[:, cols], preferred_element_type=F32
            ).astype(BF16)

    def forward(i):
        e_copy(i).wait_recv()
        for h in range(2):
            r = slice(h * step_rows, (h + 1) * step_rows)
            k.xsend[2 * i + h] = (k.early[i, r].astype(F32) + k.erecv[i, r].astype(F32)).astype(BF16)
            x_copy(2 * i + h).start()

    def early_step(i, carry):
        early_block(i)

        @pl.when(i > 0)
        def _():
            forward(i - 1)

        for at, relay, j in ((1, travel.relay_x, 2), (3, travel.relay_y, 0), (4, travel.relay_x, 3)):

            @pl.when(i == min(at, half_blocks - 1))
            def _():
                relay(j)

        return carry

    lax.fori_loop(0, half_blocks, early_step, 0)
    forward(half_blocks - 1)

    own_first = side * half_blocks
    travel.relay_y(1)
    def own_att(b, carry):
        distant(n, G, R, nb, k, b)
        for at, j in ((2, 2), (4, 3)):

            @pl.when(b == own_first + min(at, half_blocks - 1))
            def _():
                travel.relay_y(j)

        return carry

    lax.fori_loop(own_first, own_first + half_blocks, own_att, 0)
    theirs_at = pl.ds(pl.multiple_of(own_first * SB + (1 - core) * quarter, step_rows), quarter)
    ours_at = pl.ds(pl.multiple_of(own_first * SB + core * quarter, step_rows), quarter)
    p_copy = pltpu.make_async_remote_copy(
        src_ref=att.at[theirs_at], dst_ref=k.att_in.at[0], send_sem=k.p_s, recv_sem=k.p_r,
        device_id={"tp": partner}, device_id_type=MESH,
    )
    p_copy.start()

    def own_step(j, carry):
        w = ow[:, pl.ds(pl.multiple_of(j * cw, cw), cw)]
        k.halves[...] = jnp.dot(
            att[pl.ds(pl.multiple_of(own_first * SB, SB), 2 * quarter), :], w, preferred_element_type=F32
        ).astype(BF16)
        k.dsend[j] = k.halves[pl.ds(pl.multiple_of((1 - core) * quarter, step_rows), quarter), :]
        d_copy(j).start()
        k.mine[j] = k.halves[pl.ds(pl.multiple_of(core * quarter, step_rows), quarter), :]
        return carry

    lax.fori_loop(0, chunks, own_step, 0)

    travel.arrived()
    p_copy.wait_recv()
    for c in range(2):
        for step in range(half_blocks):
            a_arrival(c, step).wait_recv()

    def wide_step(j, carry):
        cols = pl.ds(pl.multiple_of(j * cw, cw), cw)
        out_cols = pl.ds(pl.multiple_of(travel.first + j * cw, cw), cw)
        o = jnp.dot(att[ours_at, :], ow[:, out_cols], preferred_element_type=F32)
        for slot in range(3):
            o = o + jnp.dot(k.att_in[slot], k.wfar[slot, :, cols], preferred_element_type=F32)
        k.out[:, out_cols] = o.astype(BF16)
        return carry

    lax.fori_loop(0, travel.columns // cw, wide_step, 0)
    def base_step(j, carry):
        d_copy(j).wait_recv()
        cols = pl.ds(pl.multiple_of(j * cw, cw), cw)
        k.base[:, cols] = k.mine[j].astype(F32) + k.drecv[j].astype(F32)
        d_copy(j).wait_send()
        return carry

    lax.fori_loop(0, chunks, base_step, 0)

    def last_step(s, carry):
        r = pl.ds(pl.multiple_of(s * step_rows, step_rows), step_rows)
        for c in range(2):
            x_arrival(c, s).wait_recv()
            cols = slice(c * side_cols, (c + 1) * side_cols)
            k.out[r, cols] = (k.base[r, cols] + k.xrecv[c, s].astype(F32)).astype(BF16)
        e_copy(s).wait_send()
        x_copy(s).wait_send()
        x_copy(half_blocks + s).wait_send()
        a_copy(s).wait_send()
        a_copy(half_blocks + s).wait_send()
        return carry

    lax.fori_loop(0, half_blocks, last_step, 0)
    p_copy.wait_send()
    travel.sent()


def layer_kernel(n, G, R, nb, kc, cw, names, *refs):
    k = types.SimpleNamespace(**dict(zip(names, refs, strict=True)))
    ow_loads = [pltpu.make_async_copy(k.ow_hbm, k.ow, k.sem_ow)]
    travel = Travel(k, PIECES)
    blocks_done = project(n, G, R, nb, kc, k, ow_loads, travel)
    attend_and_mix(n, G, R, nb, cw, k, ow_loads, blocks_done, travel)


def local(
    n,
    tokens, query_weight, key_weight, value_weight, gate_weight,
    summary_pos, key_mixing, value_mixing, out_weight, chosen,
):
    rows, depth = tokens.shape
    heads = query_weight.shape[1] // HD
    G = key_weight.shape[1] // HD
    R = heads // G
    nb = rows // SB
    spans = rows // CMP
    slot = -(-spans // 8) * 8
    all_spans = -(-n * slot // LANES) * LANES
    kc = min(1024, depth)
    chunks = depth // kc
    width = out_weight.shape[1]
    cw = 512
    wide = width // 2
    summed = width - wide
    oc = summed // cw
    gates_all = gate_weight.shape[1]
    assert G == 2 and n % 2 == 0 and 2 * gates_all == LANES and nb % 2 == 0

    vmem = pl.BlockSpec(memory_space=pltpu.VMEM)
    hbm = pl.BlockSpec(memory_space=pl.ANY)
    dma = pltpu.SemaphoreType.DMA
    V = pltpu.VMEM
    nbp = -(-nb // 8) * 8
    quarter = rows // 4
    half = nb // 2
    inputs = ["tok_hbm", "qw_hbm", "kw_hbm", "vw_hbm", "gw_hbm", "chosen", "km", "vm", "pos", "ow_hbm"]
    scratch = {
        "q_near": V((nb, G * HD, G * R * SB), BF16),
        "q_far": V((G, nb, 2 * HD, 2 * R * SB), BF16),
        "tok": V((rows, depth), BF16),
        "qw": V((depth, heads * HD), BF16),
        "kvw": V((depth, 2 * LANES), BF16),
        "gw": V((LANES, depth), BF16),
        "ow": V(out_weight.shape, BF16),
        "acc": V((rows, heads * HD), F32),
        "gacc": V((rows, LANES), F32),
        "gate": V((2, rows, heads * HD), F32),
        "keys": V((rows, LANES), BF16),
        "vals": V((LANES, rows), BF16),
        "left": V((G * nb, 2 * SB, LANES), BF16),
        "right": V((G * nb, 2 * SB, LANES), BF16),
        "named": V((G, nbp, LANES), jnp.int32),
        "bias": V((G, nbp, LANES), F32),
        "bias_smem": pltpu.SMEM((G, nbp, LANES), F32),
        "pos_wide": V((CMP, LANES), F32),
        "req": V((n, 8, LANES), jnp.int32),
        "req_in": V((n, 8, LANES), jnp.int32),
        "req_smem": pltpu.SMEM((n, 8, LANES), jnp.int32),
        "send": V((n, G, 2 * SB, LANES), BF16),
        "far": V((n - 1, G, 2 * SB, LANES), BF16),
        "sum_send": V((2 * slot, LANES), BF16),
        "sum_in": V((n, 2 * slot, LANES), BF16),
        "sum_key": V((all_spans, LANES), F32),
        "sum_val": V((all_spans, LANES), F32),
        "sum_keys": V((all_spans, LANES), BF16),
        "sum_vals": V((LANES, all_spans), BF16),
        "score": V((2, rows + n * slot, heads * HD), F32),
        "far_score": V((G, (n - 1) * SB, 2 * R * SB), F32),
        "top": V((nb, 8, heads * HD), F32),
        "total": V((nb, 8, heads * HD), F32),
        "part": V((nb, HD, heads * HD), F32),
        "mixed": V((rows, heads * HD), F32),
        "att": V((rows, heads * HD), BF16),
        "halves": V((2 * quarter, cw), BF16),
        "mine": V((oc, quarter, cw), BF16),
        "dsend": V((oc, quarter, cw), BF16),
        "drecv": V((oc, quarter, cw), BF16),
        "early": V((half, SB, summed // 2), BF16),
        "esend": V((half, SB, summed // 2), BF16),
        "erecv": V((half, SB, summed // 2), BF16),
        "xsend": V((2 * half, SB // 2, summed // 2), BF16),
        "xrecv": V((2, half, SB // 2, summed // 2), BF16),
        "base": V((quarter, summed), F32),
        "wfar": V((3, out_weight.shape[0], wide), BF16),
        "att_in": V((3, quarter, heads * HD), BF16),
        "sem_ow": dma,
        "sem_bias": dma,
        "sem_req": dma((n,)),
        "sem_tok": dma((chunks,)), "sem_kw": dma((chunks,)), "sem_vw": dma((chunks,)),
        "sem_qw": dma((chunks,)), "sem_gw": dma((2, chunks)),
        "req_s": dma((n,)), "req_r": dma((n,)), "blk_s": dma((n,)), "blk_r": dma((n,)),
        "sum_s": dma((n,)), "sum_r": dma((n,)),
        "d_s": dma((oc,)), "d_r": dma((oc,)), "e_s": dma((half,)), "e_r": dma((half,)),
        "x_s": dma((2 * half,)), "x_r": dma((2, half)),
        "a_s": dma((2 * half,)), "a_r": dma((2, half)), "p_s": dma, "p_r": dma,
        "wx_s": dma((PIECES,)), "wx_r": dma((PIECES,)), "wp_s": dma, "wp_r": dma,
        "wy_s": dma((PIECES,)), "wy_r": dma((PIECES,)),
        "wd_s": dma((2, PIECES)), "wd_r": dma((2, PIECES)),
    }
    return pl.pallas_call(
        functools.partial(layer_kernel, n, G, R, nb, kc, cw, inputs + ["out"] + list(scratch)),
        name="layer",
        out_shape=pltpu.VMEM((quarter, width), BF16),
        in_specs=[hbm] * 5 + [vmem] * 4 + [hbm],
        out_specs=vmem,
        scratch_shapes=list(scratch.values()),
        compiler_params=pltpu.CompilerParams(
            collective_id=1, has_side_effects=True, vmem_limit_bytes=VMEM_LIMIT
        ),
    )(
        tokens, query_weight, key_weight, value_weight, gate_weight.T,
        chosen, key_mixing.T, value_mixing.T, summary_pos, out_weight,
    )


def solution(mesh):
    placed = (
        P("kv", None),
        P(None, "tp"),
        P(None, "tp"),
        P(None, "tp"),
        P(),
        P(),
        P(),
        P(),
        P("tp", None),
        P("kv", "tp", None),
    )
    return jax.shard_map(
        functools.partial(local, mesh.shape["kv"]),
        mesh=mesh, in_specs=placed, out_specs=P(("kv", "tp"), None), check_vma=False,
    )
```

```python
import functools
import types

import jax
import jax.numpy as jnp
from jax import lax
from jax.experimental import pallas as pl
from jax.experimental.pallas import tpu as pltpu
from jax.sharding import PartitionSpec as P

HD = 64
CMP = 32
SB = 64
N_SEL = 16
LANES = 128
LOW = -1e30
F32 = jnp.float32
BF16 = jnp.bfloat16
MESH = pl.DeviceIdType.MESH
VMEM_LIMIT = 64_000_000
NT = (((1,), (1,)), ((), ()))


def requests(n, G, nb, k):
    place = lax.broadcasted_iota(jnp.int32, k.named.shape, 1)
    for g in range(G):
        k.named[g] = jnp.full(k.named.shape[1:], -1, jnp.int32)
        k.named[g, :nb, :N_SEL] = k.chosen[:, g, :]
        c = k.named[g]
        source = jnp.zeros_like(c)
        for s in range(1, n):
            source = source + jnp.where(c >= s * nb, 1, 0)
        inside = c - source * nb
        for s in range(n):
            hit = (c >= 0) & (source == s)
            lo = jnp.where(hit, inside, nb)
            lo = jnp.min(jnp.min(lo, axis=0, keepdims=True), axis=1, keepdims=True)
            lo = jnp.where(lo == nb, 0, lo)
            hi = jnp.where(hit, inside, 0)
            hi = jnp.max(jnp.max(hi, axis=0, keepdims=True), axis=1, keepdims=True)
            k.req[s, 2 * g : 2 * g + 1] = jnp.broadcast_to(lo, (1, LANES))
            k.req[s, 2 * g + 1 : 2 * g + 2] = jnp.broadcast_to(hi, (1, LANES))


def biases(n, G, nb, k, me):
    for g in range(G):
        c = k.named[g]
        lane = lax.broadcasted_iota(jnp.int32, c.shape, 1)
        bias = jnp.full(c.shape, LOW, F32)

        def mark(bias, hit, at):
            hit = jnp.max(jnp.where(hit, 1.0, 0.0), axis=1, keepdims=True)
            return jnp.where((lane == at) & (hit > 0.0), 0.0, bias)

        for j in range(nb):
            bias = mark(bias, c == me * nb + j, j)
        for s in range(n - 1):
            lo = k.req[s, 2 * g : 2 * g + 1]
            hi = k.req[s, 2 * g + 1 : 2 * g + 2]
            at = jnp.where(me > s, nb + 2 * (me - s - 1), -5)
            real = c >= 0
            bias = mark(bias, real & (c == s * nb + lo), at)
            bias = mark(bias, real & (c == s * nb + hi) & (hi != lo), at + 1)
        k.bias[g] = bias


class Travel:
    SPLIT = ((0, 2), (2, 1), (3, 2))

    def __init__(self, k):
        tp, me = lax.axis_index("tp"), lax.axis_index("kv")
        core, side = lax.rem(tp, 2), tp // 2
        place = lax.rem(me, 4)
        odd, upper = lax.rem(place, 2), place // 2
        self.k = k
        self.across = {"tp": (1 - side) * 2 + core}
        self.partner = {"tp": side * 2 + 1 - core}
        self.first_of = {"kv": me + 1 - 2 * odd}
        self.second_of = {"kv": me + 2 - 4 * upper}
        self.own, self.by_first, self.by_second, self.last = (
            place, place + 1 - 2 * odd, place + 2 - 4 * upper, 3 - place,
        )
        self.columns = k.wfar.shape[2]
        self.first = k.ow.shape[1] - self.columns

    def cols(self, quarter, j, base=0):
        unit = self.columns // 20
        at, size = self.SPLIT[j]
        return pl.ds(pl.multiple_of(base + (quarter * 5 + at) * unit, LANES), size * unit)

    def copy(self, src, dst, send, recv, target):
        return pltpu.make_async_remote_copy(
            src_ref=src, dst_ref=dst, send_sem=send, recv_sem=recv,
            device_id=target, device_id_type=MESH,
        )

    def x(self, j):
        k = self.k
        quarter, piece = (self.own, j) if j < 3 else (self.last, 2)
        return self.copy(
            k.ow_hbm.at[:, self.cols(quarter, piece, self.first)], k.wfar.at[1, :, self.cols(quarter, piece)],
            k.wx_s.at[j], k.wx_r.at[j], self.across,
        )

    def p(self):
        k = self.k
        return self.copy(
            k.ow_hbm.at[:, pl.ds(self.first, self.columns)], k.wfar.at[0], k.wp_s, k.wp_r, self.partner
        )

    def pass_on(self, quarter, j, sems, at, target):
        here = self.k.wfar.at[1, :, self.cols(quarter, j)]
        return self.copy(here, here, sems[0].at[at], sems[1].at[at], target)

    def y(self, j, arrival=False):
        return self.pass_on(self.by_first if arrival else self.own, j, (self.k.wy_s, self.k.wy_r), j, self.first_of)

    def z(self, j, arrival=False):
        return self.pass_on(self.by_second if arrival else self.own, j, (self.k.wz_s, self.k.wz_r), j, self.second_of)

    def g(self, j, arrival=False):
        return self.pass_on(self.last if arrival else self.by_second, j, (self.k.wg_s, self.k.wg_r), j, self.first_of)

    def d(self, q, j):
        k = self.k
        at = self.cols((self.own, self.by_first, self.by_second, self.last)[q], j)
        return self.copy(
            k.wfar.at[1, :, at], k.wfar.at[2, :, at], k.wd_s.at[q, j], k.wd_r.at[q, j], self.partner
        )

    def start(self):
        for j in range(4):
            self.x(j).start()
        self.p().start()

    def relay_x(self, j):
        self.x(j).wait_recv()
        if j < 3:
            self.z(j).start()
            self.y(j).start()
            self.d(0, j).start()
        else:
            self.d(3, 2).start()

    def relay_y(self, j):
        self.y(j, True).wait_recv()
        self.d(1, j).start()

    def relay_z(self, j):
        self.z(j, True).wait_recv()
        if j < 2:
            self.g(j).start()
        self.d(2, j).start()

    def relay_g(self, j):
        self.g(j, True).wait_recv()
        self.d(3, j).start()

    def arrived(self):
        self.p().wait_recv()
        for q in range(4):
            for j in range(3):
                self.d(q, j).wait_recv()

    def sent(self):
        self.p().wait_send()
        for j in range(4):
            self.x(j).wait_send()
        for j in range(3):
            self.y(j).wait_send()
            self.z(j).wait_send()
            if j < 2:
                self.g(j).wait_send()
            for q in range(4):
                self.d(q, j).wait_send()


def project(n, G, R, nb, kc, k, ow_loads, travel):
    tp = lax.axis_index("tp")
    me = lax.axis_index("kv")
    rows = nb * SB
    depth = k.tok.shape[1]
    chunks = depth // kc
    spans = rows // CMP
    slot = k.sum_send.shape[0] // 2

    def part(i):
        return pl.ds(i * kc, kc)

    def loads(i):
        return [
            pltpu.make_async_copy(k.tok_hbm.at[:, part(i)], k.tok.at[:, part(i)], k.sem_tok.at[i]),
            pltpu.make_async_copy(k.kw_hbm.at[part(i)], k.kvw.at[part(i), pl.ds(0, LANES)], k.sem_kw.at[i]),
            pltpu.make_async_copy(k.vw_hbm.at[part(i)], k.kvw.at[part(i), pl.ds(LANES, LANES)], k.sem_vw.at[i]),
        ]

    half_gates = k.gw.shape[0] // 2

    def late(i):
        return [
            pltpu.make_async_copy(k.qw_hbm.at[part(i)], k.qw.at[part(i)], k.sem_qw.at[i]),
            pltpu.make_async_copy(k.gw_hbm.at[:, part(i)], k.gw.at[pl.ds(0, half_gates), part(i)], k.sem_gw.at[0, i]),
            pltpu.make_async_copy(k.gw_hbm.at[:, part(i)], k.gw.at[pl.ds(half_gates, half_gates), part(i)], k.sem_gw.at[1, i]),
        ]

    small = [
        pltpu.make_async_copy(src, dst, k.sem_small.at[i])
        for i, (src, dst) in enumerate((
            (k.chosen_hbm, k.chosen), (k.km_hbm, k.km), (k.vm_hbm, k.vm), (k.pos_hbm, k.pos),
        ))
    ]
    for c in small:
        c.start()
    for i in range(chunks):
        for c in loads(i):
            c.start()

    barrier = pltpu.get_barrier_semaphore()
    for i in range(1, n):
        pl.semaphore_signal(
            barrier, inc=1, device_id={"kv": lax.rem(me + i, n)}, device_id_type=MESH
        )
    for i in range(1, 4):
        pl.semaphore_signal(barrier, inc=1, device_id={"tp": lax.rem(tp + i, 4)}, device_id_type=MESH)

    small[0].wait()
    requests(n, G, nb, k)
    pl.semaphore_wait(barrier, n + 2)

    def req_copy(i):
        return pltpu.make_async_remote_copy(
            src_ref=k.req.at[lax.rem(me + n - i, n)], dst_ref=k.req_in.at[i],
            send_sem=k.req_s.at[i], recv_sem=k.req_r.at[i],
            device_id={"kv": lax.rem(me + n - i, n)}, device_id_type=MESH,
        )

    def req_local(i):
        return pltpu.make_async_copy(k.req_in.at[i], k.req_smem.at[i], k.sem_req.at[i])

    def blk_copy(i):
        return pltpu.make_async_remote_copy(
            src_ref=k.send.at[i], dst_ref=k.far.at[i - 1],
            send_sem=k.blk_s.at[i], recv_sem=k.blk_r.at[i],
            device_id={"kv": lax.rem(me + i, n)}, device_id_type=MESH,
        )

    def sum_copy(i):
        return pltpu.make_async_remote_copy(
            src_ref=k.sum_send, dst_ref=k.sum_in.at[i],
            send_sem=k.sum_s.at[i], recv_sem=k.sum_r.at[i],
            device_id={"kv": lax.rem(me + i, n)}, device_id_type=MESH,
        )

    for i in range(1, n):
        req_copy(i).start()
    travel.start()

    biases(n, G, nb, k, me)
    bias_copy = pltpu.make_async_copy(k.bias, k.bias_smem, k.sem_bias)
    bias_copy.start()
    for i in range(1, n):

        @pl.when(me < i)
        def _():
            k.far[i - 1] = jnp.zeros(k.far.shape[1:], BF16)

    k.q_near[...] = jnp.zeros_like(k.q_near)
    k.q_far[...] = jnp.zeros_like(k.q_far)
    k.sum_key[...] = jnp.zeros_like(k.sum_key)
    k.sum_val[...] = jnp.zeros_like(k.sum_val)
    k.acc[:, : 2 * LANES] = jnp.zeros((rows, 2 * LANES), F32)

    def kv_step(i, carry):
        for c in loads(i):
            c.wait()
        for c in late(i):
            c.start()
        k.acc[:, : 2 * LANES] += jnp.dot(k.tok[:, part(i)], k.kvw[part(i), :], preferred_element_type=F32)
        return carry

    lax.fori_loop(0, chunks, kv_step, 0)
    for c in ow_loads:
        c.start()
    for c in small[1:]:
        c.wait()
    low = lax.broadcasted_iota(jnp.int32, (SB, LANES), 1) < HD
    mix_row = lax.broadcasted_iota(jnp.int32, k.km.shape, 0)
    mix_low = lax.broadcasted_iota(jnp.int32, (CMP, LANES), 1) < HD
    diagonal = lax.broadcasted_iota(jnp.int32, (CMP, CMP), 0) == lax.broadcasted_iota(
        jnp.int32, (CMP, CMP), 1
    )

    def mix_column(ref, head):
        line = jnp.where(mix_row == head, ref[...].astype(F32), 0.0)
        line = jnp.sum(line, axis=0, keepdims=True)
        return jnp.sum(jnp.where(diagonal, line, 0.0), axis=1, keepdims=True)

    k.pos_wide[:, :HD] = k.pos[...].astype(F32)
    k.pos_wide[:, HD:] = k.pos[...].astype(F32)
    both = []
    for ref, at, more in ((k.km, 0, 1.0), (k.vm, LANES, 0.0)):
        mix = jnp.where(mix_low, mix_column(ref, tp * G), mix_column(ref, tp * G + 1))
        t = k.acc[:, at : at + LANES].astype(BF16).astype(F32).reshape(spans, CMP, LANES)
        s = jnp.sum((t + k.pos_wide[...][None]) * mix[None], axis=1)
        if slot > spans:
            s = jnp.concatenate([s, s[: slot - spans] * more], axis=0)
        both.append(s)
    both = jnp.concatenate(both, axis=0).astype(BF16)
    k.sum_send[...] = both
    k.sum_key[:slot] = both.astype(F32)[:slot]
    k.sum_val[:slot] = both.astype(F32)[slot:]
    for i in range(1, n):

        @pl.when(me + i < n)
        def _():
            sum_copy(i).start()

    for t in range(nb // 2):
        r0 = slice(t * LANES, (t + 1) * LANES)
        keys = k.acc[r0, :LANES].astype(BF16).astype(F32)
        vals = jnp.transpose(k.acc[r0, LANES : 2 * LANES].astype(BF16).astype(F32))
        k.keys[r0, :] = keys.astype(BF16)
        k.vals[:, r0] = vals.astype(BF16)
        keys_r = pltpu.roll(keys, HD, 1)
        vals_r = pltpu.roll(vals, HD, 1)
        for h in range(2):
            kk, kr = keys[h * SB : (h + 1) * SB], keys_r[h * SB : (h + 1) * SB]
            v_left, v_right = (vals, vals_r) if h == 0 else (vals_r, vals)
            for g in range(G):
                left, right = (kk, kr) if g == 0 else (kr, kk)
                v = slice(g * HD, (g + 1) * HD)
                c = g * nb + 2 * t + h
                k.left[c, :SB] = jnp.where(low, left, 0.0).astype(BF16)
                k.left[c, SB:] = jnp.where(low, v_left[v], 0.0).astype(BF16)
                k.right[c, :SB] = jnp.where(low, 0.0, right).astype(BF16)
                k.right[c, SB:] = jnp.where(low, 0.0, v_right[v]).astype(BF16)
    first = range(1, min(4, n))
    for i in first:
        req_copy(i).wait_recv()
        req_local(i).start()
    def answer(i):
        req_local(i).wait()

        @pl.when(me + i < n)
        def _():
            for g in range(G):
                lo = k.req_smem[i, 2 * g, 0]
                hi = k.req_smem[i, 2 * g + 1, 0]
                k.send[i, g] = k.left[g * nb + lo] + k.right[g * nb + hi]
            blk_copy(i).start()

    for i in reversed(first):
        answer(i)
    k.acc[...] = jnp.zeros_like(k.acc)
    k.gacc[...] = jnp.zeros_like(k.gacc)

    def q_step(i, carry):
        for c in late(i):
            c.wait()
        k.acc[...] += jnp.dot(k.tok[:, part(i)], k.qw[part(i), :], preferred_element_type=F32)
        k.gacc[...] += lax.dot_general(
            k.tok[:, part(i)], k.gw[:, part(i)], NT, preferred_element_type=F32
        )
        return carry

    q_step(0, 0)
    for i in range(len(first) + 1, n):
        req_copy(i).wait_recv()
        req_local(i).start()
    for i in range(n - 1, len(first), -1):
        answer(i)
    lax.fori_loop(1, chunks, q_step, 0)
    travel.relay_x(0)
    wide_low = lax.broadcasted_iota(jnp.int32, k.gacc.shape, 1) < half_gates
    gates = jax.nn.sigmoid(k.gacc[...])
    gates_hi = gates.astype(BF16).astype(F32)
    gates = jnp.where(wide_low, gates_hi, gates - gates_hi).astype(BF16)
    spread_row = lax.broadcasted_iota(jnp.int32, (LANES, G * R * HD), 0)
    spread_col = lax.broadcasted_iota(jnp.int32, (LANES, G * R * HD), 1)
    spread_at = (tp * G * R + spread_col // HD) * 2
    for branch in range(2):
        spread = jnp.where(spread_row % half_gates == spread_at + branch, 1.0, 0.0).astype(BF16)
        k.gate[branch] = jnp.dot(gates, spread, preferred_element_type=F32)

    tall_low = lax.broadcasted_iota(jnp.int32, (HD, LANES), 1) < SB

    def query_step(t, carry):
        r0 = pl.ds(pl.multiple_of(t * LANES, LANES), LANES)
        for g in range(G):
            for pair in range(R // 2):
                at = (g * R // 2 + pair) * LANES
                x = jnp.transpose(k.acc[r0, at : at + LANES].astype(BF16).astype(F32) * (HD ** -0.5))
                turned = pltpu.roll(x, SB, 1)
                for h, (left, right) in enumerate(((x, turned), (turned, x))):
                    y = jnp.where(tall_low, left[:HD], right[HD:]).astype(BF16)
                    lo = slice(pair * LANES, (pair + 1) * LANES)
                    hi = slice(R * SB + pair * LANES, R * SB + (pair + 1) * LANES)
                    k.q_near[2 * t + h, g * HD : (g + 1) * HD, g * R * SB + pair * LANES : g * R * SB + (pair + 1) * LANES] = y
                    k.q_far[g, 2 * t + h, :HD, lo] = y
                    k.q_far[g, 2 * t + h, HD:, hi] = y
        return carry

    lax.fori_loop(0, nb // 2, query_step, 0)
    travel.relay_x(1)
    bias_copy.wait()
    for i in range(1, n):
        req_copy(i).wait_send()

        @pl.when(me + i < n)
        def _():
            sum_copy(i).wait_send()

        @pl.when(me - i >= 0)
        def _():
            sum_copy(i).wait_recv()
            both = k.sum_in[i].astype(F32)
            k.sum_key[i * slot : (i + 1) * slot] = both[:slot]
            k.sum_val[i * slot : (i + 1) * slot] = both[slot:]

    k.sum_keys[...] = k.sum_key[...].astype(BF16)
    k.sum_vals[...] = jnp.transpose(k.sum_val[...]).astype(BF16)
    def blocks_done():
        for i in range(1, n):

            @pl.when(me + i < n)
            def _():
                blk_copy(i).wait_send()

            @pl.when(me - i >= 0)
            def _():
                blk_copy(i).wait_recv()

    return blocks_done


def row8(x):
    return jnp.max(x.reshape(x.shape[0] // 8, 8, x.shape[1]), axis=0)


def sum8(x):
    return jnp.sum(x.reshape(x.shape[0] // 8, 8, x.shape[1]), axis=0)


def turn(outs):
    t = jnp.transpose(jnp.concatenate(outs, axis=0))
    turned = pltpu.roll(t, HD, 1)
    low = lax.broadcasted_iota(jnp.int32, (SB, LANES), 1) < HD
    tiles = []
    for first, second in ((t, turned), (turned, t)):
        for e in range(0, t.shape[0], 2 * SB):
            tiles.append(jnp.where(low, first[e : e + SB], second[e + SB : e + 2 * SB]))
    return tiles


def near_scores(n, k, b):
    own = (b + 1) * SB
    count = n * k.sum_send.shape[0] // 2
    keys = jnp.concatenate([k.keys[:own], k.sum_keys[:count]], axis=0)
    k.score[b % 2, : own + count] = jnp.dot(keys, k.q_near[b], preferred_element_type=F32)


def near(n, G, R, nb, k, b):
    me = lax.axis_index("kv")
    width = R * SB
    score = k.score.at[b % 2]
    rows = slice(b * SB, (b + 1) * SB)
    shape = (SB, G * width)
    later = lax.broadcasted_iota(jnp.int32, shape, 0) > lax.broadcasted_iota(jnp.int32, shape, 1) % SB

    def bias(j):
        return jnp.concatenate([jnp.full((8, width), k.bias_smem[g, b, j], F32) for g in range(G)], axis=1)

    def block(j):
        s = score[j * SB : (j + 1) * SB]
        return s + jnp.where(later, LOW, 0.0) if j == b else s

    top = None
    for j in range(b + 1):
        t = row8(block(j)) + bias(j)
        top = t if top is None else jnp.maximum(top, t)
    top = jnp.max(top, axis=0, keepdims=True)
    total = jnp.zeros((8, G * width), F32)
    weights = []
    for j in range(b + 1):
        p = jnp.exp(block(j) - (top - bias(j)[:1]))
        total = total + sum8(p)
        weights.append(p.astype(BF16))
    if b % 2 == 0:
        weights.append(jnp.zeros(shape, BF16))
    keys = len(weights) * SB
    weights = jnp.concatenate(weights, axis=0)
    k.top[b] = jnp.broadcast_to(top, k.top.shape[1:])
    k.total[b] = total
    for g in range(G):
        cols = slice(g * width, (g + 1) * width)
        k.part[b, :, cols] = jnp.dot(
            k.vals[g * HD : (g + 1) * HD, :keys], weights[:, cols], preferred_element_type=F32
        )

    slot = k.sum_send.shape[0] // 2
    spans = nb * SB // CMP
    base = (b + 1) * SB
    seen_shape = (slot, G * width)
    span = lax.broadcasted_iota(jnp.int32, seen_shape, 0)
    seen = (span < spans) & (
        span * CMP + (CMP - 1) <= b * SB + lax.broadcasted_iota(jnp.int32, seen_shape, 1) % SB
    )

    def summary(i):
        s = score[base + i * slot : base + (i + 1) * slot]
        return jnp.where(seen, s, LOW) if i == 0 else s

    def gone(i):
        return jnp.where(me >= i, 0.0, LOW).astype(F32)

    top = row8(summary(0))
    for i in range(1, n):
        top = jnp.maximum(top, row8(summary(i)) + gone(i))
    top = jnp.max(top, axis=0, keepdims=True)
    total = jnp.zeros((8, G * width), F32)
    real = spans - spans // 8 * 8
    partial = lax.broadcasted_iota(jnp.int32, (8, G * width), 0) < real
    weights = []
    for i in range(n):
        p = jnp.exp(summary(i) - (top - gone(i)))
        total = total + sum8(p[: spans // 8 * 8])
        if real:
            total = total + jnp.where(partial, p[spans // 8 * 8 :], 0.0)
        weights.append(p)
    more = k.sum_vals.shape[1] - n * slot
    if more:
        weights.append(jnp.zeros((more, G * width), F32))
    weights = jnp.concatenate(weights, axis=0).astype(BF16)
    total = jnp.sum(total, axis=0, keepdims=True)
    scale = jnp.where(top > LOW * 0.5, 1.0 / total, 0.0)
    outs = []
    for g in range(G):
        cols = slice(g * width, (g + 1) * width)
        o = jnp.dot(k.sum_vals[g * HD : (g + 1) * HD, :], weights[:, cols], preferred_element_type=F32)
        outs.append(o * scale[:, cols])
    for t, tile in enumerate(turn(outs)):
        cols = slice(t * LANES, (t + 1) * LANES)
        k.mixed[rows, cols] = tile * k.gate[0, rows, cols]


def distant(n, G, R, nb, k, b):
    width = R * SB
    own = pl.ds(b * SB, SB)
    outs = []
    for g in range(G):
        cols = slice(g * width, (g + 1) * width)
        keys = k.far[:, g, :SB, :].reshape((n - 1) * SB, LANES)
        k.far_score[g] = jnp.dot(keys, k.q_far[g, b], preferred_element_type=F32)

        def bias(i, h):
            return k.bias_smem[g, b, nb + 2 * i + h]

        before = k.top[b, :1, cols]
        top = jnp.broadcast_to(before, (8, width))
        for i in range(n - 1):
            t = row8(k.far_score[g, i * SB : (i + 1) * SB])
            for h in range(2):
                top = jnp.maximum(top, t[:, h * width : (h + 1) * width] + bias(i, h))
        top = jnp.max(top, axis=0, keepdims=True)
        keep = jnp.exp(before - top)
        total = k.total[b, :, cols] * keep
        weights = []
        for i in range(n - 1):
            for h in range(2):
                s = k.far_score[g, i * SB : (i + 1) * SB, h * width : (h + 1) * width]
                p = jnp.exp(s - (top - bias(i, h)))
                total = total + sum8(p)
                weights.append(p.astype(BF16))
        weights = jnp.concatenate(weights, axis=0)
        vals = jnp.concatenate([k.far[i, g, SB:, :] for i in range(n - 1)], axis=1)
        o = k.part[b, :, cols] * keep + jnp.dot(vals, weights, preferred_element_type=F32)
        outs.append(o * (1.0 / jnp.sum(total, axis=0, keepdims=True)))
    for t, tile in enumerate(turn(outs)):
        cols = slice(t * LANES, (t + 1) * LANES)
        k.att[own, cols] = (k.mixed[own, cols] + tile * k.gate[1, own, cols]).astype(BF16)


def attend_and_mix(n, G, R, nb, cw, k, ow_loads, blocks_done, travel):
    tp = lax.axis_index("tp")
    core = lax.rem(tp, 2)
    side = tp // 2
    partner = side * 2 + 1 - core
    rows = nb * SB
    quarter = rows // 4
    half_blocks = nb // 2
    width = k.base.shape[1]
    chunks = width // cw
    side_cols = width // 2
    step_rows = SB // 2
    att, ow = k.att, k.ow

    near_scores(n, k, 0)
    for b in range(nb):
        if b + 1 < nb:
            near_scores(n, k, b + 1)
        near(n, G, R, nb, k, b)
    for c in ow_loads:
        c.wait()
    travel.relay_x(2)
    blocks_done()

    def d_copy(j):
        return pltpu.make_async_remote_copy(
            src_ref=k.dsend.at[j], dst_ref=k.drecv.at[j],
            send_sem=k.d_s.at[j], recv_sem=k.d_r.at[j],
            device_id={"tp": partner}, device_id_type=MESH,
        )

    def e_copy(i):
        return pltpu.make_async_remote_copy(
            src_ref=k.esend.at[i], dst_ref=k.erecv.at[i],
            send_sem=k.e_s.at[i], recv_sem=k.e_r.at[i],
            device_id={"tp": partner}, device_id_type=MESH,
        )

    def x_copy(i):
        step = lax.rem(i, half_blocks)
        return pltpu.make_async_remote_copy(
            src_ref=k.xsend.at[i], dst_ref=k.xrecv.at[core, step],
            send_sem=k.x_s.at[i], recv_sem=k.x_r.at[core, step],
            device_id={"tp": (1 - side) * 2 + i // half_blocks}, device_id_type=MESH,
        )

    def x_arrival(c, step):
        return pltpu.make_async_remote_copy(
            src_ref=k.xsend.at[step], dst_ref=k.xrecv.at[c, step],
            send_sem=k.x_s.at[step], recv_sem=k.x_r.at[c, step],
            device_id={"tp": (1 - side) * 2 + core}, device_id_type=MESH,
        )

    other_first = (1 - side) * half_blocks

    def a_copy(i):
        to, step = i // half_blocks, lax.rem(i, half_blocks)
        rows_of = pl.ds(pl.multiple_of(other_first * SB + i * step_rows, step_rows), step_rows)
        into = pl.ds(pl.multiple_of(step * step_rows, step_rows), step_rows)
        return pltpu.make_async_remote_copy(
            src_ref=att.at[rows_of], dst_ref=k.att_in.at[1 + lax.rem(to + core, 2), into],
            send_sem=k.a_s.at[i], recv_sem=k.a_r.at[core, step],
            device_id={"tp": (1 - side) * 2 + to}, device_id_type=MESH,
        )

    def a_arrival(c, step):
        into = pl.ds(pl.multiple_of(step * step_rows, step_rows), step_rows)
        return pltpu.make_async_remote_copy(
            src_ref=att.at[into], dst_ref=k.att_in.at[1 + lax.rem(c + core, 2), into],
            send_sem=k.a_s.at[step], recv_sem=k.a_r.at[c, step],
            device_id={"tp": (1 - side) * 2 + core}, device_id_type=MESH,
        )

    def early_block(i):
        distant(n, G, R, nb, k, other_first + i)
        for h in range(2):
            a_copy(2 * i + h).start()
        a = att[pl.ds((other_first + i) * SB, SB), :]
        cols = pl.ds(pl.multiple_of((1 - core) * side_cols, LANES), side_cols)
        k.esend[i] = jnp.dot(a, ow[:, cols], preferred_element_type=F32).astype(BF16)
        e_copy(i).start()
        cols = pl.ds(pl.multiple_of(core * side_cols, LANES), side_cols)
        k.early[i] = jnp.dot(a, ow[:, cols], preferred_element_type=F32).astype(BF16)

    def forward(i):
        e_copy(i).wait_recv()
        for h in range(2):
            r = slice(h * step_rows, (h + 1) * step_rows)
            k.xsend[2 * i + h] = (k.early[i, r].astype(F32) + k.erecv[i, r].astype(F32)).astype(BF16)
            x_copy(2 * i + h).start()

    def early_step(i, carry):
        early_block(i)

        @pl.when(i > 0)
        def _():
            forward(i - 1)

        for at, relays in (
            (1, ((travel.relay_x, 3), (travel.relay_y, 0))),
            (2, ((travel.relay_y, 1),)),
            (3, ((travel.relay_z, 0),)),
            (4, ((travel.relay_z, 1), (travel.relay_y, 2))),
        ):

            @pl.when(i == min(at, half_blocks - 1))
            def _():
                for relay, j in relays:
                    relay(j)

        return carry

    lax.fori_loop(0, half_blocks, early_step, 0)
    forward(half_blocks - 1)

    own_first = side * half_blocks
    def own_att(b, carry):
        distant(n, G, R, nb, k, b)
        for at, relays in (
            (3, ((travel.relay_g, 0), (travel.relay_z, 2))),
            (4, ((travel.relay_g, 1),)),
        ):

            @pl.when(b == own_first + min(at, half_blocks - 1))
            def _():
                for relay, j in relays:
                    relay(j)

        return carry

    lax.fori_loop(own_first, own_first + half_blocks, own_att, 0)
    theirs_at = pl.ds(pl.multiple_of(own_first * SB + (1 - core) * quarter, step_rows), quarter)
    ours_at = pl.ds(pl.multiple_of(own_first * SB + core * quarter, step_rows), quarter)
    p_copy = pltpu.make_async_remote_copy(
        src_ref=att.at[theirs_at], dst_ref=k.att_in.at[0], send_sem=k.p_s, recv_sem=k.p_r,
        device_id={"tp": partner}, device_id_type=MESH,
    )
    p_copy.start()

    def own_step(j, carry):
        w = ow[:, pl.ds(pl.multiple_of(j * cw, cw), cw)]
        k.halves[...] = jnp.dot(
            att[pl.ds(pl.multiple_of(own_first * SB, SB), 2 * quarter), :], w, preferred_element_type=F32
        ).astype(BF16)
        k.dsend[j] = k.halves[pl.ds(pl.multiple_of((1 - core) * quarter, step_rows), quarter), :]
        d_copy(j).start()
        k.mine[j] = k.halves[pl.ds(pl.multiple_of(core * quarter, step_rows), quarter), :]
        return carry

    lax.fori_loop(0, chunks, own_step, 0)

    travel.arrived()
    p_copy.wait_recv()
    for c in range(2):
        for step in range(half_blocks):
            a_arrival(c, step).wait_recv()

    def wide_step(j, carry):
        cols = pl.ds(pl.multiple_of(j * cw, cw), cw)
        out_cols = pl.ds(pl.multiple_of(travel.first + j * cw, cw), cw)
        o = jnp.dot(att[ours_at, :], ow[:, out_cols], preferred_element_type=F32)
        for slot in range(3):
            o = o + jnp.dot(k.att_in[slot], k.wfar[slot, :, cols], preferred_element_type=F32)
        k.out[:, out_cols] = o.astype(BF16)
        return carry

    lax.fori_loop(0, travel.columns // cw, wide_step, 0)
    def base_step(j, carry):
        d_copy(j).wait_recv()
        cols = pl.ds(pl.multiple_of(j * cw, cw), cw)
        k.base[:, cols] = k.mine[j].astype(F32) + k.drecv[j].astype(F32)
        d_copy(j).wait_send()
        return carry

    lax.fori_loop(0, chunks, base_step, 0)

    def last_step(s, carry):
        r = pl.ds(pl.multiple_of(s * step_rows, step_rows), step_rows)
        for c in range(2):
            x_arrival(c, s).wait_recv()
            cols = slice(c * side_cols, (c + 1) * side_cols)
            k.out[r, cols] = (k.base[r, cols] + k.xrecv[c, s].astype(F32)).astype(BF16)
        e_copy(s).wait_send()
        x_copy(s).wait_send()
        x_copy(half_blocks + s).wait_send()
        a_copy(s).wait_send()
        a_copy(half_blocks + s).wait_send()
        return carry

    lax.fori_loop(0, half_blocks, last_step, 0)
    p_copy.wait_send()
    travel.sent()


def layer_kernel(n, G, R, nb, kc, cw, names, *refs):
    k = types.SimpleNamespace(**dict(zip(names, refs, strict=True)))
    ow_loads = [pltpu.make_async_copy(k.ow_hbm, k.ow, k.sem_ow)]
    travel = Travel(k)
    blocks_done = project(n, G, R, nb, kc, k, ow_loads, travel)
    attend_and_mix(n, G, R, nb, cw, k, ow_loads, blocks_done, travel)


def local(
    n,
    tokens, query_weight, key_weight, value_weight, gate_weight,
    summary_pos, key_mixing, value_mixing, out_weight, chosen,
):
    rows, depth = tokens.shape
    heads = query_weight.shape[1] // HD
    G = key_weight.shape[1] // HD
    R = heads // G
    nb = rows // SB
    spans = rows // CMP
    slot = -(-spans // 8) * 8
    all_spans = -(-n * slot // LANES) * LANES
    kc = min(1024, depth)
    chunks = depth // kc
    width = out_weight.shape[1]
    cw = 512
    wide = width // (20 * LANES * 8 // 5) * 20 * LANES
    summed = width - wide
    oc = summed // cw
    gates_all = gate_weight.shape[1]
    assert G == 2 and n % 4 == 0 and 2 * gates_all == LANES and nb % 2 == 0

    vmem = pl.BlockSpec(memory_space=pltpu.VMEM)
    hbm = pl.BlockSpec(memory_space=pl.ANY)
    dma = pltpu.SemaphoreType.DMA
    V = pltpu.VMEM
    nbp = -(-nb // 8) * 8
    quarter = rows // 4
    half = nb // 2
    inputs = ["tok_hbm", "qw_hbm", "kw_hbm", "vw_hbm", "gw_hbm", "chosen_hbm", "km_hbm", "vm_hbm", "pos_hbm", "ow_hbm"]
    scratch = {
        "q_near": V((nb, G * HD, G * R * SB), BF16),
        "q_far": V((G, nb, 2 * HD, 2 * R * SB), BF16),
        "chosen": V(chosen.shape, jnp.int32),
        "km": V(key_mixing.shape[::-1], BF16),
        "vm": V(value_mixing.shape[::-1], BF16),
        "pos": V(summary_pos.shape, BF16),
        "sem_small": dma((4,)),
        "tok": V((rows, depth), BF16),
        "qw": V((depth, heads * HD), BF16),
        "kvw": V((depth, 2 * LANES), BF16),
        "gw": V((LANES, depth), BF16),
        "ow": V(out_weight.shape, BF16),
        "acc": V((rows, heads * HD), F32),
        "gacc": V((rows, LANES), F32),
        "gate": V((2, rows, heads * HD), F32),
        "keys": V((rows, LANES), BF16),
        "vals": V((LANES, rows), BF16),
        "left": V((G * nb, 2 * SB, LANES), BF16),
        "right": V((G * nb, 2 * SB, LANES), BF16),
        "named": V((G, nbp, LANES), jnp.int32),
        "bias": V((G, nbp, LANES), F32),
        "bias_smem": pltpu.SMEM((G, nbp, LANES), F32),
        "pos_wide": V((CMP, LANES), F32),
        "req": V((n, 8, LANES), jnp.int32),
        "req_in": V((n, 8, LANES), jnp.int32),
        "req_smem": pltpu.SMEM((n, 8, LANES), jnp.int32),
        "send": V((n, G, 2 * SB, LANES), BF16),
        "far": V((n - 1, G, 2 * SB, LANES), BF16),
        "sum_send": V((2 * slot, LANES), BF16),
        "sum_in": V((n, 2 * slot, LANES), BF16),
        "sum_key": V((all_spans, LANES), F32),
        "sum_val": V((all_spans, LANES), F32),
        "sum_keys": V((all_spans, LANES), BF16),
        "sum_vals": V((LANES, all_spans), BF16),
        "score": V((2, rows + n * slot, heads * HD), F32),
        "far_score": V((G, (n - 1) * SB, 2 * R * SB), F32),
        "top": V((nb, 8, heads * HD), F32),
        "total": V((nb, 8, heads * HD), F32),
        "part": V((nb, HD, heads * HD), F32),
        "mixed": V((rows, heads * HD), F32),
        "att": V((rows, heads * HD), BF16),
        "halves": V((2 * quarter, cw), BF16),
        "mine": V((oc, quarter, cw), BF16),
        "dsend": V((oc, quarter, cw), BF16),
        "drecv": V((oc, quarter, cw), BF16),
        "early": V((half, SB, summed // 2), BF16),
        "esend": V((half, SB, summed // 2), BF16),
        "erecv": V((half, SB, summed // 2), BF16),
        "xsend": V((2 * half, SB // 2, summed // 2), BF16),
        "xrecv": V((2, half, SB // 2, summed // 2), BF16),
        "base": V((quarter, summed), F32),
        "wfar": V((3, out_weight.shape[0], wide), BF16),
        "att_in": V((3, quarter, heads * HD), BF16),
        "sem_ow": dma,
        "sem_bias": dma,
        "sem_req": dma((n,)),
        "sem_tok": dma((chunks,)), "sem_kw": dma((chunks,)), "sem_vw": dma((chunks,)),
        "sem_qw": dma((chunks,)), "sem_gw": dma((2, chunks)),
        "req_s": dma((n,)), "req_r": dma((n,)), "blk_s": dma((n,)), "blk_r": dma((n,)),
        "sum_s": dma((n,)), "sum_r": dma((n,)),
        "d_s": dma((oc,)), "d_r": dma((oc,)), "e_s": dma((half,)), "e_r": dma((half,)),
        "x_s": dma((2 * half,)), "x_r": dma((2, half)),
        "a_s": dma((2 * half,)), "a_r": dma((2, half)), "p_s": dma, "p_r": dma,
        "wx_s": dma((4,)), "wx_r": dma((4,)), "wp_s": dma, "wp_r": dma,
        "wy_s": dma((3,)), "wy_r": dma((3,)), "wz_s": dma((3,)), "wz_r": dma((3,)),
        "wg_s": dma((2,)), "wg_r": dma((2,)), "wd_s": dma((4, 3)), "wd_r": dma((4, 3)),
    }
    return pl.pallas_call(
        functools.partial(layer_kernel, n, G, R, nb, kc, cw, inputs + ["out"] + list(scratch)),
        name="layer",
        out_shape=pltpu.VMEM((quarter, width), BF16),
        in_specs=[hbm] * 10,
        out_specs=vmem,
        scratch_shapes=list(scratch.values()),
        compiler_params=pltpu.CompilerParams(
            collective_id=1, has_side_effects=True, vmem_limit_bytes=VMEM_LIMIT
        ),
    )(
        tokens, query_weight, key_weight, value_weight, gate_weight.T,
        chosen, key_mixing.T, value_mixing.T, summary_pos, out_weight,
    )


def solution(mesh):
    placed = (
        P("kv", None),
        P(None, "tp"),
        P(None, "tp"),
        P(None, "tp"),
        P(),
        P(),
        P(),
        P(),
        P("tp", None),
        P("kv", "tp", None),
    )
    return jax.shard_map(
        functools.partial(local, mesh.shape["kv"]),
        mesh=mesh, in_specs=placed, out_specs=P(("kv", "tp"), None), check_vma=False,
    )
```

```python
import functools
import types

import jax
import jax.numpy as jnp
from jax import lax
from jax.experimental import pallas as pl
from jax.experimental.pallas import tpu as pltpu
from jax.sharding import PartitionSpec as P

HD = 64
CMP = 32
SB = 64
N_SEL = 16
LANES = 128
LOW = -1e30
F32 = jnp.float32
BF16 = jnp.bfloat16
MESH = pl.DeviceIdType.MESH
VMEM_LIMIT = 64_000_000
NT = (((1,), (1,)), ((), ()))


def all_sent(ref, sem):
    pltpu.make_async_copy(ref, ref, sem).wait()


def requests(n, G, nb, k):
    place = lax.broadcasted_iota(jnp.int32, k.named.shape, 1)
    for g in range(G):
        k.named[g] = jnp.full(k.named.shape[1:], -1, jnp.int32)
        k.named[g, :nb, :N_SEL] = k.chosen[:, g, :]
        c = k.named[g]
        source = jnp.zeros_like(c)
        for s in range(1, n):
            source = source + jnp.where(c >= s * nb, 1, 0)
        inside = c - source * nb
        for s in range(n):
            hit = (c >= 0) & (source == s)
            lo = jnp.where(hit, inside, nb)
            lo = jnp.min(jnp.min(lo, axis=0, keepdims=True), axis=1, keepdims=True)
            lo = jnp.where(lo == nb, 0, lo)
            hi = jnp.where(hit, inside, 0)
            hi = jnp.max(jnp.max(hi, axis=0, keepdims=True), axis=1, keepdims=True)
            k.req[s, 2 * g : 2 * g + 1] = jnp.broadcast_to(lo, (1, LANES))
            k.req[s, 2 * g + 1 : 2 * g + 2] = jnp.broadcast_to(hi, (1, LANES))


def biases(n, G, nb, k, me):
    for g in range(G):
        c = k.named[g]
        lane = lax.broadcasted_iota(jnp.int32, c.shape, 1)
        bias = jnp.full(c.shape, LOW, F32)

        def mark(bias, hit, at):
            hit = jnp.max(jnp.where(hit, 1.0, 0.0), axis=1, keepdims=True)
            return jnp.where((lane == at) & (hit > 0.0), 0.0, bias)

        for j in range(nb):
            bias = mark(bias, c == me * nb + j, j)
        for s in range(n - 1):
            lo = k.req[s, 2 * g : 2 * g + 1]
            hi = k.req[s, 2 * g + 1 : 2 * g + 2]
            at = jnp.where(me > s, nb + 2 * (me - s - 1), -5)
            real = c >= 0
            bias = mark(bias, real & (c == s * nb + lo), at)
            bias = mark(bias, real & (c == s * nb + hi) & (hi != lo), at + 1)
        k.bias[g] = bias


class Travel:
    SPLIT = ((0, 2), (2, 1), (3, 2))

    def __init__(self, k):
        tp, me = lax.axis_index("tp"), lax.axis_index("kv")
        core, side = lax.rem(tp, 2), tp // 2
        place = lax.rem(me, 4)
        odd, upper = lax.rem(place, 2), place // 2
        self.k = k
        self.across = {"tp": (1 - side) * 2 + core}
        self.partner = {"tp": side * 2 + 1 - core}
        self.first_of = {"kv": me + 1 - 2 * odd}
        self.second_of = {"kv": me + 2 - 4 * upper}
        self.own, self.by_first, self.by_second, self.last = (
            place, place + 1 - 2 * odd, place + 2 - 4 * upper, 3 - place,
        )
        self.columns = k.wfar.shape[2]
        self.first = k.ow.shape[1] - self.columns

    def cols(self, quarter, j, base=0):
        unit = self.columns // 20
        at, size = self.SPLIT[j]
        return pl.ds(pl.multiple_of(base + (quarter * 5 + at) * unit, LANES), size * unit)

    def copy(self, src, dst, send, recv, target):
        return pltpu.make_async_remote_copy(
            src_ref=src, dst_ref=dst, send_sem=send, recv_sem=recv,
            device_id=target, device_id_type=MESH,
        )

    def x(self, j):
        k = self.k
        quarter, piece = (self.own, j) if j < 3 else (self.last, 2)
        return self.copy(
            k.ow_hbm.at[:, self.cols(quarter, piece, self.first)], k.wfar.at[1, :, self.cols(quarter, piece)],
            k.wx_s, k.wx_r.at[j], self.across,
        )

    def p(self):
        k = self.k
        return self.copy(
            k.ow_hbm.at[:, pl.ds(self.first, self.columns)], k.wfar.at[0], k.wp_s, k.wp_r, self.partner
        )

    def pass_on(self, quarter, j, sems, at, target):
        here = self.k.wfar.at[1, :, self.cols(quarter, j)]
        return self.copy(here, here, sems[0], sems[1].at[at], target)

    def y(self, j, arrival=False):
        return self.pass_on(self.by_first if arrival else self.own, j, (self.k.wy_s, self.k.wy_r), j, self.first_of)

    def z(self, j, arrival=False):
        return self.pass_on(self.by_second if arrival else self.own, j, (self.k.wz_s, self.k.wz_r), j, self.second_of)

    def g(self, j, arrival=False):
        return self.pass_on(self.last if arrival else self.by_second, j, (self.k.wg_s, self.k.wg_r), j, self.first_of)

    def d(self, q, j):
        k = self.k
        at = self.cols((self.own, self.by_first, self.by_second, self.last)[q], j)
        return self.copy(
            k.wfar.at[1, :, at], k.wfar.at[2, :, at], k.wd_s, k.wd_r.at[q], self.partner
        )

    def start(self):
        for j in range(4):
            self.x(j).start()
        self.p().start()

    def relay_x(self, j):
        self.x(j).wait_recv()
        if j < 3:
            self.z(j).start()
            self.y(j).start()
            self.d(0, j).start()
        else:
            self.d(3, 2).start()

    def relay_y(self, j):
        self.y(j, True).wait_recv()
        self.d(1, j).start()

    def relay_z(self, j):
        self.z(j, True).wait_recv()
        if j < 2:
            self.g(j).start()
        self.d(2, j).start()

    def relay_g(self, j):
        self.g(j, True).wait_recv()
        self.d(3, j).start()

    def quarter(self, q, base=0):
        unit = self.columns // 20
        at = base + (self.own, self.by_first, self.by_second, self.last)[q] * 5 * unit
        return pl.ds(pl.multiple_of(at, LANES), 5 * unit)

    def arrived(self, q):
        all_sent(self.k.wfar.at[2, :, self.quarter(q)], self.k.wd_r.at[q])

    def sent(self):
        k, unit = self.k, self.columns // 20
        self.p().wait_send()
        for sem, size in ((k.wx_s, 7), (k.wy_s, 5), (k.wz_s, 5), (k.wg_s, 3), (k.wd_s, 20)):
            all_sent(k.wfar.at[1, :, pl.ds(0, size * unit)], sem)


def project(n, G, R, nb, kc, k, ow_loads, travel):
    tp = lax.axis_index("tp")
    me = lax.axis_index("kv")
    rows = nb * SB
    depth = k.tok.shape[1]
    chunks = depth // kc
    spans = rows // CMP
    slot = k.sum_send.shape[0] // 2

    def part(i):
        return pl.ds(i * kc, kc)

    def loads(i):
        return [
            pltpu.make_async_copy(k.tok_hbm.at[:, part(i)], k.tok.at[:, part(i)], k.sem_tok.at[i]),
            pltpu.make_async_copy(k.kw_hbm.at[part(i)], k.kvw.at[part(i), pl.ds(0, LANES)], k.sem_kw.at[i]),
            pltpu.make_async_copy(k.vw_hbm.at[part(i)], k.kvw.at[part(i), pl.ds(LANES, LANES)], k.sem_vw.at[i]),
        ]

    half_gates = k.gw.shape[0] // 2

    def late(i):
        return [
            pltpu.make_async_copy(k.qw_hbm.at[part(i)], k.qw.at[part(i)], k.sem_tok.at[i]),
            pltpu.make_async_copy(k.gw_hbm.at[:, part(i)], k.gw.at[pl.ds(0, half_gates), part(i)], k.sem_kw.at[i]),
            pltpu.make_async_copy(k.gw_hbm.at[:, part(i)], k.gw.at[pl.ds(half_gates, half_gates), part(i)], k.sem_vw.at[i]),
        ]

    small = [
        pltpu.make_async_copy(src, dst, k.sem_small.at[i])
        for i, (src, dst) in enumerate((
            (k.chosen_hbm, k.chosen), (k.km_hbm, k.km), (k.vm_hbm, k.vm), (k.pos_hbm, k.pos),
        ))
    ]
    for c in small:
        c.start()
    for i in range(chunks):
        for c in loads(i):
            c.start()

    barrier = pltpu.get_barrier_semaphore()
    for i in range(1, n):
        pl.semaphore_signal(
            barrier, inc=1, device_id={"kv": lax.rem(me + i, n)}, device_id_type=MESH
        )
    for i in range(1, 4):
        pl.semaphore_signal(barrier, inc=1, device_id={"tp": lax.rem(tp + i, 4)}, device_id_type=MESH)

    small[0].wait()
    requests(n, G, nb, k)
    pl.semaphore_wait(barrier, n + 2)

    def req_copy(i):
        return pltpu.make_async_remote_copy(
            src_ref=k.req.at[lax.rem(me + n - i, n)], dst_ref=k.req_in.at[i],
            send_sem=k.req_s, recv_sem=k.req_r.at[i],
            device_id={"kv": lax.rem(me + n - i, n)}, device_id_type=MESH,
        )

    def req_local(i):
        return pltpu.make_async_copy(k.req_in.at[i], k.req_smem.at[i], k.sem_req.at[i])

    def blk_copy(i):
        return pltpu.make_async_remote_copy(
            src_ref=k.send.at[i], dst_ref=k.far.at[i - 1],
            send_sem=k.blk_s.at[i], recv_sem=k.blk_r.at[i],
            device_id={"kv": lax.rem(me + i, n)}, device_id_type=MESH,
        )

    def sum_copy(i):
        return pltpu.make_async_remote_copy(
            src_ref=k.sum_send, dst_ref=k.sum_in.at[i],
            send_sem=k.sum_s.at[i], recv_sem=k.sum_r.at[i],
            device_id={"kv": lax.rem(me + i, n)}, device_id_type=MESH,
        )

    for i in range(1, n):
        req_copy(i).start()
    travel.start()

    biases(n, G, nb, k, me)
    bias_copy = pltpu.make_async_copy(k.bias, k.bias_smem, k.sem_bias)
    bias_copy.start()
    for i in range(1, n):

        @pl.when(me < i)
        def _():
            k.far[i - 1] = jnp.zeros(k.far.shape[1:], BF16)

    k.q_near[...] = jnp.zeros_like(k.q_near)
    k.q_far[...] = jnp.zeros_like(k.q_far)
    k.sum_key[...] = jnp.zeros_like(k.sum_key)
    k.sum_val[...] = jnp.zeros_like(k.sum_val)
    k.acc[:, : 2 * LANES] = jnp.zeros((rows, 2 * LANES), F32)

    def kv_step(i, carry):
        for c in loads(i):
            c.wait()
        for c in late(i):
            c.start()
        k.acc[:, : 2 * LANES] += jnp.dot(k.tok[:, part(i)], k.kvw[part(i), :], preferred_element_type=F32)
        return carry

    lax.fori_loop(0, chunks, kv_step, 0)
    for c in ow_loads:
        c.start()
    for c in small[1:]:
        c.wait()
    low = lax.broadcasted_iota(jnp.int32, (SB, LANES), 1) < HD
    mix_row = lax.broadcasted_iota(jnp.int32, k.km.shape, 0)
    mix_low = lax.broadcasted_iota(jnp.int32, (CMP, LANES), 1) < HD
    diagonal = lax.broadcasted_iota(jnp.int32, (CMP, CMP), 0) == lax.broadcasted_iota(
        jnp.int32, (CMP, CMP), 1
    )

    def mix_column(ref, head):
        line = jnp.where(mix_row == head, ref[...].astype(F32), 0.0)
        line = jnp.sum(line, axis=0, keepdims=True)
        return jnp.sum(jnp.where(diagonal, line, 0.0), axis=1, keepdims=True)

    k.pos_wide[:, :HD] = k.pos[...].astype(F32)
    k.pos_wide[:, HD:] = k.pos[...].astype(F32)
    both = []
    for ref, at, more in ((k.km, 0, 1.0), (k.vm, LANES, 0.0)):
        mix = jnp.where(mix_low, mix_column(ref, tp * G), mix_column(ref, tp * G + 1))
        t = k.acc[:, at : at + LANES].astype(BF16).astype(F32).reshape(spans, CMP, LANES)
        s = jnp.sum((t + k.pos_wide[...][None]) * mix[None], axis=1)
        if slot > spans:
            s = jnp.concatenate([s, s[: slot - spans] * more], axis=0)
        both.append(s)
    both = jnp.concatenate(both, axis=0).astype(BF16)
    k.sum_send[...] = both
    k.sum_key[:slot] = both.astype(F32)[:slot]
    k.sum_val[:slot] = both.astype(F32)[slot:]
    for i in range(1, n):

        @pl.when(me + i < n)
        def _():
            sum_copy(i).start()

    for t in range(nb // 2):
        r0 = slice(t * LANES, (t + 1) * LANES)
        keys = k.acc[r0, :LANES].astype(BF16).astype(F32)
        vals = jnp.transpose(k.acc[r0, LANES : 2 * LANES].astype(BF16).astype(F32))
        k.keys[r0, :] = keys.astype(BF16)
        k.vals[:, r0] = vals.astype(BF16)
        keys_r = pltpu.roll(keys, HD, 1)
        vals_r = pltpu.roll(vals, HD, 1)
        for h in range(2):
            kk, kr = keys[h * SB : (h + 1) * SB], keys_r[h * SB : (h + 1) * SB]
            v_left, v_right = (vals, vals_r) if h == 0 else (vals_r, vals)
            for g in range(G):
                left, right = (kk, kr) if g == 0 else (kr, kk)
                v = slice(g * HD, (g + 1) * HD)
                c = g * nb + 2 * t + h
                k.left[c, :SB] = jnp.where(low, left, 0.0).astype(BF16)
                k.left[c, SB:] = jnp.where(low, v_left[v], 0.0).astype(BF16)
                k.right[c, :SB] = jnp.where(low, 0.0, right).astype(BF16)
                k.right[c, SB:] = jnp.where(low, 0.0, v_right[v]).astype(BF16)
    first = range(1, min(4, n))
    for i in first:
        req_copy(i).wait_recv()
        req_local(i).start()
    def answer(i):
        req_local(i).wait()

        @pl.when(me + i < n)
        def _():
            for g in range(G):
                lo = k.req_smem[i, 2 * g, 0]
                hi = k.req_smem[i, 2 * g + 1, 0]
                k.send[i, g] = k.left[g * nb + lo] + k.right[g * nb + hi]
            blk_copy(i).start()

    for i in reversed(first):
        answer(i)
    k.acc[...] = jnp.zeros_like(k.acc)
    k.gacc[...] = jnp.zeros_like(k.gacc)

    def q_step(i, carry):
        for c in late(i):
            c.wait()
        k.acc[...] += jnp.dot(k.tok[:, part(i)], k.qw[part(i), :], preferred_element_type=F32)
        k.gacc[...] += lax.dot_general(
            k.tok[:, part(i)], k.gw[:, part(i)], NT, preferred_element_type=F32
        )
        return carry

    q_step(0, 0)
    for i in range(len(first) + 1, n):
        req_copy(i).wait_recv()
        req_local(i).start()
    for i in range(n - 1, len(first), -1):
        answer(i)
    lax.fori_loop(1, chunks, q_step, 0)
    travel.relay_x(0)
    wide_low = lax.broadcasted_iota(jnp.int32, k.gacc.shape, 1) < half_gates
    gates = jax.nn.sigmoid(k.gacc[...])
    gates_hi = gates.astype(BF16).astype(F32)
    gates = jnp.where(wide_low, gates_hi, gates - gates_hi).astype(BF16)
    spread_row = lax.broadcasted_iota(jnp.int32, (LANES, G * R * HD), 0)
    spread_col = lax.broadcasted_iota(jnp.int32, (LANES, G * R * HD), 1)
    spread_at = (tp * G * R + spread_col // HD) * 2
    for branch in range(2):
        spread = jnp.where(spread_row % half_gates == spread_at + branch, 1.0, 0.0).astype(BF16)
        k.gate[branch] = jnp.dot(gates, spread, preferred_element_type=F32)

    tall_low = lax.broadcasted_iota(jnp.int32, (HD, LANES), 1) < SB

    def query_step(t, carry):
        r0 = pl.ds(pl.multiple_of(t * LANES, LANES), LANES)
        for g in range(G):
            for pair in range(R // 2):
                at = (g * R // 2 + pair) * LANES
                x = jnp.transpose(k.acc[r0, at : at + LANES].astype(BF16).astype(F32) * (HD ** -0.5))
                turned = pltpu.roll(x, SB, 1)
                for h, (left, right) in enumerate(((x, turned), (turned, x))):
                    y = jnp.where(tall_low, left[:HD], right[HD:]).astype(BF16)
                    lo = slice(pair * LANES, (pair + 1) * LANES)
                    hi = slice(R * SB + pair * LANES, R * SB + (pair + 1) * LANES)
                    k.q_near[2 * t + h, g * HD : (g + 1) * HD, g * R * SB + pair * LANES : g * R * SB + (pair + 1) * LANES] = y
                    k.q_far[g, 2 * t + h, :HD, lo] = y
                    k.q_far[g, 2 * t + h, HD:, hi] = y
        return carry

    lax.fori_loop(0, nb // 2, query_step, 0)
    travel.relay_x(1)
    bias_copy.wait()
    all_sent(k.req.at[pl.ds(0, n - 1)], k.req_s)
    for i in range(1, n):

        @pl.when(me + i < n)
        def _():
            sum_copy(i).wait_send()

        @pl.when(me - i >= 0)
        def _():
            sum_copy(i).wait_recv()
            both = k.sum_in[i].astype(F32)
            k.sum_key[i * slot : (i + 1) * slot] = both[:slot]
            k.sum_val[i * slot : (i + 1) * slot] = both[slot:]

    k.sum_keys[...] = k.sum_key[...].astype(BF16)
    k.sum_vals[...] = jnp.transpose(k.sum_val[...]).astype(BF16)
    def blocks_done():
        for i in range(1, n):

            @pl.when(me + i < n)
            def _():
                blk_copy(i).wait_send()

            @pl.when(me - i >= 0)
            def _():
                blk_copy(i).wait_recv()

    return blocks_done


def row8(x):
    return jnp.max(x.reshape(x.shape[0] // 8, 8, x.shape[1]), axis=0)


def sum8(x):
    return jnp.sum(x.reshape(x.shape[0] // 8, 8, x.shape[1]), axis=0)


def turn(outs):
    t = jnp.transpose(jnp.concatenate(outs, axis=0))
    turned = pltpu.roll(t, HD, 1)
    low = lax.broadcasted_iota(jnp.int32, (SB, LANES), 1) < HD
    tiles = []
    for first, second in ((t, turned), (turned, t)):
        for e in range(0, t.shape[0], 2 * SB):
            tiles.append(jnp.where(low, first[e : e + SB], second[e + SB : e + 2 * SB]))
    return tiles


def near_scores(n, k, b):
    own = (b + 1) * SB
    count = n * k.sum_send.shape[0] // 2
    keys = jnp.concatenate([k.keys[:own], k.sum_keys[:count]], axis=0)
    k.score[b % 2, : own + count] = jnp.dot(keys, k.q_near[b], preferred_element_type=F32)


def near(n, G, R, nb, k, b):
    me = lax.axis_index("kv")
    width = R * SB
    score = k.score.at[b % 2]
    rows = slice(b * SB, (b + 1) * SB)
    shape = (SB, G * width)
    later = lax.broadcasted_iota(jnp.int32, shape, 0) > lax.broadcasted_iota(jnp.int32, shape, 1) % SB

    def bias(j):
        return jnp.concatenate([jnp.full((8, width), k.bias_smem[g, b, j], F32) for g in range(G)], axis=1)

    def block(j):
        s = score[j * SB : (j + 1) * SB]
        return s + jnp.where(later, LOW, 0.0) if j == b else s

    top = None
    for j in range(b + 1):
        t = row8(block(j)) + bias(j)
        top = t if top is None else jnp.maximum(top, t)
    top = jnp.max(top, axis=0, keepdims=True)
    total = jnp.zeros((8, G * width), F32)
    weights = []
    for j in range(b + 1):
        p = jnp.exp(block(j) - (top - bias(j)[:1]))
        total = total + sum8(p)
        weights.append(p.astype(BF16))
    if b % 2 == 0:
        weights.append(jnp.zeros(shape, BF16))
    keys = len(weights) * SB
    weights = jnp.concatenate(weights, axis=0)
    k.top[b] = jnp.broadcast_to(top, k.top.shape[1:])
    k.total[b] = total
    for g in range(G):
        cols = slice(g * width, (g + 1) * width)
        k.part[b, :, cols] = jnp.dot(
            k.vals[g * HD : (g + 1) * HD, :keys], weights[:, cols], preferred_element_type=F32
        )

    slot = k.sum_send.shape[0] // 2
    spans = nb * SB // CMP
    base = (b + 1) * SB
    seen_shape = (slot, G * width)
    span = lax.broadcasted_iota(jnp.int32, seen_shape, 0)
    seen = (span < spans) & (
        span * CMP + (CMP - 1) <= b * SB + lax.broadcasted_iota(jnp.int32, seen_shape, 1) % SB
    )

    def summary(i):
        s = score[base + i * slot : base + (i + 1) * slot]
        return jnp.where(seen, s, LOW) if i == 0 else s

    def gone(i):
        return jnp.where(me >= i, 0.0, LOW).astype(F32)

    top = row8(summary(0))
    for i in range(1, n):
        top = jnp.maximum(top, row8(summary(i)) + gone(i))
    top = jnp.max(top, axis=0, keepdims=True)
    total = jnp.zeros((8, G * width), F32)
    real = spans - spans // 8 * 8
    partial = lax.broadcasted_iota(jnp.int32, (8, G * width), 0) < real
    weights = []
    for i in range(n):
        p = jnp.exp(summary(i) - (top - gone(i)))
        total = total + sum8(p[: spans // 8 * 8])
        if real:
            total = total + jnp.where(partial, p[spans // 8 * 8 :], 0.0)
        weights.append(p)
    more = k.sum_vals.shape[1] - n * slot
    if more:
        weights.append(jnp.zeros((more, G * width), F32))
    weights = jnp.concatenate(weights, axis=0).astype(BF16)
    total = jnp.sum(total, axis=0, keepdims=True)
    scale = jnp.where(top > LOW * 0.5, 1.0 / total, 0.0)
    outs = []
    for g in range(G):
        cols = slice(g * width, (g + 1) * width)
        o = jnp.dot(k.sum_vals[g * HD : (g + 1) * HD, :], weights[:, cols], preferred_element_type=F32)
        outs.append(o * scale[:, cols])
    for t, tile in enumerate(turn(outs)):
        cols = slice(t * LANES, (t + 1) * LANES)
        k.mixed[rows, cols] = tile * k.gate[0, rows, cols]


def far_scores(n, G, k, b, at):
    for g in range(G):
        keys = k.far[:, g, :SB, :].reshape((n - 1) * SB, LANES)
        k.far_score[at, g] = jnp.dot(keys, k.q_far[g, b], preferred_element_type=F32)


def distant(n, G, R, nb, k, b, at):
    width = R * SB
    own = pl.ds(pl.multiple_of(b * SB, SB), SB)
    outs = []
    for g in range(G):
        cols = slice(g * width, (g + 1) * width)

        def bias(i, h):
            return k.bias_smem[g, b, nb + 2 * i + h]

        before = k.top[b, :1, cols]
        top = jnp.broadcast_to(before, (8, width))
        for i in range(n - 1):
            t = row8(k.far_score[at, g, i * SB : (i + 1) * SB])
            for h in range(2):
                top = jnp.maximum(top, t[:, h * width : (h + 1) * width] + bias(i, h))
        top = jnp.max(top, axis=0, keepdims=True)
        keep = jnp.exp(before - top)
        total = k.total[b, :, cols] * keep
        weights = []
        for i in range(n - 1):
            for h in range(2):
                s = k.far_score[at, g, i * SB : (i + 1) * SB, h * width : (h + 1) * width]
                p = jnp.exp(s - (top - bias(i, h)))
                total = total + sum8(p)
                weights.append(p.astype(BF16))
        weights = jnp.concatenate(weights, axis=0)
        vals = jnp.concatenate([k.far[i, g, SB:, :] for i in range(n - 1)], axis=1)
        o = k.part[b, :, cols] * keep + jnp.dot(vals, weights, preferred_element_type=F32)
        outs.append(o * (1.0 / jnp.sum(total, axis=0, keepdims=True)))
    for t, tile in enumerate(turn(outs)):
        cols = slice(t * LANES, (t + 1) * LANES)
        k.att[own, cols] = (k.mixed[own, cols] + tile * k.gate[1, own, cols]).astype(BF16)


def attend_and_mix(n, G, R, nb, cw, k, ow_loads, blocks_done, travel):
    tp = lax.axis_index("tp")
    core = lax.rem(tp, 2)
    side = tp // 2
    partner = side * 2 + 1 - core
    rows = nb * SB
    quarter = rows // 4
    half_blocks = nb // 2
    width = k.base.shape[1]
    chunks = width // cw
    side_cols = width // 2
    step_rows = SB // 2
    att, ow = k.att, k.ow

    near_scores(n, k, 0)
    for b in range(nb):
        if b + 1 < nb:
            near_scores(n, k, b + 1)
        near(n, G, R, nb, k, b)
    for c in ow_loads:
        c.wait()
    travel.relay_x(2)
    blocks_done()

    def d_copy(j):
        return pltpu.make_async_remote_copy(
            src_ref=k.dsend.at[j], dst_ref=k.drecv.at[j],
            send_sem=k.d_s, recv_sem=k.d_r,
            device_id={"tp": partner}, device_id_type=MESH,
        )

    def e_copy(i):
        return pltpu.make_async_remote_copy(
            src_ref=k.esend.at[i], dst_ref=k.erecv.at[i],
            send_sem=k.e_s, recv_sem=k.e_r.at[i],
            device_id={"tp": partner}, device_id_type=MESH,
        )

    def x_copy(i):
        step = i % half_blocks
        return pltpu.make_async_remote_copy(
            src_ref=k.xsend.at[i], dst_ref=k.xrecv.at[core, step],
            send_sem=k.x_s, recv_sem=k.x_r,
            device_id={"tp": (1 - side) * 2 + i // half_blocks}, device_id_type=MESH,
        )

    other_first = (1 - side) * half_blocks

    def a_copy(i):
        to, step = i // half_blocks, i % half_blocks
        rows_of = pl.ds(pl.multiple_of(other_first * SB + i * step_rows, step_rows), step_rows)
        into = pl.ds(pl.multiple_of(step * step_rows, step_rows), step_rows)
        return pltpu.make_async_remote_copy(
            src_ref=att.at[rows_of], dst_ref=k.att_in.at[1 + lax.rem(to + core, 2), into],
            send_sem=k.a_s, recv_sem=k.a_r,
            device_id={"tp": (1 - side) * 2 + to}, device_id_type=MESH,
        )

    own_first = side * half_blocks

    def block(i):
        first = other_first if i < half_blocks else own_first
        return first + i % half_blocks

    def attend(i):
        ahead = k.far_score.shape[0] - 1
        if i + ahead < nb and (ahead or i):
            far_scores(n, G, k, block(i + ahead), (i + ahead) % (ahead + 1))
        distant(n, G, R, nb, k, block(i), i % (ahead + 1))

    def early_block(i):
        attend(i)
        for h in range(2):
            a_copy(2 * i + h).start()
        a = att[pl.ds((other_first + i) * SB, SB), :]
        cols = pl.ds(pl.multiple_of((1 - core) * side_cols, LANES), side_cols)
        k.esend[i] = jnp.dot(a, ow[:, cols], preferred_element_type=F32).astype(BF16)
        e_copy(i).start()
        cols = pl.ds(pl.multiple_of(core * side_cols, LANES), side_cols)
        k.early[i] = jnp.dot(a, ow[:, cols], preferred_element_type=F32).astype(BF16)

    def forward(i):
        e_copy(i).wait_recv()
        for h in range(2):
            r = slice(h * step_rows, (h + 1) * step_rows)
            k.xsend[2 * i + h] = (k.early[i, r].astype(F32) + k.erecv[i, r].astype(F32)).astype(BF16)
            x_copy(2 * i + h).start()

    relays = {
        1: ((travel.relay_x, 3), (travel.relay_y, 0)),
        2: ((travel.relay_y, 1),),
        3: ((travel.relay_z, 0),),
        4: ((travel.relay_z, 1), (travel.relay_y, 2)),
        8: ((travel.relay_g, 0), (travel.relay_z, 2)),
        9: ((travel.relay_g, 1),),
    }
    far_scores(n, G, k, block(0), 0)
    for i in range(nb):
        if i < half_blocks:
            early_block(i)
            if i > 0:
                forward(i - 1)
        else:
            attend(i)
        if i == half_blocks - 1:
            forward(i)
        for relay, j in relays.pop(i, ()):
            relay(j)
    for late in relays.values():
        for relay, j in late:
            relay(j)
    theirs_at = pl.ds(pl.multiple_of(own_first * SB + (1 - core) * quarter, step_rows), quarter)
    ours_at = pl.ds(pl.multiple_of(own_first * SB + core * quarter, step_rows), quarter)
    p_copy = pltpu.make_async_remote_copy(
        src_ref=att.at[theirs_at], dst_ref=k.att_in.at[0], send_sem=k.p_s, recv_sem=k.p_r,
        device_id={"tp": partner}, device_id_type=MESH,
    )
    p_copy.start()

    def own_step(j, carry):
        w = ow[:, pl.ds(pl.multiple_of(j * cw, cw), cw)]
        k.halves[...] = jnp.dot(
            att[pl.ds(pl.multiple_of(own_first * SB, SB), 2 * quarter), :], w, preferred_element_type=F32
        ).astype(BF16)
        k.dsend[j] = k.halves[pl.ds(pl.multiple_of((1 - core) * quarter, step_rows), quarter), :]
        d_copy(j).start()
        k.mine[j] = k.halves[pl.ds(pl.multiple_of(core * quarter, step_rows), quarter), :]
        return carry

    lax.fori_loop(0, chunks, own_step, 0)

    p_copy.wait_recv()
    all_sent(k.att_in.at[pl.ds(1, 2)], k.a_r)
    for q in range(4):
        travel.arrived(q)
        if q == 0:
            travel.p().wait_recv()
        cols, out_cols = travel.quarter(q), travel.quarter(q, travel.first)
        o = jnp.dot(att[ours_at, :], ow[:, out_cols], preferred_element_type=F32)
        for slot in range(3):
            o = o + jnp.dot(k.att_in[slot], k.wfar[slot, :, cols], preferred_element_type=F32)
        k.out[:, out_cols] = o.astype(BF16)
    all_sent(k.drecv, k.d_r)
    all_sent(k.dsend, k.d_s)

    def base_step(j, carry):
        cols = pl.ds(pl.multiple_of(j * cw, cw), cw)
        k.base[:, cols] = k.mine[j].astype(F32) + k.drecv[j].astype(F32)
        return carry

    lax.fori_loop(0, chunks, base_step, 0)

    all_sent(k.xrecv, k.x_r)

    def last_step(s, carry):
        r = pl.ds(pl.multiple_of(s * step_rows, step_rows), step_rows)
        for c in range(2):
            cols = slice(c * side_cols, (c + 1) * side_cols)
            k.out[r, cols] = (k.base[r, cols] + k.xrecv[c, s].astype(F32)).astype(BF16)
        return carry

    lax.fori_loop(0, half_blocks, last_step, 0)
    all_sent(k.esend, k.e_s)
    all_sent(k.xsend, k.x_s)
    all_sent(att.at[pl.ds(0, 2 * quarter)], k.a_s)
    p_copy.wait_send()
    travel.sent()


def layer_kernel(n, G, R, nb, kc, cw, names, *refs):
    k = types.SimpleNamespace(**dict(zip(names, refs, strict=True)))
    ow_loads = [pltpu.make_async_copy(k.ow_hbm, k.ow, k.sem_ow)]
    travel = Travel(k)
    blocks_done = project(n, G, R, nb, kc, k, ow_loads, travel)
    attend_and_mix(n, G, R, nb, cw, k, ow_loads, blocks_done, travel)


def local(
    n,
    tokens, query_weight, key_weight, value_weight, gate_weight,
    summary_pos, key_mixing, value_mixing, out_weight, chosen,
):
    rows, depth = tokens.shape
    heads = query_weight.shape[1] // HD
    G = key_weight.shape[1] // HD
    R = heads // G
    nb = rows // SB
    spans = rows // CMP
    slot = -(-spans // 8) * 8
    all_spans = -(-n * slot // LANES) * LANES
    kc = min(1024, depth)
    chunks = depth // kc
    width = out_weight.shape[1]
    cw = 512
    wide = width // (20 * LANES * 8 // 5) * 20 * LANES
    summed = width - wide
    oc = summed // cw
    gates_all = gate_weight.shape[1]
    assert G == 2 and n % 4 == 0 and 2 * gates_all == LANES and nb % 2 == 0

    vmem = pl.BlockSpec(memory_space=pltpu.VMEM)
    hbm = pl.BlockSpec(memory_space=pl.ANY)
    dma = pltpu.SemaphoreType.DMA
    V = pltpu.VMEM
    nbp = -(-nb // 8) * 8
    quarter = rows // 4
    half = nb // 2
    inputs = ["tok_hbm", "qw_hbm", "kw_hbm", "vw_hbm", "gw_hbm", "chosen_hbm", "km_hbm", "vm_hbm", "pos_hbm", "ow_hbm"]
    scratch = {
        "q_near": V((nb, G * HD, G * R * SB), BF16),
        "q_far": V((G, nb, 2 * HD, 2 * R * SB), BF16),
        "chosen": V(chosen.shape, jnp.int32),
        "km": V(key_mixing.shape[::-1], BF16),
        "vm": V(value_mixing.shape[::-1], BF16),
        "pos": V(summary_pos.shape, BF16),
        "sem_small": dma((4,)),
        "tok": V((rows, depth), BF16),
        "qw": V((depth, heads * HD), BF16),
        "kvw": V((depth, 2 * LANES), BF16),
        "gw": V((LANES, depth), BF16),
        "ow": V(out_weight.shape, BF16),
        "acc": V((rows, heads * HD), F32),
        "gacc": V((rows, LANES), F32),
        "gate": V((2, rows, heads * HD), F32),
        "keys": V((rows, LANES), BF16),
        "vals": V((LANES, rows), BF16),
        "left": V((G * nb, 2 * SB, LANES), BF16),
        "right": V((G * nb, 2 * SB, LANES), BF16),
        "named": V((G, nbp, LANES), jnp.int32),
        "bias": V((G, nbp, LANES), F32),
        "bias_smem": pltpu.SMEM((G, nbp, LANES), F32),
        "pos_wide": V((CMP, LANES), F32),
        "req": V((n, 8, LANES), jnp.int32),
        "req_in": V((n, 8, LANES), jnp.int32),
        "req_smem": pltpu.SMEM((n, 8, LANES), jnp.int32),
        "send": V((n, G, 2 * SB, LANES), BF16),
        "far": V((n - 1, G, 2 * SB, LANES), BF16),
        "sum_send": V((2 * slot, LANES), BF16),
        "sum_in": V((n, 2 * slot, LANES), BF16),
        "sum_key": V((all_spans, LANES), F32),
        "sum_val": V((all_spans, LANES), F32),
        "sum_keys": V((all_spans, LANES), BF16),
        "sum_vals": V((LANES, all_spans), BF16),
        "score": V((2, rows + n * slot, heads * HD), F32),
        "far_score": V((2 if n <= 16 else 1, G, (n - 1) * SB, 2 * R * SB), F32),
        "top": V((nb, 8, heads * HD), F32),
        "total": V((nb, 8, heads * HD), F32),
        "part": V((nb, HD, heads * HD), F32),
        "mixed": V((rows, heads * HD), F32),
        "att": V((rows, heads * HD), BF16),
        "halves": V((2 * quarter, cw), BF16),
        "mine": V((oc, quarter, cw), BF16),
        "dsend": V((oc, quarter, cw), BF16),
        "drecv": V((oc, quarter, cw), BF16),
        "early": V((half, SB, summed // 2), BF16),
        "esend": V((half, SB, summed // 2), BF16),
        "erecv": V((half, SB, summed // 2), BF16),
        "xsend": V((2 * half, SB // 2, summed // 2), BF16),
        "xrecv": V((2, half, SB // 2, summed // 2), BF16),
        "base": V((quarter, summed), F32),
        "wfar": V((3, out_weight.shape[0], wide), BF16),
        "att_in": V((3, quarter, heads * HD), BF16),
        "sem_ow": dma,
        "sem_bias": dma,
        "sem_req": dma((n,)),
        "sem_tok": dma((chunks,)), "sem_kw": dma((chunks,)), "sem_vw": dma((chunks,)),
        "req_s": dma, "req_r": dma((n,)), "blk_s": dma((n,)), "blk_r": dma((n,)),
        "sum_s": dma((n,)), "sum_r": dma((n,)),
        "d_s": dma, "d_r": dma, "e_s": dma, "e_r": dma((half,)), "x_s": dma, "x_r": dma,
        "a_s": dma, "a_r": dma, "p_s": dma, "p_r": dma,
        "wx_s": dma, "wx_r": dma((4,)), "wp_s": dma, "wp_r": dma,
        "wy_s": dma, "wy_r": dma((3,)), "wz_s": dma, "wz_r": dma((3,)),
        "wg_s": dma, "wg_r": dma((2,)), "wd_s": dma, "wd_r": dma((4,)),
    }
    return pl.pallas_call(
        functools.partial(layer_kernel, n, G, R, nb, kc, cw, inputs + ["out"] + list(scratch)),
        name="layer",
        out_shape=pltpu.VMEM((quarter, width), BF16),
        in_specs=[hbm] * 10,
        out_specs=vmem,
        scratch_shapes=list(scratch.values()),
        compiler_params=pltpu.CompilerParams(
            collective_id=1, has_side_effects=True, vmem_limit_bytes=VMEM_LIMIT
        ),
    )(
        tokens, query_weight, key_weight, value_weight, gate_weight.T,
        chosen, key_mixing.T, value_mixing.T, summary_pos, out_weight,
    )


def solution(mesh):
    placed = (
        P("kv", None),
        P(None, "tp"),
        P(None, "tp"),
        P(None, "tp"),
        P(),
        P(),
        P(),
        P(),
        P("tp", None),
        P("kv", "tp", None),
    )
    return jax.shard_map(
        functools.partial(local, mesh.shape["kv"]),
        mesh=mesh, in_specs=placed, out_specs=P(("kv", "tp"), None), check_vma=False,
    )
```

```python
import functools
import types

import jax
import jax.numpy as jnp
from jax import lax
from jax.experimental import pallas as pl
from jax.experimental.pallas import tpu as pltpu
from jax.sharding import PartitionSpec as P

HD = 64
CMP = 32
SB = 64
N_SEL = 16
LANES = 128
LOW = -1e30
F32 = jnp.float32
BF16 = jnp.bfloat16
MESH = pl.DeviceIdType.MESH
VMEM_LIMIT = 64_000_000
NT = (((1,), (1,)), ((), ()))


def all_sent(ref, sem):
    pltpu.make_async_copy(ref, ref, sem).wait()


def requests(n, G, nb, k):
    place = lax.broadcasted_iota(jnp.int32, k.named.shape, 1)
    for g in range(G):
        k.named[g] = jnp.full(k.named.shape[1:], -1, jnp.int32)
        k.named[g, :nb, :N_SEL] = k.chosen[:, g, :]
        c = k.named[g]
        source = jnp.zeros_like(c)
        for s in range(1, n):
            source = source + jnp.where(c >= s * nb, 1, 0)
        inside = c - source * nb
        for s in range(n):
            hit = (c >= 0) & (source == s)
            lo = jnp.where(hit, inside, nb)
            lo = jnp.min(jnp.min(lo, axis=0, keepdims=True), axis=1, keepdims=True)
            lo = jnp.where(lo == nb, 0, lo)
            hi = jnp.where(hit, inside, 0)
            hi = jnp.max(jnp.max(hi, axis=0, keepdims=True), axis=1, keepdims=True)
            k.req[s, 2 * g : 2 * g + 1] = jnp.broadcast_to(lo, (1, LANES))
            k.req[s, 2 * g + 1 : 2 * g + 2] = jnp.broadcast_to(hi, (1, LANES))


def biases(n, G, nb, k, me):
    for g in range(G):
        c = k.named[g]
        lane = lax.broadcasted_iota(jnp.int32, c.shape, 1)
        bias = jnp.full(c.shape, LOW, F32)

        def mark(bias, hit, at):
            hit = jnp.max(jnp.where(hit, 1.0, 0.0), axis=1, keepdims=True)
            return jnp.where((lane == at) & (hit > 0.0), 0.0, bias)

        for j in range(nb):
            bias = mark(bias, c == me * nb + j, j)
        for s in range(n - 1):
            lo = k.req[s, 2 * g : 2 * g + 1]
            hi = k.req[s, 2 * g + 1 : 2 * g + 2]
            at = jnp.where(me > s, nb + 2 * (me - s - 1), -5)
            real = c >= 0
            bias = mark(bias, real & (c == s * nb + lo), at)
            bias = mark(bias, real & (c == s * nb + hi) & (hi != lo), at + 1)
        k.bias[g] = bias


class Travel:
    SPLIT = ((0, 1), (1, 2), (3, 1), (4, 1))

    def __init__(self, k):
        tp, me = lax.axis_index("tp"), lax.axis_index("kv")
        core, side = lax.rem(tp, 2), tp // 2
        place = lax.rem(me, 4)
        odd, upper = lax.rem(place, 2), place // 2
        self.k = k
        self.across = {"tp": (1 - side) * 2 + core}
        self.partner = {"tp": side * 2 + 1 - core}
        self.first_of = {"kv": me + 1 - 2 * odd}
        self.second_of = {"kv": me + 2 - 4 * upper}
        self.own, self.by_first, self.by_second, self.last = (
            place, place + 1 - 2 * odd, place + 2 - 4 * upper, 3 - place,
        )
        self.columns = k.wfar.shape[2]
        self.first = k.ow.shape[1] - self.columns

    def cols(self, quarter, j, base=0):
        unit = self.columns // 20
        at, size = self.SPLIT[j]
        return pl.ds(pl.multiple_of(base + (quarter * 5 + at) * unit, LANES), size * unit)

    def copy(self, src, dst, send, recv, target):
        return pltpu.make_async_remote_copy(
            src_ref=src, dst_ref=dst, send_sem=send, recv_sem=recv,
            device_id=target, device_id_type=MESH,
        )

    def x(self, j):
        k = self.k
        quarter, piece = (self.own, j) if j < 4 else (self.last, 3)
        return self.copy(
            k.ow_hbm.at[:, self.cols(quarter, piece, self.first)], k.wfar.at[1, :, self.cols(quarter, piece)],
            k.wx_s, k.wx_r.at[j], self.across,
        )

    def p(self):
        k = self.k
        return self.copy(
            k.ow_hbm.at[:, pl.ds(self.first, self.columns)], k.wfar.at[0], k.wp_s, k.wp_r, self.partner
        )

    def pass_on(self, quarter, j, sems, at, target):
        here = self.k.wfar.at[1, :, self.cols(quarter, j)]
        return self.copy(here, here, sems[0], sems[1].at[at], target)

    def y(self, j, arrival=False):
        return self.pass_on(self.by_first if arrival else self.own, j, (self.k.wy_s, self.k.wy_r), j, self.first_of)

    def z(self, j, arrival=False):
        return self.pass_on(self.by_second if arrival else self.own, j, (self.k.wz_s, self.k.wz_r), j, self.second_of)

    def g(self, j, arrival=False):
        return self.pass_on(self.last if arrival else self.by_second, j, (self.k.wg_s, self.k.wg_r), j, self.first_of)

    def h(self, arrival=False):
        return self.pass_on(self.last if arrival else self.by_first, 2, (self.k.wh_s, self.k.wh_r), 0, self.second_of)

    def d(self, q, j):
        k = self.k
        at = self.cols((self.own, self.by_first, self.by_second, self.last)[q], j)
        return self.copy(
            k.wfar.at[1, :, at], k.wfar.at[2, :, at], k.wd_s, k.wd_r.at[q], self.partner
        )

    def start(self):
        for j in range(5):
            self.x(j).start()
        self.p().start()

    def relay_x(self, j):
        self.x(j).wait_recv()
        if j < 4:
            self.z(j).start()
            self.y(j).start()
            self.d(0, j).start()
        else:
            self.d(3, 3).start()

    def relay_y(self, j):
        self.y(j, True).wait_recv()
        if j == 2:
            self.h().start()
        self.d(1, j).start()

    def relay_z(self, j):
        self.z(j, True).wait_recv()
        if j < 2:
            self.g(j).start()
        self.d(2, j).start()

    def relay_h(self):
        self.h(True).wait_recv()
        self.d(3, 2).start()

    def relay_g(self, j):
        self.g(j, True).wait_recv()
        self.d(3, j).start()

    def quarter(self, q, base=0):
        unit = self.columns // 20
        at = base + (self.own, self.by_first, self.by_second, self.last)[q] * 5 * unit
        return pl.ds(pl.multiple_of(at, LANES), 5 * unit)

    def arrived(self, q):
        all_sent(self.k.wfar.at[2, :, self.quarter(q)], self.k.wd_r.at[q])

    def sent(self):
        k, unit = self.k, self.columns // 20
        self.p().wait_send()
        for sem, size in ((k.wx_s, 6), (k.wy_s, 5), (k.wz_s, 5), (k.wg_s, 3), (k.wh_s, 1), (k.wd_s, 20)):
            all_sent(k.wfar.at[1, :, pl.ds(0, size * unit)], sem)


def project(n, G, R, nb, kc, k, ow_loads, travel):
    tp = lax.axis_index("tp")
    me = lax.axis_index("kv")
    rows = nb * SB
    depth = k.tok.shape[1]
    chunks = depth // kc
    spans = rows // CMP
    slot = k.sum_send.shape[0] // 2

    def part(i):
        return pl.ds(i * kc, kc)

    def loads(i):
        return [
            pltpu.make_async_copy(k.tok_hbm.at[:, part(i)], k.tok.at[:, part(i)], k.sem_tok.at[i]),
            pltpu.make_async_copy(k.kw_hbm.at[part(i)], k.kvw.at[part(i), pl.ds(0, LANES)], k.sem_kw.at[i]),
            pltpu.make_async_copy(k.vw_hbm.at[part(i)], k.kvw.at[part(i), pl.ds(LANES, LANES)], k.sem_vw.at[i]),
        ]

    half_gates = k.gw.shape[0] // 2

    def late(i):
        return [
            pltpu.make_async_copy(k.qw_hbm.at[part(i)], k.qw.at[part(i)], k.sem_tok.at[i]),
            pltpu.make_async_copy(k.gw_hbm.at[:, part(i)], k.gw.at[pl.ds(0, half_gates), part(i)], k.sem_kw.at[i]),
            pltpu.make_async_copy(k.gw_hbm.at[:, part(i)], k.gw.at[pl.ds(half_gates, half_gates), part(i)], k.sem_vw.at[i]),
        ]

    small = [
        pltpu.make_async_copy(src, dst, k.sem_small.at[i])
        for i, (src, dst) in enumerate((
            (k.chosen_hbm, k.chosen), (k.km_hbm, k.km), (k.vm_hbm, k.vm), (k.pos_hbm, k.pos),
        ))
    ]
    for c in small:
        c.start()
    for i in range(chunks):
        for c in loads(i):
            c.start()

    barrier = pltpu.get_barrier_semaphore()
    for i in range(1, n):
        pl.semaphore_signal(
            barrier, inc=1, device_id={"kv": lax.rem(me + i, n)}, device_id_type=MESH
        )
    for i in range(1, 4):
        pl.semaphore_signal(barrier, inc=1, device_id={"tp": lax.rem(tp + i, 4)}, device_id_type=MESH)

    small[0].wait()
    requests(n, G, nb, k)
    pl.semaphore_wait(barrier, n + 2)

    def req_copy(i):
        return pltpu.make_async_remote_copy(
            src_ref=k.req.at[lax.rem(me + n - i, n)], dst_ref=k.req_in.at[i],
            send_sem=k.req_s, recv_sem=k.req_r.at[i],
            device_id={"kv": lax.rem(me + n - i, n)}, device_id_type=MESH,
        )

    def req_local(i):
        return pltpu.make_async_copy(k.req_in.at[i], k.req_smem.at[i], k.sem_req.at[i])

    def blk_copy(i):
        return pltpu.make_async_remote_copy(
            src_ref=k.send.at[i], dst_ref=k.far.at[i - 1],
            send_sem=k.blk_s.at[i], recv_sem=k.blk_r.at[i],
            device_id={"kv": lax.rem(me + i, n)}, device_id_type=MESH,
        )

    def sum_copy(i):
        return pltpu.make_async_remote_copy(
            src_ref=k.sum_send, dst_ref=k.sum_in.at[i],
            send_sem=k.sum_s.at[i], recv_sem=k.sum_r.at[i],
            device_id={"kv": lax.rem(me + i, n)}, device_id_type=MESH,
        )

    for i in range(1, n):
        req_copy(i).start()
    travel.start()

    biases(n, G, nb, k, me)
    bias_copy = pltpu.make_async_copy(k.bias, k.bias_smem, k.sem_bias)
    bias_copy.start()
    for i in range(1, n):

        @pl.when(me < i)
        def _():
            k.far[i - 1] = jnp.zeros(k.far.shape[1:], BF16)

    k.q_near[...] = jnp.zeros_like(k.q_near)
    k.q_far[...] = jnp.zeros_like(k.q_far)
    k.sum_key[...] = jnp.zeros_like(k.sum_key)
    k.sum_val[...] = jnp.zeros_like(k.sum_val)
    k.acc[:, : 2 * LANES] = jnp.zeros((rows, 2 * LANES), F32)

    def kv_step(i, carry):
        for c in loads(i):
            c.wait()
        for c in late(i):
            c.start()
        k.acc[:, : 2 * LANES] += jnp.dot(k.tok[:, part(i)], k.kvw[part(i), :], preferred_element_type=F32)
        return carry

    lax.fori_loop(0, chunks, kv_step, 0)
    for c in ow_loads:
        c.start()
    for c in small[1:]:
        c.wait()
    low = lax.broadcasted_iota(jnp.int32, (SB, LANES), 1) < HD
    mix_row = lax.broadcasted_iota(jnp.int32, k.km.shape, 0)
    mix_low = lax.broadcasted_iota(jnp.int32, (CMP, LANES), 1) < HD
    diagonal = lax.broadcasted_iota(jnp.int32, (CMP, CMP), 0) == lax.broadcasted_iota(
        jnp.int32, (CMP, CMP), 1
    )

    def mix_column(ref, head):
        line = jnp.where(mix_row == head, ref[...].astype(F32), 0.0)
        line = jnp.sum(line, axis=0, keepdims=True)
        return jnp.sum(jnp.where(diagonal, line, 0.0), axis=1, keepdims=True)

    k.pos_wide[:, :HD] = k.pos[...].astype(F32)
    k.pos_wide[:, HD:] = k.pos[...].astype(F32)
    both = []
    for ref, at, more in ((k.km, 0, 1.0), (k.vm, LANES, 0.0)):
        mix = jnp.where(mix_low, mix_column(ref, tp * G), mix_column(ref, tp * G + 1))
        t = k.acc[:, at : at + LANES].astype(BF16).astype(F32).reshape(spans, CMP, LANES)
        s = jnp.sum((t + k.pos_wide[...][None]) * mix[None], axis=1)
        if slot > spans:
            s = jnp.concatenate([s, s[: slot - spans] * more], axis=0)
        both.append(s)
    both = jnp.concatenate(both, axis=0).astype(BF16)
    k.sum_send[...] = both
    k.sum_key[:slot] = both.astype(F32)[:slot]
    k.sum_val[:slot] = both.astype(F32)[slot:]
    for i in range(1, n):

        @pl.when(me + i < n)
        def _():
            sum_copy(i).start()

    for t in range(nb // 2):
        r0 = slice(t * LANES, (t + 1) * LANES)
        keys = k.acc[r0, :LANES].astype(BF16).astype(F32)
        vals = jnp.transpose(k.acc[r0, LANES : 2 * LANES].astype(BF16).astype(F32))
        k.keys[r0, :] = keys.astype(BF16)
        k.vals[:, r0] = vals.astype(BF16)
        keys_r = pltpu.roll(keys, HD, 1)
        vals_r = pltpu.roll(vals, HD, 1)
        for h in range(2):
            kk, kr = keys[h * SB : (h + 1) * SB], keys_r[h * SB : (h + 1) * SB]
            v_left, v_right = (vals, vals_r) if h == 0 else (vals_r, vals)
            for g in range(G):
                left, right = (kk, kr) if g == 0 else (kr, kk)
                v = slice(g * HD, (g + 1) * HD)
                c = g * nb + 2 * t + h
                k.left[c, :SB] = jnp.where(low, left, 0.0).astype(BF16)
                k.left[c, SB:] = jnp.where(low, v_left[v], 0.0).astype(BF16)
                k.right[c, :SB] = jnp.where(low, 0.0, right).astype(BF16)
                k.right[c, SB:] = jnp.where(low, 0.0, v_right[v]).astype(BF16)
    first = range(1, min(4, n))
    for i in first:
        req_copy(i).wait_recv()
        req_local(i).start()
    def answer(i):
        req_local(i).wait()

        @pl.when(me + i < n)
        def _():
            for g in range(G):
                lo = k.req_smem[i, 2 * g, 0]
                hi = k.req_smem[i, 2 * g + 1, 0]
                k.send[i, g] = k.left[g * nb + lo] + k.right[g * nb + hi]
            blk_copy(i).start()

    for i in reversed(first):
        answer(i)
    k.acc[...] = jnp.zeros_like(k.acc)
    k.gacc[...] = jnp.zeros_like(k.gacc)

    def q_step(i, carry):
        for c in late(i):
            c.wait()
        k.acc[...] += jnp.dot(k.tok[:, part(i)], k.qw[part(i), :], preferred_element_type=F32)
        k.gacc[...] += lax.dot_general(
            k.tok[:, part(i)], k.gw[:, part(i)], NT, preferred_element_type=F32
        )
        return carry

    q_step(0, 0)
    for i in range(len(first) + 1, n):
        req_copy(i).wait_recv()
        req_local(i).start()
    for i in range(n - 1, len(first), -1):
        answer(i)
    travel.relay_x(0)
    lax.fori_loop(1, chunks, q_step, 0)
    wide_low = lax.broadcasted_iota(jnp.int32, k.gacc.shape, 1) < half_gates
    gates = jax.nn.sigmoid(k.gacc[...])
    gates_hi = gates.astype(BF16).astype(F32)
    gates = jnp.where(wide_low, gates_hi, gates - gates_hi).astype(BF16)
    spread_row = lax.broadcasted_iota(jnp.int32, (LANES, G * R * HD), 0)
    spread_col = lax.broadcasted_iota(jnp.int32, (LANES, G * R * HD), 1)
    spread_at = (tp * G * R + spread_col // HD) * 2
    for branch in range(2):
        spread = jnp.where(spread_row % half_gates == spread_at + branch, 1.0, 0.0).astype(BF16)
        k.gate[branch] = jnp.dot(gates, spread, preferred_element_type=F32)

    tall_low = lax.broadcasted_iota(jnp.int32, (HD, LANES), 1) < SB

    def query_step(t, carry):
        r0 = pl.ds(pl.multiple_of(t * LANES, LANES), LANES)
        for g in range(G):
            for pair in range(R // 2):
                at = (g * R // 2 + pair) * LANES
                x = jnp.transpose(k.acc[r0, at : at + LANES].astype(BF16).astype(F32) * (HD ** -0.5))
                turned = pltpu.roll(x, SB, 1)
                for h, (left, right) in enumerate(((x, turned), (turned, x))):
                    y = jnp.where(tall_low, left[:HD], right[HD:]).astype(BF16)
                    lo = slice(pair * LANES, (pair + 1) * LANES)
                    hi = slice(R * SB + pair * LANES, R * SB + (pair + 1) * LANES)
                    k.q_near[2 * t + h, g * HD : (g + 1) * HD, g * R * SB + pair * LANES : g * R * SB + (pair + 1) * LANES] = y
                    k.q_far[g, 2 * t + h, :HD, lo] = y
                    k.q_far[g, 2 * t + h, HD:, hi] = y
        return carry

    lax.fori_loop(0, nb // 2, query_step, 0)
    travel.relay_x(1)
    bias_copy.wait()
    all_sent(k.req.at[pl.ds(0, n - 1)], k.req_s)
    for i in range(1, n):

        @pl.when(me + i < n)
        def _():
            sum_copy(i).wait_send()

        @pl.when(me - i >= 0)
        def _():
            sum_copy(i).wait_recv()
            both = k.sum_in[i].astype(F32)
            k.sum_key[i * slot : (i + 1) * slot] = both[:slot]
            k.sum_val[i * slot : (i + 1) * slot] = both[slot:]

    k.sum_keys[...] = k.sum_key[...].astype(BF16)
    k.sum_vals[...] = jnp.transpose(k.sum_val[...]).astype(BF16)
    def blocks_done():
        for i in range(1, n):

            @pl.when(me + i < n)
            def _():
                blk_copy(i).wait_send()

            @pl.when(me - i >= 0)
            def _():
                blk_copy(i).wait_recv()

    return blocks_done


def row8(x):
    return jnp.max(x.reshape(x.shape[0] // 8, 8, x.shape[1]), axis=0)


def sum8(x):
    return jnp.sum(x.reshape(x.shape[0] // 8, 8, x.shape[1]), axis=0)


def turn(outs):
    t = jnp.transpose(jnp.concatenate(outs, axis=0))
    turned = pltpu.roll(t, HD, 1)
    low = lax.broadcasted_iota(jnp.int32, (SB, LANES), 1) < HD
    tiles = []
    for first, second in ((t, turned), (turned, t)):
        for e in range(0, t.shape[0], 2 * SB):
            tiles.append(jnp.where(low, first[e : e + SB], second[e + SB : e + 2 * SB]))
    return tiles


def near_scores(n, k, b):
    own = (b + 1) * SB
    count = n * k.sum_send.shape[0] // 2
    keys = jnp.concatenate([k.keys[:own], k.sum_keys[:count]], axis=0)
    k.score[b % 2, : own + count] = jnp.dot(keys, k.q_near[b], preferred_element_type=F32)


def near(n, G, R, nb, k, b):
    me = lax.axis_index("kv")
    width = R * SB
    score = k.score.at[b % 2]
    rows = slice(b * SB, (b + 1) * SB)
    shape = (SB, G * width)
    later = lax.broadcasted_iota(jnp.int32, shape, 0) > lax.broadcasted_iota(jnp.int32, shape, 1) % SB

    def bias(j):
        return jnp.concatenate([jnp.full((8, width), k.bias_smem[g, b, j], F32) for g in range(G)], axis=1)

    def block(j):
        s = score[j * SB : (j + 1) * SB]
        return s + jnp.where(later, LOW, 0.0) if j == b else s

    top = None
    for j in range(b + 1):
        t = row8(block(j)) + bias(j)
        top = t if top is None else jnp.maximum(top, t)
    top = jnp.max(top, axis=0, keepdims=True)
    total = jnp.zeros((8, G * width), F32)
    weights = []
    for j in range(b + 1):
        p = jnp.exp(block(j) - (top - bias(j)[:1]))
        total = total + sum8(p)
        weights.append(p.astype(BF16))
    if b % 2 == 0:
        weights.append(jnp.zeros(shape, BF16))
    keys = len(weights) * SB
    weights = jnp.concatenate(weights, axis=0)
    k.top[b] = jnp.broadcast_to(top, k.top.shape[1:])
    k.total[b] = total
    for g in range(G):
        cols = slice(g * width, (g + 1) * width)
        k.part[b, :, cols] = jnp.dot(
            k.vals[g * HD : (g + 1) * HD, :keys], weights[:, cols], preferred_element_type=F32
        )

    slot = k.sum_send.shape[0] // 2
    spans = nb * SB // CMP
    base = (b + 1) * SB
    seen_shape = (slot, G * width)
    span = lax.broadcasted_iota(jnp.int32, seen_shape, 0)
    seen = (span < spans) & (
        span * CMP + (CMP - 1) <= b * SB + lax.broadcasted_iota(jnp.int32, seen_shape, 1) % SB
    )

    def summary(i):
        s = score[base + i * slot : base + (i + 1) * slot]
        return jnp.where(seen, s, LOW) if i == 0 else s

    def gone(i):
        return jnp.where(me >= i, 0.0, LOW).astype(F32)

    top = row8(summary(0))
    for i in range(1, n):
        top = jnp.maximum(top, row8(summary(i)) + gone(i))
    top = jnp.max(top, axis=0, keepdims=True)
    total = jnp.zeros((8, G * width), F32)
    real = spans - spans // 8 * 8
    partial = lax.broadcasted_iota(jnp.int32, (8, G * width), 0) < real
    weights = []
    for i in range(n):
        p = jnp.exp(summary(i) - (top - gone(i)))
        total = total + sum8(p[: spans // 8 * 8])
        if real:
            total = total + jnp.where(partial, p[spans // 8 * 8 :], 0.0)
        weights.append(p)
    more = k.sum_vals.shape[1] - n * slot
    if more:
        weights.append(jnp.zeros((more, G * width), F32))
    weights = jnp.concatenate(weights, axis=0).astype(BF16)
    total = jnp.sum(total, axis=0, keepdims=True)
    scale = jnp.where(top > LOW * 0.5, 1.0 / total, 0.0)
    outs = []
    for g in range(G):
        cols = slice(g * width, (g + 1) * width)
        o = jnp.dot(k.sum_vals[g * HD : (g + 1) * HD, :], weights[:, cols], preferred_element_type=F32)
        outs.append(o * scale[:, cols])
    for t, tile in enumerate(turn(outs)):
        cols = slice(t * LANES, (t + 1) * LANES)
        k.mixed[rows, cols] = tile * k.gate[0, rows, cols]


def far_scores(n, G, k, b, at):
    for g in range(G):
        keys = k.far[:, g, :SB, :].reshape((n - 1) * SB, LANES)
        k.far_score[at, g] = jnp.dot(keys, k.q_far[g, b], preferred_element_type=F32)


def distant(n, G, R, nb, k, b, at):
    width = R * SB
    own = pl.ds(pl.multiple_of(b * SB, SB), SB)
    outs = []
    for g in range(G):
        cols = slice(g * width, (g + 1) * width)

        def bias(i, h):
            return k.bias_smem[g, b, nb + 2 * i + h]

        before = k.top[b, :1, cols]
        top = jnp.broadcast_to(before, (8, width))
        for i in range(n - 1):
            t = row8(k.far_score[at, g, i * SB : (i + 1) * SB])
            for h in range(2):
                top = jnp.maximum(top, t[:, h * width : (h + 1) * width] + bias(i, h))
        top = jnp.max(top, axis=0, keepdims=True)
        keep = jnp.exp(before - top)
        total = k.total[b, :, cols] * keep
        weights = []
        for i in range(n - 1):
            for h in range(2):
                s = k.far_score[at, g, i * SB : (i + 1) * SB, h * width : (h + 1) * width]
                p = jnp.exp(s - (top - bias(i, h)))
                total = total + sum8(p)
                weights.append(p.astype(BF16))
        weights = jnp.concatenate(weights, axis=0)
        vals = jnp.concatenate([k.far[i, g, SB:, :] for i in range(n - 1)], axis=1)
        o = k.part[b, :, cols] * keep + jnp.dot(vals, weights, preferred_element_type=F32)
        outs.append(o * (1.0 / jnp.sum(total, axis=0, keepdims=True)))
    for t, tile in enumerate(turn(outs)):
        cols = slice(t * LANES, (t + 1) * LANES)
        k.att[own, cols] = (k.mixed[own, cols] + tile * k.gate[1, own, cols]).astype(BF16)


def attend_and_mix(n, G, R, nb, cw, k, ow_loads, blocks_done, travel):
    tp = lax.axis_index("tp")
    core = lax.rem(tp, 2)
    side = tp // 2
    partner = side * 2 + 1 - core
    rows = nb * SB
    quarter = rows // 4
    half_blocks = nb // 2
    width = k.base.shape[1]
    chunks = width // cw
    side_cols = width // 2
    step_rows = SB // 2
    att, ow = k.att, k.ow

    near_scores(n, k, 0)
    for b in range(nb):
        if b + 1 < nb:
            near_scores(n, k, b + 1)
        near(n, G, R, nb, k, b)
    for c in ow_loads:
        c.wait()
    travel.relay_x(2)
    travel.relay_x(3)
    blocks_done()

    def d_copy(j):
        return pltpu.make_async_remote_copy(
            src_ref=k.dsend.at[j], dst_ref=k.drecv.at[j],
            send_sem=k.d_s, recv_sem=k.d_r,
            device_id={"tp": partner}, device_id_type=MESH,
        )

    def e_copy(i):
        return pltpu.make_async_remote_copy(
            src_ref=k.esend.at[i], dst_ref=k.erecv.at[i],
            send_sem=k.e_s, recv_sem=k.e_r.at[i],
            device_id={"tp": partner}, device_id_type=MESH,
        )

    def x_copy(i):
        step = i % half_blocks
        return pltpu.make_async_remote_copy(
            src_ref=k.xsend.at[i], dst_ref=k.xrecv.at[core, step],
            send_sem=k.x_s, recv_sem=k.x_r,
            device_id={"tp": (1 - side) * 2 + i // half_blocks}, device_id_type=MESH,
        )

    other_first = (1 - side) * half_blocks

    def a_copy(i):
        to, step = i // half_blocks, i % half_blocks
        rows_of = pl.ds(pl.multiple_of(other_first * SB + i * step_rows, step_rows), step_rows)
        into = pl.ds(pl.multiple_of(step * step_rows, step_rows), step_rows)
        return pltpu.make_async_remote_copy(
            src_ref=att.at[rows_of], dst_ref=k.att_in.at[1 + lax.rem(to + core, 2), into],
            send_sem=k.a_s, recv_sem=k.a_r,
            device_id={"tp": (1 - side) * 2 + to}, device_id_type=MESH,
        )

    own_first = side * half_blocks

    def block(i):
        first = other_first if i < half_blocks else own_first
        return first + i % half_blocks

    def attend(i):
        ahead = k.far_score.shape[0] - 1
        if i + ahead < nb and (ahead or i):
            far_scores(n, G, k, block(i + ahead), (i + ahead) % (ahead + 1))
        distant(n, G, R, nb, k, block(i), i % (ahead + 1))

    def early_block(i):
        attend(i)
        for h in range(2):
            a_copy(2 * i + h).start()
        a = att[pl.ds((other_first + i) * SB, SB), :]
        cols = pl.ds(pl.multiple_of((1 - core) * side_cols, LANES), side_cols)
        k.esend[i] = jnp.dot(a, ow[:, cols], preferred_element_type=F32).astype(BF16)
        e_copy(i).start()
        cols = pl.ds(pl.multiple_of(core * side_cols, LANES), side_cols)
        k.early[i] = jnp.dot(a, ow[:, cols], preferred_element_type=F32).astype(BF16)

    def forward(i):
        e_copy(i).wait_recv()
        for h in range(2):
            r = slice(h * step_rows, (h + 1) * step_rows)
            k.xsend[2 * i + h] = (k.early[i, r].astype(F32) + k.erecv[i, r].astype(F32)).astype(BF16)
            x_copy(2 * i + h).start()

    relays = {
        1: ((travel.relay_x, 4),),
        2: ((travel.relay_y, 0), (travel.relay_y, 1)),
        3: ((travel.relay_z, 0),),
        4: ((travel.relay_y, 2), (travel.relay_y, 3)),
    }
    far_scores(n, G, k, block(0), 0)
    for i in range(nb):
        if i < half_blocks:
            early_block(i)
            if i > 0:
                forward(i - 1)
        else:
            attend(i)
        if i == half_blocks - 1:
            forward(i)
        for relay, j in relays.pop(i, ()):
            relay(j)
    for late in relays.values():
        for relay, j in late:
            relay(j)
    theirs_at = pl.ds(pl.multiple_of(own_first * SB + (1 - core) * quarter, step_rows), quarter)
    ours_at = pl.ds(pl.multiple_of(own_first * SB + core * quarter, step_rows), quarter)
    p_copy = pltpu.make_async_remote_copy(
        src_ref=att.at[theirs_at], dst_ref=k.att_in.at[0], send_sem=k.p_s, recv_sem=k.p_r,
        device_id={"tp": partner}, device_id_type=MESH,
    )
    p_copy.start()
    travel.relay_z(1)

    def own_step(j, carry):
        w = ow[:, pl.ds(pl.multiple_of(j * cw, cw), cw)]
        k.halves[...] = jnp.dot(
            att[pl.ds(pl.multiple_of(own_first * SB, SB), 2 * quarter), :], w, preferred_element_type=F32
        ).astype(BF16)
        k.dsend[j] = k.halves[pl.ds(pl.multiple_of((1 - core) * quarter, step_rows), quarter), :]
        d_copy(j).start()
        k.mine[j] = k.halves[pl.ds(pl.multiple_of(core * quarter, step_rows), quarter), :]
        return carry

    lax.fori_loop(0, chunks, own_step, 0)

    p_copy.wait_recv()
    all_sent(k.att_in.at[pl.ds(1, 2)], k.a_r)
    travel.p().wait_recv()

    def wide(q):
        travel.arrived(q)
        cols, out_cols = travel.quarter(q), travel.quarter(q, travel.first)
        o = jnp.dot(att[ours_at, :], ow[:, out_cols], preferred_element_type=F32)
        for slot in range(3):
            o = o + jnp.dot(k.att_in[slot], k.wfar[slot, :, cols], preferred_element_type=F32)
        k.out[:, out_cols] = o.astype(BF16)

    wide(0)
    wide(1)
    all_sent(k.drecv, k.d_r)
    all_sent(k.dsend, k.d_s)

    def base_step(j, carry):
        cols = pl.ds(pl.multiple_of(j * cw, cw), cw)
        k.base[:, cols] = k.mine[j].astype(F32) + k.drecv[j].astype(F32)
        return carry

    lax.fori_loop(0, chunks, base_step, 0)

    travel.relay_g(0)
    travel.relay_z(2)
    travel.relay_z(3)
    travel.relay_g(1)
    travel.relay_h()
    wide(2)
    wide(3)
    all_sent(k.xrecv, k.x_r)

    def last_step(s, carry):
        r = pl.ds(pl.multiple_of(s * step_rows, step_rows), step_rows)
        for c in range(2):
            cols = slice(c * side_cols, (c + 1) * side_cols)
            k.out[r, cols] = (k.base[r, cols] + k.xrecv[c, s].astype(F32)).astype(BF16)
        return carry

    lax.fori_loop(0, half_blocks, last_step, 0)
    all_sent(k.esend, k.e_s)
    all_sent(k.xsend, k.x_s)
    all_sent(att.at[pl.ds(0, 2 * quarter)], k.a_s)
    p_copy.wait_send()
    travel.sent()


def layer_kernel(n, G, R, nb, kc, cw, names, *refs):
    k = types.SimpleNamespace(**dict(zip(names, refs, strict=True)))
    ow_loads = [pltpu.make_async_copy(k.ow_hbm, k.ow, k.sem_ow)]
    travel = Travel(k)
    blocks_done = project(n, G, R, nb, kc, k, ow_loads, travel)
    attend_and_mix(n, G, R, nb, cw, k, ow_loads, blocks_done, travel)


def local(
    n,
    tokens, query_weight, key_weight, value_weight, gate_weight,
    summary_pos, key_mixing, value_mixing, out_weight, chosen,
):
    rows, depth = tokens.shape
    heads = query_weight.shape[1] // HD
    G = key_weight.shape[1] // HD
    R = heads // G
    nb = rows // SB
    spans = rows // CMP
    slot = -(-spans // 8) * 8
    all_spans = -(-n * slot // LANES) * LANES
    kc = min(1024, depth)
    chunks = depth // kc
    width = out_weight.shape[1]
    cw = 512
    wide = width // (20 * LANES * 8 // 5) * 20 * LANES
    summed = width - wide
    oc = summed // cw
    gates_all = gate_weight.shape[1]
    assert G == 2 and n % 4 == 0 and 2 * gates_all == LANES and nb % 2 == 0

    vmem = pl.BlockSpec(memory_space=pltpu.VMEM)
    hbm = pl.BlockSpec(memory_space=pl.ANY)
    dma = pltpu.SemaphoreType.DMA
    V = pltpu.VMEM
    nbp = -(-nb // 8) * 8
    quarter = rows // 4
    half = nb // 2
    inputs = ["tok_hbm", "qw_hbm", "kw_hbm", "vw_hbm", "gw_hbm", "chosen_hbm", "km_hbm", "vm_hbm", "pos_hbm", "ow_hbm"]
    scratch = {
        "q_near": V((nb, G * HD, G * R * SB), BF16),
        "q_far": V((G, nb, 2 * HD, 2 * R * SB), BF16),
        "chosen": V(chosen.shape, jnp.int32),
        "km": V(key_mixing.shape[::-1], BF16),
        "vm": V(value_mixing.shape[::-1], BF16),
        "pos": V(summary_pos.shape, BF16),
        "sem_small": dma((4,)),
        "tok": V((rows, depth), BF16),
        "qw": V((depth, heads * HD), BF16),
        "kvw": V((depth, 2 * LANES), BF16),
        "gw": V((LANES, depth), BF16),
        "ow": V(out_weight.shape, BF16),
        "acc": V((rows, heads * HD), F32),
        "gacc": V((rows, LANES), F32),
        "gate": V((2, rows, heads * HD), F32),
        "keys": V((rows, LANES), BF16),
        "vals": V((LANES, rows), BF16),
        "left": V((G * nb, 2 * SB, LANES), BF16),
        "right": V((G * nb, 2 * SB, LANES), BF16),
        "named": V((G, nbp, LANES), jnp.int32),
        "bias": V((G, nbp, LANES), F32),
        "bias_smem": pltpu.SMEM((G, nbp, LANES), F32),
        "pos_wide": V((CMP, LANES), F32),
        "req": V((n, 8, LANES), jnp.int32),
        "req_in": V((n, 8, LANES), jnp.int32),
        "req_smem": pltpu.SMEM((n, 8, LANES), jnp.int32),
        "send": V((n, G, 2 * SB, LANES), BF16),
        "far": V((n - 1, G, 2 * SB, LANES), BF16),
        "sum_send": V((2 * slot, LANES), BF16),
        "sum_in": V((n, 2 * slot, LANES), BF16),
        "sum_key": V((all_spans, LANES), F32),
        "sum_val": V((all_spans, LANES), F32),
        "sum_keys": V((all_spans, LANES), BF16),
        "sum_vals": V((LANES, all_spans), BF16),
        "score": V((2, rows + n * slot, heads * HD), F32),
        "far_score": V((2 if n <= 16 else 1, G, (n - 1) * SB, 2 * R * SB), F32),
        "top": V((nb, 8, heads * HD), F32),
        "total": V((nb, 8, heads * HD), F32),
        "part": V((nb, HD, heads * HD), F32),
        "mixed": V((rows, heads * HD), F32),
        "att": V((rows, heads * HD), BF16),
        "halves": V((2 * quarter, cw), BF16),
        "mine": V((oc, quarter, cw), BF16),
        "dsend": V((oc, quarter, cw), BF16),
        "drecv": V((oc, quarter, cw), BF16),
        "early": V((half, SB, summed // 2), BF16),
        "esend": V((half, SB, summed // 2), BF16),
        "erecv": V((half, SB, summed // 2), BF16),
        "xsend": V((2 * half, SB // 2, summed // 2), BF16),
        "xrecv": V((2, half, SB // 2, summed // 2), BF16),
        "base": V((quarter, summed), F32),
        "wfar": V((3, out_weight.shape[0], wide), BF16),
        "att_in": V((3, quarter, heads * HD), BF16),
        "sem_ow": dma,
        "sem_bias": dma,
        "sem_req": dma((n,)),
        "sem_tok": dma((chunks,)), "sem_kw": dma((chunks,)), "sem_vw": dma((chunks,)),
        "req_s": dma, "req_r": dma((n,)), "blk_s": dma((n,)), "blk_r": dma((n,)),
        "sum_s": dma((n,)), "sum_r": dma((n,)),
        "d_s": dma, "d_r": dma, "e_s": dma, "e_r": dma((half,)), "x_s": dma, "x_r": dma,
        "a_s": dma, "a_r": dma, "p_s": dma, "p_r": dma,
        "wx_s": dma, "wx_r": dma((5,)), "wp_s": dma, "wp_r": dma,
        "wy_s": dma, "wy_r": dma((4,)), "wz_s": dma, "wz_r": dma((4,)),
        "wh_s": dma, "wh_r": dma((1,)), "wg_s": dma, "wg_r": dma((2,)), "wd_s": dma, "wd_r": dma((4,)),
    }
    return pl.pallas_call(
        functools.partial(layer_kernel, n, G, R, nb, kc, cw, inputs + ["out"] + list(scratch)),
        name="layer",
        out_shape=pltpu.VMEM((quarter, width), BF16),
        in_specs=[hbm] * 10,
        out_specs=vmem,
        scratch_shapes=list(scratch.values()),
        compiler_params=pltpu.CompilerParams(
            collective_id=1, has_side_effects=True, vmem_limit_bytes=VMEM_LIMIT
        ),
    )(
        tokens, query_weight, key_weight, value_weight, gate_weight.T,
        chosen, key_mixing.T, value_mixing.T, summary_pos, out_weight,
    )


def solution(mesh):
    placed = (
        P("kv", None),
        P(None, "tp"),
        P(None, "tp"),
        P(None, "tp"),
        P(),
        P(),
        P(),
        P(),
        P("tp", None),
        P("kv", "tp", None),
    )
    return jax.shard_map(
        functools.partial(local, mesh.shape["kv"]),
        mesh=mesh, in_specs=placed, out_specs=P(("kv", "tp"), None), check_vma=False,
    )
```
